512 devices in a mesh: sp: 64 (over z, y), fs: 4 (over x), tp: 2 (over core).
Axes of the slice: x: 4, y: 8, z: 8, core: 2. Of those that a mesh axis runs over, the one named last changes fastest.
Arguments:
- state_head_inputs: bfloat16 [4, 8192, 1024], P('fs', 'sp', 'tp'), may hold values from -6 to 6
- state_write_vectors: bfloat16 [4, 8192, 256], P('fs', 'sp', 'tp'), may hold values from -3 to 3
- state_read_vectors: bfloat16 [4, 8192, 256], P('fs', 'sp', 'tp'), may hold values from -3 to 3
- state_output_gate: bfloat16 [4, 8192, 1024], P('fs', 'sp', 'tp'), may hold values from -6 to 6
- presoftplus_steps: float32 [4, 16, 8192], P('fs', 'tp', 'sp'), may hold values from -6 to 6
- extra_decay_log: float32 [4, 16, 8192], P('fs', 'tp', 'sp'), may hold values from -2.1 to 0, as said below
- lane_shrinkage_powers: float32 [16], P('tp')
- bypass_coefficient_vector: float32 [16], P('tp'), may hold values from 0.5 to 4
- feeder_smoothing_stencil: bfloat16 [4, 1024], P(None, 'tp'), may hold values from -3 to 3
- stored_smoothing_stencil: bfloat16 [4, 256], P(None, 'tp'), may hold values from -3 to 3
- lookup_smoothing_stencil: bfloat16 [4, 256], P(None, 'tp'), may hold values from -3 to 3
- bundled_rescaling_vector: float32 [1024], P('tp'), may hold values from 0.1 to 1.9
- queries: bfloat16 [4, 8192, 1024], P('fs', 'sp', 'tp'), may hold values from -8 to 8
- attention_keys: bfloat16 [4, 8192, 256], P('fs', 'sp', 'tp'), may hold values from -8 to 8
- attention_values: bfloat16 [4, 8192, 256], P('fs', 'sp', 'tp'), may hold values from -6 to 6
- forget_gate_cumsum: float32 [4, 8192, 16], P('fs', 'sp', 'tp'), as said below
- state_out_weight: bfloat16 [1024, 2048], P('tp', 'fs'), may hold values from -0.1875 to 0.1875
- attention_out_weight: bfloat16 [1024, 2048], P('tp', 'fs'), may hold values from -0.75 to 0.75
Outputs:
- layer_output: bfloat16 [4, 8192, 2048], P('fs', ('sp', 'tp'))
The draws below stay inside these ranges and needn't reach their ends.
Inputs may be any that keep to these rules, and one draw needn't show every extreme that they name: `extra_decay_log`: nonpositive. `forget_gate_cumsum`: never rises along the positions of a sequence.
All inputs are finite; a program needn't handle non-finite values.
Results may differ from the reference program's by a relative error of at most 0.019.
Values may be sent and summed in bfloat16 or wider, within the bound.
A program may use at most 64 MiB of HBM per device.

```python
import math
import jax
import jax.numpy as jnp
from jax import lax

D = 2048
SPACE_MODEL_LANES = 16
FOX_QUESTIONERS = 16
KV_HEADS = 4
HEAD_DIM = 64
STATE = 128
GROUPS = 2
CONV = 4
TOKENS_PER_SHARD = 128
SEQS = 4
LENGTH = 8192
SSD_WIDTH = 1024
FOX_WIDTH = 1024


def fast_rate():
    return 1.0 / min(40, max(TOKENS_PER_SHARD // 4, 2))


def head_rates(plain_quantity, lane_tally):
    order_key, slow_key, quick_key = jax.random.split(plain_quantity, 3)
    order = jax.random.permutation(order_key, lane_tally)
    lingering_shrinkage = order < lane_tally // 2
    slow_rate = jax.random.uniform(slow_key, (lane_tally,), jnp.float32, 0.1, 0.6) / LENGTH
    quick = fast_rate() * jnp.exp(jax.random.uniform(quick_key, (lane_tally,), jnp.float32, -0.35, 0.35))
    return (jnp.where(lingering_shrinkage, slow_rate, quick), lingering_shrinkage)


def sudden_line_selector(plain_quantity, lane_tally):
    place_key, depth_key = jax.random.split(plain_quantity, 2)
    places = jax.random.randint(place_key, (SEQS, lane_tally, 3), 0, LENGTH)
    depth = jnp.log(jax.random.uniform(depth_key, (SEQS, lane_tally, 3), jnp.float32, 0.5, 0.8))
    positions = jnp.arange(LENGTH)
    hits = positions[None, None, None, :] == places[..., None]
    return jnp.sum(jnp.where(hits, depth[..., None], 0.0), axis=2)


def drawn_pairs(key):
    plain_quantity = jax.random.fold_in(key, 7)
    query_key, keys_key = jax.random.split(plain_quantity, 2)
    queries = jnp.clip(jax.random.normal(query_key, (SEQS, LENGTH, FOX_QUESTIONERS * HEAD_DIM), jnp.float32), -6.0, 6.0)
    keys = jnp.clip(jax.random.normal(keys_key, (SEQS, LENGTH, KV_HEADS * HEAD_DIM), jnp.float32), -6.0, 6.0)
    return (queries.astype(jnp.bfloat16), keys.astype(jnp.bfloat16))


def draw_queries(key, part):
    return drawn_pairs(key)[0]


def draw_attention_keys(key, part):
    return drawn_pairs(key)[1]


def draw_forget_gate_cumsum(key, part):
    plain_quantity = jax.random.fold_in(key, 31)
    ratio_generator, portion_generator, sample_generator_start, sudden_generator = jax.random.split(plain_quantity, 4)
    shrinkage_ratios, lingering_shrinkage = head_rates(ratio_generator, FOX_QUESTIONERS)
    blocks = LENGTH // TOKENS_PER_SHARD
    stretch_coefficient = jnp.exp(jax.random.uniform(portion_generator, (SEQS, blocks, FOX_QUESTIONERS), jnp.float32, math.log(0.5), math.log(2.0)))
    stretch_coefficient = jnp.repeat(stretch_coefficient, TOKENS_PER_SHARD, axis=1)
    scatter_breadth = jnp.exp(0.7 * jnp.clip(jax.random.normal(sample_generator_start, (SEQS, LENGTH, FOX_QUESTIONERS), jnp.float32), -4.0, 4.0))
    sudden_arrivals = sudden_line_selector(sudden_generator, FOX_QUESTIONERS).transpose(0, 2, 1) * lingering_shrinkage.astype(jnp.float32)
    return jnp.cumsum(-shrinkage_ratios * stretch_coefficient * scatter_breadth + sudden_arrivals, axis=1)


def draw_lane_shrinkage_powers(key, part):
    shrinkage_ratios, _ = head_rates(jax.random.fold_in(key, 41), SPACE_MODEL_LANES)
    return jnp.log(shrinkage_ratios)


def draw_presoftplus_steps(key, part):
    plain_quantity = jax.random.fold_in(key, 47)
    offset_key, noise_key = jax.random.split(plain_quantity, 2)
    blocks = LENGTH // TOKENS_PER_SHARD
    offset = jax.random.uniform(offset_key, (SEQS, SPACE_MODEL_LANES, blocks), jnp.float32, -1.2, 1.2)
    offset = jnp.repeat(offset, TOKENS_PER_SHARD, axis=2)
    noise = jnp.clip(jax.random.normal(noise_key, (SEQS, SPACE_MODEL_LANES, LENGTH), jnp.float32), -4.0, 4.0)
    return offset + 0.8 * noise


def draw_extra_decay_log(key, part):
    return sudden_line_selector(jax.random.fold_in(key, 53), SPACE_MODEL_LANES)


def block_levels(key, extent, cuts, smallest, largest):
    def one(dim, blocks):
        draws = jax.random.uniform(jax.random.fold_in(jax.random.fold_in(key, 6), dim), (blocks,), jnp.float32, smallest / len(cuts), largest / len(cuts))
        return jnp.repeat(jnp.exp(draws), extent[dim] // blocks).reshape((-1,) + (1,) * (len(extent) - dim - 1))

    gain = one(*cuts[0])
    for cut in cuts[1:]:
        gain = gain * one(*cut)
    return gain


def gaussian(key, extent, scale, limit, cuts=(), held_as=jnp.bfloat16):
    gain = block_levels(key, extent, cuts, -0.22, 0.18) if cuts else 1.0
    drawn = jax.random.normal(key, extent, jnp.float32) * scale * gain
    return jnp.minimum(jnp.maximum(drawn, -limit), limit).astype(held_as)


def setup_inputs(seed: int = 0) -> dict:
    key_list = jax.random.split(jax.random.key(seed), 19)
    state_head_inputs = gaussian(key_list[0], (SEQS, LENGTH, SSD_WIDTH), 1.0, 6.0, ((0, 4), (1, 64), (2, 2)))
    state_write_vectors = gaussian(key_list[1], (SEQS, LENGTH, GROUPS * STATE), 0.5, 3.0, ((0, 4), (1, 64), (2, 2)))
    state_read_vectors = gaussian(key_list[2], (SEQS, LENGTH, GROUPS * STATE), 0.5, 3.0, ((0, 4), (1, 64), (2, 2)))
    state_output_gate = gaussian(key_list[3], (SEQS, LENGTH, SSD_WIDTH), 1.0, 6.0, ((0, 4), (1, 64), (2, 2)))
    presoftplus_steps = draw_presoftplus_steps(jax.random.fold_in(key_list[18], 71), 0)
    extra_decay_log = draw_extra_decay_log(jax.random.fold_in(key_list[18], 71), 0)
    lane_shrinkage_powers = draw_lane_shrinkage_powers(jax.random.fold_in(key_list[18], 71), 0)
    bypass_coefficient_vector = jnp.clip(jnp.exp(math.log(4.0) - 2.0794415 * jax.random.uniform(key_list[7], (SPACE_MODEL_LANES,), jnp.float32) ** block_levels(key_list[7], (SPACE_MODEL_LANES,), ((0, 2),), -0.2, 0.2)), 0.5, 4.0)
    feeder_smoothing_stencil = gaussian(key_list[8], (CONV, SSD_WIDTH), CONV ** -0.5, 3.0, ((1, 2),))
    stored_smoothing_stencil = gaussian(key_list[9], (CONV, GROUPS * STATE), CONV ** -0.5, 3.0, ((1, 2),))
    lookup_smoothing_stencil = gaussian(key_list[10], (CONV, GROUPS * STATE), CONV ** -0.5, 3.0, ((1, 2),))
    bundled_rescaling_vector = jnp.clip(1.0 + 0.18 * jax.random.normal(key_list[11], (SSD_WIDTH,), jnp.float32), 0.1, 1.9)
    queries = draw_queries(jax.random.fold_in(key_list[18], 71), 0)
    attention_keys = draw_attention_keys(jax.random.fold_in(key_list[18], 71), 0)
    attention_values = gaussian(key_list[14], (SEQS, LENGTH, KV_HEADS * HEAD_DIM), 1.0, 6.0, ((0, 4), (1, 64), (2, 2)))
    forget_gate_cumsum = draw_forget_gate_cumsum(jax.random.fold_in(key_list[18], 71), 0)
    state_out_weight = gaussian(key_list[16], (SSD_WIDTH, D), SSD_WIDTH ** -0.5, 0.1875, ((0, 2), (1, 4)))
    attention_out_weight = gaussian(key_list[17], (FOX_WIDTH, D), HEAD_DIM ** -0.5, 0.75, ((0, 2), (1, 4)))
    return {"state_head_inputs": state_head_inputs, "state_write_vectors": state_write_vectors, "state_read_vectors": state_read_vectors, "state_output_gate": state_output_gate, "presoftplus_steps": presoftplus_steps, "extra_decay_log": extra_decay_log, "lane_shrinkage_powers": lane_shrinkage_powers, "bypass_coefficient_vector": bypass_coefficient_vector, "feeder_smoothing_stencil": feeder_smoothing_stencil, "stored_smoothing_stencil": stored_smoothing_stencil, "lookup_smoothing_stencil": lookup_smoothing_stencil, "bundled_rescaling_vector": bundled_rescaling_vector, "queries": queries, "attention_keys": attention_keys, "attention_values": attention_values, "forget_gate_cumsum": forget_gate_cumsum, "state_out_weight": state_out_weight, "attention_out_weight": attention_out_weight}


EPSILON = 1e-06
NEGATIVE = -1e+30

def rounded_value(values):
    return lax.optimization_barrier(values.astype(jnp.bfloat16)).astype(jnp.float32)

def causal_filter(feeder_quantities, taps):
    length = feeder_quantities.shape[0]
    tap_count = taps.shape[0]
    padded = jnp.concatenate([jnp.zeros((tap_count - 1, feeder_quantities.shape[1]), jnp.float32), feeder_quantities.astype(jnp.float32)], axis=0)
    summed = jnp.zeros((length, feeder_quantities.shape[1]), jnp.float32)
    for offset in range(tap_count):
        summed = summed + taps[offset].astype(jnp.float32) * padded[offset:offset + length]
    return jax.nn.silu(summed).astype(jnp.bfloat16)

def memory_series_yield(feeder_quantities, stored_quantity, fetched_quantity, opening_quantity, bare_stride, sudden_arrivals, lane_shrinkage_powers, bypass_coefficient_vector, feeder_smoothing_stencil, stored_smoothing_stencil, lookup_smoothing_stencil, bundled_rescaling_vector):
    conv_values = causal_filter(feeder_quantities, feeder_smoothing_stencil)
    conv_write = causal_filter(stored_quantity, stored_smoothing_stencil)
    conv_read = causal_filter(fetched_quantity, lookup_smoothing_stencil)
    stride_duration = jax.nn.softplus(bare_stride)
    shrinkage_natural_power = stride_duration * (-jnp.exp(lane_shrinkage_powers))[:, None] + sudden_arrivals
    lane_tally = stride_duration.shape[0]
    per_group = lane_tally // GROUPS
    blocks = LENGTH // TOKENS_PER_SHARD
    positions = jnp.arange(TOKENS_PER_SHARD, dtype=jnp.int32)
    causal = positions[:, None] >= positions[None, :]

    def advance(carried, pieces):
        values, writes, reads, steps, decays = pieces
        cumulative = jnp.cumsum(decays, axis=1)
        input_heads = values.reshape(TOKENS_PER_SHARD, GROUPS, per_group, HEAD_DIM).astype(jnp.float32)
        write_groups = writes.reshape(TOKENS_PER_SHARD, GROUPS, STATE).astype(jnp.float32)
        read_groups = reads.reshape(TOKENS_PER_SHARD, GROUPS, STATE).astype(jnp.float32)
        inner_products = jnp.einsum('tgn,sgn->gts', read_groups, write_groups)
        log_gap = jnp.where(causal[None], cumulative[:, :, None] - cumulative[:, None, :], -jnp.inf)
        weights = jnp.exp(log_gap) * steps[:, None, :]
        mix_weights = rounded_value(inner_products[:, None] * weights.reshape(GROUPS, per_group, TOKENS_PER_SHARD, TOKENS_PER_SHARD))
        local_part = jnp.einsum('ghts,sghp->tghp', mix_weights, input_heads)
        end_scale = (jnp.exp(cumulative[:, -1:] - cumulative) * steps).T.reshape(TOKENS_PER_SHARD, GROUPS, per_group)
        weighted = rounded_value(input_heads * end_scale[..., None])
        block_state = jnp.einsum('sghp,sgn->ghpn', weighted, write_groups)
        total_decay = jnp.exp(cumulative[:, -1]).reshape(GROUPS, per_group)
        carried_part = jnp.einsum('tgn,ghpn->tghp', read_groups, rounded_value(carried))
        carried_part = carried_part * jnp.exp(cumulative).T.reshape(TOKENS_PER_SHARD, GROUPS, per_group)[..., None]
        mixer_sum = local_part + carried_part + bypass_coefficient_vector.reshape(GROUPS, per_group)[None, :, :, None] * input_heads
        following = total_decay[..., None, None] * carried + block_state
        return (following, mixer_sum)
    pieces = (conv_values.reshape(blocks, TOKENS_PER_SHARD, -1), conv_write.reshape(blocks, TOKENS_PER_SHARD, -1), conv_read.reshape(blocks, TOKENS_PER_SHARD, -1), stride_duration.reshape(lane_tally, blocks, TOKENS_PER_SHARD).transpose(1, 0, 2), shrinkage_natural_power.reshape(lane_tally, blocks, TOKENS_PER_SHARD).transpose(1, 0, 2))
    starting = jnp.zeros((GROUPS, per_group, HEAD_DIM, STATE), jnp.float32)
    _, sums = lax.scan(advance, starting, pieces)
    gated_rows = sums.reshape(LENGTH, GROUPS, per_group * HEAD_DIM) * jax.nn.silu(opening_quantity.astype(jnp.float32)).reshape(LENGTH, GROUPS, -1)
    stretch_coefficient = lax.rsqrt(lax.optimization_barrier(jnp.mean(gated_rows * gated_rows, axis=-1, keepdims=True)) + EPSILON)
    return (gated_rows * stretch_coefficient * bundled_rescaling_vector.reshape(GROUPS, -1)).reshape(LENGTH, -1).astype(jnp.bfloat16)

def attend_sequence(queries, keys, values, gates):
    blocks = LENGTH // TOKENS_PER_SHARD
    lane_tally = gates.shape[1]
    key_group_count = keys.shape[1] // HEAD_DIM
    repeat_factor = lane_tally // key_group_count
    query_blocks = queries.reshape(blocks, TOKENS_PER_SHARD, key_group_count, repeat_factor, HEAD_DIM)
    key_blocks = keys.reshape(blocks, TOKENS_PER_SHARD, key_group_count, HEAD_DIM)
    value_blocks = values.reshape(blocks, TOKENS_PER_SHARD, key_group_count, HEAD_DIM)
    gate_blocks = gates.reshape(blocks, TOKENS_PER_SHARD, lane_tally)
    attention_score_scale = HEAD_DIM ** (-0.5)

    def one_block(pieces):
        query_block, query_gates, block_index = pieces
        query_head_count = query_block.astype(jnp.float32)
        query_index = block_index * TOKENS_PER_SHARD + jnp.arange(TOKENS_PER_SHARD, dtype=jnp.int32)

        def advance(key_index, partial_value):
            running_max, running_sum, weighted_sum = partial_value
            key_tile = key_blocks[key_index].astype(jnp.float32)
            value_tile = value_blocks[key_index].astype(jnp.float32)
            key_gates = gate_blocks[key_index]
            attention_scores = jnp.einsum('ezxp,czp->zxec', query_head_count, key_tile).reshape(lane_tally, TOKENS_PER_SHARD, TOKENS_PER_SHARD) * attention_score_scale
            attention_scores = attention_scores + query_gates.T[:, :, None] - key_gates.T[:, None, :]
            key_place = key_index * TOKENS_PER_SHARD + jnp.arange(TOKENS_PER_SHARD, dtype=jnp.int32)
            visible = key_place[None, :] <= query_index[:, None]
            attention_scores = jnp.where(visible[None], attention_scores, NEGATIVE)
            new_max = jnp.maximum(running_max, lax.optimization_barrier(jnp.max(attention_scores, axis=-1)))
            shrink = jnp.exp(running_max - new_max)
            attention_probs = jnp.where(visible[None], jnp.exp(attention_scores - new_max[..., None]), 0.0)
            running_sum = running_sum * shrink + lax.optimization_barrier(jnp.sum(attention_probs, axis=-1))
            weighted_value_sum = jnp.einsum('fljx,xfc->fljc', rounded_value(attention_probs).reshape(key_group_count, repeat_factor, TOKENS_PER_SHARD, TOKENS_PER_SHARD), value_tile)
            weighted_sum = weighted_sum * shrink[..., None] + weighted_value_sum.reshape(lane_tally, TOKENS_PER_SHARD, HEAD_DIM)
            return (new_max, running_sum, weighted_sum)
        starting = (jnp.full((lane_tally, TOKENS_PER_SHARD), NEGATIVE, jnp.float32), jnp.zeros((lane_tally, TOKENS_PER_SHARD), jnp.float32), jnp.zeros((lane_tally, TOKENS_PER_SHARD, HEAD_DIM), jnp.float32))
        _, running_sum, weighted_sum = lax.fori_loop(0, block_index + 1, advance, starting)
        return (weighted_sum / running_sum[..., None]).transpose(1, 0, 2).reshape(TOKENS_PER_SHARD, -1).astype(jnp.bfloat16)
    outputs = lax.map(one_block, (query_blocks, gate_blocks, jnp.arange(blocks, dtype=jnp.int32)))
    return outputs.reshape(LENGTH, -1)

def reference(state_head_inputs, state_write_vectors, state_read_vectors, state_output_gate, presoftplus_steps, extra_decay_log, lane_shrinkage_powers, bypass_coefficient_vector, feeder_smoothing_stencil, stored_smoothing_stencil, lookup_smoothing_stencil, bundled_rescaling_vector, queries, attention_keys, attention_values, forget_gate_cumsum, state_out_weight, attention_out_weight):
    results = []
    for sequence_input in range(SEQS):
        state_result = memory_series_yield(state_head_inputs[sequence_input], state_write_vectors[sequence_input], state_read_vectors[sequence_input], state_output_gate[sequence_input], presoftplus_steps[sequence_input], extra_decay_log[sequence_input], lane_shrinkage_powers, bypass_coefficient_vector, feeder_smoothing_stencil, stored_smoothing_stencil, lookup_smoothing_stencil, bundled_rescaling_vector)
        attend_out = attend_sequence(queries[sequence_input], attention_keys[sequence_input], attention_values[sequence_input], forget_gate_cumsum[sequence_input])
        merged = jnp.dot(state_result, state_out_weight, preferred_element_type=jnp.float32) + jnp.dot(attend_out, attention_out_weight, preferred_element_type=jnp.float32)
        results.append(merged.astype(jnp.bfloat16))
    return jnp.stack(results)
```

```python
import jax
import jax.numpy as jnp
from jax import lax
from jax.experimental import pallas as pl
from jax.experimental.pallas import tpu as pltpu
from jax.sharding import Mesh
from jax.sharding import PartitionSpec as P

SP = ("sp_0", "sp_1")
SP_TP = ("sp_0", "sp_1", "tp")
MESH = pl.DeviceIdType.MESH
BF16 = jnp.bfloat16
F32 = jnp.float32

RING = 8
FS = 4
ROWS = 128
HD = 64
BLOCK = ROWS + 16
MSG = HD + 16
EPSILON = 1e-06
NEG = -1e30

NT = (((1,), (1,)), ((), ()))
TN = (((0,), (0,)), ((), ()))


def mod8(i):
    return lax.rem(i + 2 * RING, RING)


def mod4(i):
    return lax.rem(i + 2 * FS, FS)


def dot(a, b, dims=None):
    if dims is None:
        return jnp.dot(a, b, preferred_element_type=F32)
    return lax.dot_general(a, b, dims, preferred_element_type=F32)


def silu(f):
    return f / (1.0 + jnp.exp(-f))


def split3(g):
    hi = g.astype(BF16).astype(F32)
    rest = g - hi
    mid = rest.astype(BF16).astype(F32)
    return hi, mid, rest - mid


def kernel(
    x_ref, w_ref, r_ref, gate_ref, step_ref, extra_ref, lane_ref, bypass_ref,
    xtap_ref, wtap_ref, rtap_ref, gain_ref, q_ref, k_ref, v_ref, g_ref, w1_ref, w2_ref,
    out_ref,
    kv, qs, wide, hx, hw, hr, m_sc, acc_sc, msg, s1, tot, s2, pre, cumpre, back, carried,
    xs_sc, ms_sc, rd_sc, ecum_sc, wbuf, give, take,
    kv1_send, kv1_recv, kv_send, kv_recv, s1_send, s1_recv, s2_send, s2_recv, s3_send, s3_recv,
    w_send, w_recv, own_sem, halo_send, halo_recv, tp_send, tp_recv,
):
    z, y = lax.axis_index("sp_0"), lax.axis_index("sp_1")
    fx, tp = lax.axis_index("fs"), lax.axis_index("tp")
    me = z * RING + y
    maj = (z, y)
    axis_of = ("sp_0", "sp_1")
    after, before = lax.rem(me + 1, RING * RING), lax.rem(me + RING * RING - 1, RING * RING)

    def at_sp(i):
        return {"sp_0": i // RING, "sp_1": lax.rem(i, RING)}

    def remote(src, dst, send, recv, where):
        return pltpu.make_async_remote_copy(
            src_ref=src, dst_ref=dst, send_sem=send, recv_sem=recv,
            device_id=where, device_id_type=MESH,
        )

    lane = lax.broadcasted_iota(jnp.int32, (ROWS, ROWS), 1)
    sub = lax.broadcasted_iota(jnp.int32, (ROWS, ROWS), 0)
    low = lane < HD
    sub8 = lax.broadcasted_iota(jnp.int32, (8, ROWS), 0)

    kf, vf = k_ref[...].astype(F32), v_ref[...].astype(F32)
    both = (
        jnp.where(low, kf, pltpu.roll(vf, HD, 1)).astype(BF16),
        jnp.where(low, pltpu.roll(kf, HD, 1), vf).astype(BF16),
    )
    wide[...] = jnp.zeros_like(wide)
    wide[:, 0:8] = g_ref[...]
    gt = wide[...].T[0:8]
    hi, mid, lo = split3(gt)
    four = sub8 < 4
    rows0 = jnp.concatenate(
        [jnp.where(four, hi, pltpu.roll(lo, 4, 0)), jnp.where(four, mid, 0.0)], axis=0
    )
    rows1 = jnp.concatenate(
        [jnp.where(four, pltpu.roll(hi, 4, 0), lo), jnp.where(four, pltpu.roll(mid, 4, 0), 0.0)], axis=0
    )
    kv[0, z, y, 0:ROWS] = both[0]
    kv[1, y, z, 0:ROWS] = both[1]
    kv[0, z, y, ROWS:BLOCK] = rows0.astype(BF16)
    kv[1, y, z, ROWS:BLOCK] = rows1.astype(BF16)
    for p in range(4):
        qf = q_ref[:, 128 * p : 128 * p + 128].astype(F32) * 0.125
        qs[2 * p] = jnp.where(low, qf, 0.0).astype(BF16)
        qs[2 * p + 1] = jnp.where(low, pltpu.roll(qf, HD, 1), 0.0).astype(BF16)

    barrier = pltpu.get_barrier_semaphore()
    peers = [{"sp_1": mod8(y + d)} for d in range(1, RING)]
    peers += [{"sp_0": mod8(z + d)} for d in range(1, RING)]
    peers += [{"fs": mod4(fx + 1)}, {"fs": mod4(fx - 1)}, {"tp": 1 - tp}]
    peers += [at_sp(after), at_sp(before)]
    for peer in peers:
        pl.semaphore_signal(barrier, inc=1, device_id=peer, device_id_type=MESH)
    pl.semaphore_wait(barrier, len(peers))

    halos = []
    for i, (src, dst) in enumerate(((x_ref, hx), (w_ref, hw), (r_ref, hr))):
        halos.append(
            remote(src.at[pl.ds(ROWS - 16, 16)], dst, halo_send.at[i], halo_recv.at[i], at_sp(after))
        )
        halos[-1].start()

    def first(c, d):
        peer = mod8(maj[1 - c] + d)
        own = kv.at[c, maj[c], maj[1 - c]]
        return remote(own, own, kv1_send.at[c, d], kv1_recv.at[c, RING - d],
                      {axis_of[1 - c]: peer})

    def first_arrival(c, d):
        peer = mod8(maj[1 - c] + d)
        slot = kv.at[c, maj[c], peer]
        return remote(slot, slot, kv1_send.at[c, d], kv1_recv.at[c, d], {axis_of[1 - c]: peer})

    for d in range(1, RING):
        for c in range(2):
            first(c, d).start()

    right, left = {"fs": mod4(fx + 1)}, {"fs": mod4(fx - 1)}
    owns = [
        pltpu.make_async_copy(w1_ref, wbuf.at[0, fx], own_sem.at[0]),
        pltpu.make_async_copy(w2_ref, wbuf.at[1, fx], own_sem.at[1]),
    ]

    def weights(j, d):
        src = (w1_ref, w2_ref)[j]
        return remote(src, wbuf.at[j, fx], w_send.at[j, d], w_recv.at[j, d], (right, left)[d])

    def weights_arrival(j, d):
        slot = wbuf.at[j, mod4(fx - 1) if d == 0 else mod4(fx + 1)]
        return remote(slot, slot, w_send.at[j, d], w_recv.at[j, d], (right, left)[d])

    def passed_on(j):
        slot = wbuf.at[j, mod4(fx - 1) if j == 0 else mod4(fx + 1)]
        return remote(slot, slot, w_send.at[j, 2], w_recv.at[j, 2], (right, left)[j])

    def passed_arrival(j):
        slot = wbuf.at[j, mod4(fx + 2)]
        return remote(slot, slot, w_send.at[j, 2], w_recv.at[j, 2], (right, left)[j])

    for o in owns:
        o.start()
    for j in range(2):
        for d in range(2):
            weights(j, d).start()

    for h in range(8):
        c = h // 4
        own = both[c]
        s = dot(qs[h], own, NT) - gt[h : h + 1, :]
        s = jnp.where(lane <= sub, s, NEG)
        m = jnp.max(s, axis=1, keepdims=True)
        p = jnp.exp(s - m)
        m_sc[h] = jnp.broadcast_to(m, (ROWS, ROWS))
        acc_sc[h] = dot(p.astype(BF16), jnp.where(low, 1.0, own.astype(F32)).astype(BF16))

    for h in halos:
        h.wait_recv()
    opening = me > 0

    def filtered(rows, halo, taps):
        old = jnp.where(opening, halo[...].astype(F32), 0.0)
        padded = jnp.concatenate([old, rows[...].astype(F32)], axis=0)
        t = taps[...].astype(F32)
        total = t[0:1] * padded[13 : 13 + ROWS]
        for o in range(1, 4):
            total = total + t[o : o + 1] * padded[13 + o : 13 + o + ROWS]
        return silu(total).astype(BF16)

    xs_sc[...] = filtered(x_ref, hx, xtap_ref)
    wr = filtered(w_ref, hw, wtap_ref)
    rd = filtered(r_ref, hr, rtap_ref)
    rd_sc[...] = rd
    raw = step_ref[...]
    step = jnp.maximum(raw, 0.0) + jnp.log1p(jnp.exp(-jnp.abs(raw)))
    rate = jnp.zeros((8, ROWS), F32)
    for h in range(8):
        rate = jnp.where(sub8 == h, lane_ref[h], rate)
    cum = step * (-jnp.exp(rate)) + extra_ref[...]
    lane8 = lax.broadcasted_iota(jnp.int32, (8, ROWS), 1)
    for shift in (1, 2, 4, 8, 16, 32, 64):
        cum = cum + jnp.where(lane8 >= shift, pltpu.roll(cum, shift, 1), 0.0)
    end = cum[:, ROWS - 1 : ROWS]
    scale = jnp.exp(end - cum) * step
    wide[0:8] = cum
    wide[8:16] = scale
    wide[16:24] = jnp.broadcast_to(end, (8, ROWS))
    turned = wide[...].T
    inner = dot(rd, wr, NT)
    causal = lane <= sub
    for p in range(4):
        xp = xs_sc[:, 128 * p : 128 * p + 128]
        parts = []
        for e in range(2):
            h = 2 * p + e
            gap = jnp.where(causal, turned[:, h : h + 1] - cum[h : h + 1, :], NEG)
            mix = inner * (jnp.exp(gap) * step[h : h + 1, :])
            parts.append(dot(mix.astype(BF16), xp))
        xf = xp.astype(F32)
        skip = jnp.where(low, bypass_ref[2 * p], bypass_ref[2 * p + 1])
        ms_sc[:, 128 * p : 128 * p + 128] = jnp.where(low, parts[0], parts[1]) + skip * xf
        ends = jnp.where(low, turned[:, 8 + 2 * p : 9 + 2 * p], turned[:, 9 + 2 * p : 10 + 2 * p])
        ecum_sc[:, 128 * p : 128 * p + 128] = jnp.exp(
            jnp.where(low, turned[:, 2 * p : 2 * p + 1], turned[:, 2 * p + 1 : 2 * p + 2])
        )
        state = dot((xf * ends).astype(BF16), wr, TN)
        for e in range(2):
            h = 2 * p + e
            msg[h, 0:HD] = state[HD * e : HD * e + HD].astype(BF16)

    def decay_rows(total):
        a, b, c3 = split3(total)
        return jnp.concatenate([jnp.where(four, a, c3), b], axis=0).astype(BF16)

    def decay_of(rows):
        f = rows.astype(F32)
        return (f[0:1] + f[8:9]) + f[4:5]

    for h in range(8):
        msg[h, HD:MSG] = decay_rows(jnp.broadcast_to(end[h : h + 1], (8, ROWS)))

    def around(src, dst, send, recv, axis, d):
        me_on = y if axis == "sp_1" else z
        peer = mod8(me_on + d)
        return remote(src(peer), dst.at[me_on], send.at[d], recv.at[RING - d], {axis: peer})

    def around_arrival(dst, send, recv, axis, d):
        me_on = y if axis == "sp_1" else z
        peer = mod8(me_on + d)
        slot = dst.at[peer]
        return remote(slot, slot, send.at[d], recv.at[d], {axis: peer})

    s1_out = [around(lambda p: msg.at[p], s1, s1_send, s1_recv, "sp_1", d) for d in range(1, RING)]
    for o in s1_out:
        o.start()
    s1[y] = msg[y]

    def bundle(c, row, half):
        return kv.at[c, row, pl.ds(4 * half, 4)]

    def hop(c, d, k):
        away = -(k // 2) if d == 0 else k // 2
        half = (0 if d == 0 else 1) if k == 6 else k % 2
        slot = bundle(c, mod8(maj[c] + away), half)
        to = mod8(maj[c] + (1 if d == 0 else -1))
        return remote(slot, slot, kv_send.at[c, d, k], kv_recv.at[c, d, k], {axis_of[c]: to})

    def hop_arrival(c, d, k):
        away = -(k // 2) - 1 if d == 0 else k // 2 + 1
        half = (0 if d == 0 else 1) if k == 6 else k % 2
        slot = bundle(c, mod8(maj[c] + away), half)
        to = mod8(maj[c] + (1 if d == 0 else -1))
        return remote(slot, slot, kv_send.at[c, d, k], kv_recv.at[c, d, k], {axis_of[c]: to})

    def attend(up, down, half_up, half_down):
        def one(c, carry):
            mine = jnp.where(c == 0, z, y)
            row_u, row_d = mod8(mine + up), mod8(mine + down)
            stride = jnp.where(c == 0, RING, 1)
            inner_stride = jnp.where(c == 0, 1, RING)
            lead_u = row_u * stride + 4 * half_up * inner_stride
            lead_d = row_d * stride + 4 * half_down * inner_stride

            @pl.when(jnp.minimum(lead_u, lead_d) < me)
            def _():
                keys, bias, vals = [], [], []
                for row, half, lead in ((row_u, half_up, lead_u), (row_d, half_down, lead_d)):
                    for b in range(4):
                        rows = kv[c, row, 4 * half + b, 0:ROWS]
                        g = kv[c, row, 4 * half + b, ROWS:BLOCK].astype(F32)
                        g = g[0:8] + g[8:16]
                        g = g + pltpu.roll(g, 4, 0)
                        seen = lead + b * inner_stride < me
                        bias.append(jnp.where(seen, -g, NEG))
                        keys.append(rows)
                        vals.append(jnp.where(low, jnp.ones_like(rows), rows))
                keys = jnp.concatenate(keys, axis=0)
                vals = jnp.concatenate(vals, axis=0)
                bias = jnp.concatenate(bias, axis=1)
                for i in range(4):
                    h = 4 * c + i
                    s = dot(qs[h], keys, NT) + bias[i : i + 1, :]
                    m_old = m_sc[h]
                    m_new = jnp.maximum(m_old, jnp.max(s, axis=1, keepdims=True))
                    m_sc[h] = m_new
                    p = jnp.exp(s - m_new[:, 0:1])
                    acc_sc[h] = acc_sc[h] * jnp.exp(m_old - m_new) + dot(p.astype(BF16), vals)

            return carry

        lax.fori_loop(0, 2, one, 0)

    for d in range(1, RING):
        for c in range(2):
            first_arrival(c, d).wait_recv()
    for k in range(2):
        for c in range(2):
            for d in range(2):
                hop(c, d, k).start()
    attend(0, 0, 0, 1)

    def stage(k):
        if k == 0:
            weights_arrival(0, 0).wait_recv()
            passed_on(0).start()
        if k == 1:
            for d in range(1, RING):
                around_arrival(s1, s1_send, s1_recv, "sp_1", d).wait_recv()
            run = jnp.zeros((HD, ROWS), F32)
            total = jnp.zeros((1, ROWS), F32)
            for j in range(RING):
                pre[j] = run
                cumpre[j] = jnp.broadcast_to(total, (8, ROWS))
                ld = decay_of(s1[j, HD:MSG])
                run = jnp.exp(ld) * run + s1[j, 0:HD].astype(F32)
                total = total + ld
            tot[0:HD] = run.astype(BF16)
            tot[HD:MSG] = decay_rows(jnp.broadcast_to(total, (8, ROWS)))
            for d in range(1, RING):
                around(lambda p: tot, s2, s2_send, s2_recv, "sp_0", d).start()
        if k == 3:
            for d in range(1, RING):
                around_arrival(s2, s2_send, s2_recv, "sp_0", d).wait_recv()
            s2[z] = tot[...]
            entering = jnp.zeros((HD, ROWS), F32)
            for j in range(RING - 1):
                later = jnp.exp(decay_of(s2[j, HD:MSG])) * entering + s2[j, 0:HD].astype(F32)
                entering = jnp.where(j < z, later, entering)
            for j in range(RING):
                back[j] = (pre[j] + jnp.exp(cumpre[j, 0:1]) * entering).astype(BF16)
            for d in range(1, RING):
                around(lambda p: back.at[p], carried, s3_send, s3_recv, "sp_1", d).start()
            carried[y] = back[y]
        if k == 4:
            weights_arrival(1, 1).wait_recv()
            passed_on(1).start()
        if k == 5:
            for d in range(1, RING):
                around_arrival(carried, s3_send, s3_recv, "sp_1", d).wait_recv()
            states = jnp.concatenate([carried[h] for h in range(8)], axis=0)
            u = dot(rd_sc[...], states, NT) * ecum_sc[...] + ms_sc[...]
            u = u * silu(gate_ref[...].astype(F32))
            stretch = lax.rsqrt(jnp.mean(u * u, axis=1, keepdims=True) + EPSILON)
            xs_sc[...] = (u * stretch * gain_ref[...]).astype(BF16)

    for k in range(7):
        for c in range(2):
            for d in range(2):
                hop_arrival(c, d, k).wait_recv()
        for c in range(2):
            if k < 5:
                hop(c, 0, k + 2).start()
            if k < 4:
                hop(c, 1, k + 2).start()
            if k == 5:
                hop(c, 1, 6).start()
        half_up = 0 if k == 6 else k % 2
        half_down = 1 if k == 6 else k % 2
        attend(-(k // 2) - 1, k // 2 + 1, half_up, half_down)
        stage(k)

    attended = []
    for p in range(4):
        a, b = acc_sc[2 * p], acc_sc[2 * p + 1]
        first_half = pltpu.roll(a, HD, 1) / a
        second_half = b / pltpu.roll(b, HD, 1)
        attended.append(jnp.where(low, first_half, second_half).astype(BF16))
    attended = jnp.concatenate(attended, axis=1)
    state_out = xs_sc[...]
    for o in owns:
        o.wait()
    weights_arrival(0, 1).wait_recv()
    weights_arrival(1, 0).wait_recv()
    for j in range(2):
        passed_arrival(j).wait_recv()
    whole = []
    half_rows = ROWS // 2
    for f in range(FS):
        merged = dot(state_out, wbuf[0, f]) + dot(attended, wbuf[1, f])
        top, bottom = merged[0:half_rows], merged[half_rows:ROWS]
        give[f] = jnp.where(tp == 0, bottom, top).astype(BF16)
        copy = remote(give.at[f], take.at[f], tp_send.at[f], tp_recv.at[f], {"tp": 1 - tp})
        copy.start()
        whole.append(jnp.where(tp == 0, top, bottom))
    for f in range(FS):
        copy = remote(give.at[f], take.at[f], tp_send.at[f], tp_recv.at[f], {"tp": 1 - tp})
        copy.wait_recv()
        out_ref[:, 512 * f : 512 * f + 512] = (whole[f] + take[f].astype(F32)).astype(BF16)

    for f in range(FS):
        remote(give.at[f], take.at[f], tp_send.at[f], tp_recv.at[f], {"tp": 1 - tp}).wait_send()
    for h in halos:
        h.wait_send()
    for d in range(1, RING):
        for c in range(2):
            first(c, d).wait_send()
        around(lambda p: msg.at[p], s1, s1_send, s1_recv, "sp_1", d).wait_send()
        around(lambda p: tot, s2, s2_send, s2_recv, "sp_0", d).wait_send()
        around(lambda p: back.at[p], carried, s3_send, s3_recv, "sp_1", d).wait_send()
    for k in range(7):
        for c in range(2):
            for d in range(2):
                hop(c, d, k).wait_send()
    for j in range(2):
        for d in range(2):
            weights(j, d).wait_send()
        passed_on(j).wait_send()


def shards(
    state_head_inputs, state_write_vectors, state_read_vectors, state_output_gate,
    presoftplus_steps, extra_decay_log, lane_shrinkage_powers, bypass_coefficient_vector,
    feeder_smoothing_stencil, stored_smoothing_stencil, lookup_smoothing_stencil,
    bundled_rescaling_vector, queries, attention_keys, attention_values, forget_gate_cumsum,
    state_out_weight, attention_out_weight,
):
    vmem = pl.BlockSpec(memory_space=pltpu.VMEM)
    smem = pl.BlockSpec(memory_space=pltpu.SMEM)
    anyw = pl.BlockSpec(memory_space=pl.ANY)
    dma = pltpu.SemaphoreType.DMA
    out = pl.pallas_call(
        kernel,
        out_shape=jax.ShapeDtypeStruct((ROWS // 2, 512 * FS), BF16),
        in_specs=[vmem] * 6 + [smem] * 2 + [vmem] * 8 + [anyw] * 2,
        out_specs=vmem,
        scratch_shapes=[
            pltpu.VMEM((2, RING, RING, BLOCK, ROWS), BF16),
            pltpu.VMEM((8, ROWS, ROWS), BF16),
            pltpu.VMEM((ROWS, ROWS), F32),
            pltpu.VMEM((16, 512), BF16),
            pltpu.VMEM((16, ROWS), BF16),
            pltpu.VMEM((16, ROWS), BF16),
            pltpu.VMEM((8, ROWS, ROWS), F32),
            pltpu.VMEM((8, ROWS, ROWS), F32),
            pltpu.VMEM((RING, MSG, ROWS), BF16),
            pltpu.VMEM((RING, MSG, ROWS), BF16),
            pltpu.VMEM((MSG, ROWS), BF16),
            pltpu.VMEM((RING, MSG, ROWS), BF16),
            pltpu.VMEM((RING, HD, ROWS), F32),
            pltpu.VMEM((RING, 8, ROWS), F32),
            pltpu.VMEM((RING, HD, ROWS), BF16),
            pltpu.VMEM((RING, HD, ROWS), BF16),
            pltpu.VMEM((ROWS, 512), BF16),
            pltpu.VMEM((ROWS, 512), F32),
            pltpu.VMEM((ROWS, ROWS), BF16),
            pltpu.VMEM((ROWS, 512), F32),
            pltpu.VMEM((2, FS, 512, 512), BF16),
            pltpu.VMEM((FS, ROWS // 2, 512), BF16),
            pltpu.VMEM((FS, ROWS // 2, 512), BF16),
            dma((2, RING)), dma((2, RING)),
            dma((2, 2, 7)), dma((2, 2, 7)),
            dma((RING,)), dma((RING,)), dma((RING,)), dma((RING,)), dma((RING,)), dma((RING,)),
            dma((2, 3)), dma((2, 3)), dma((2,)),
            dma((3,)), dma((3,)), dma((FS,)), dma((FS,)),
        ],
        compiler_params=pltpu.CompilerParams(
            collective_id=0, has_side_effects=True, vmem_limit_bytes=48 * 1024 * 1024
        ),
        name="mixer",
    )(
        state_head_inputs[0], state_write_vectors[0], state_read_vectors[0], state_output_gate[0],
        presoftplus_steps[0], extra_decay_log[0], lane_shrinkage_powers, bypass_coefficient_vector,
        feeder_smoothing_stencil, stored_smoothing_stencil, lookup_smoothing_stencil,
        bundled_rescaling_vector.reshape(1, -1), queries[0], attention_keys[0], attention_values[0],
        forget_gate_cumsum[0], state_out_weight, attention_out_weight,
    )
    return out[None]


def solution(mesh):
    split = Mesh(
        mesh.devices.reshape(8, 8, mesh.shape["fs"], mesh.shape["tp"]), ("sp_0", "sp_1", "fs", "tp")
    )
    placed = (
        P("fs", SP, "tp"),
        P("fs", SP, "tp"),
        P("fs", SP, "tp"),
        P("fs", SP, "tp"),
        P("fs", "tp", SP),
        P("fs", "tp", SP),
        P("tp"),
        P("tp"),
        P(None, "tp"),
        P(None, "tp"),
        P(None, "tp"),
        P("tp"),
        P("fs", SP, "tp"),
        P("fs", SP, "tp"),
        P("fs", SP, "tp"),
        P("fs", SP, "tp"),
        P("tp", "fs"),
        P("tp", "fs"),
    )
    return jax.shard_map(
        shards, mesh=split, in_specs=placed, out_specs=P("fs", SP_TP, None), check_vma=False
    )
```

```python
import jax
import jax.numpy as jnp
from jax import lax
from jax.experimental import pallas as pl
from jax.experimental.pallas import tpu as pltpu
from jax.sharding import Mesh
from jax.sharding import PartitionSpec as P

SP = ("sp_0", "sp_1")
SP_TP = ("sp_0", "sp_1", "tp")
MESH = pl.DeviceIdType.MESH
BF16 = jnp.bfloat16
F32 = jnp.float32

RING = 8
FS = 4
ROWS = 128
HD = 64
BLOCK = ROWS + 16
MSG = HD + 16
EPSILON = 1e-06
NEG = -1e30

NT = (((1,), (1,)), ((), ()))
TN = (((0,), (0,)), ((), ()))


def mod8(i):
    return lax.rem(i + 2 * RING, RING)


def mod4(i):
    return lax.rem(i + 2 * FS, FS)


def dot(a, b, dims=None):
    if dims is None:
        return jnp.dot(a, b, preferred_element_type=F32)
    return lax.dot_general(a, b, dims, preferred_element_type=F32)


def silu(f):
    return f / (1.0 + jnp.exp(-f))


def split3(g):
    hi = g.astype(BF16).astype(F32)
    rest = g - hi
    mid = rest.astype(BF16).astype(F32)
    return hi, mid, rest - mid


def kernel(
    x_in, w_in, r_in, gate_in, step_in, extra_in, lane_in, bypass_in, xtap_in, wtap_in, rtap_in,
    gain_in, q_in, k_in, v_in, g_in, w1_ref, w2_ref,
    out_ref,
    x_ref, w_ref, r_ref, gate_ref, step_ref, extra_ref, lane_ref, bypass_ref, xtap_ref, wtap_ref, rtap_ref,
    gain_ref, q_ref, k_ref, v_ref, g_ref,
    kv, qs, wide, hx, hw, hr, m_sc, acc_sc, msg, s1, tot, s2, pre, cumpre, back, carried,
    xs_sc, ms_sc, rd_sc, ecum_sc, wbuf, give, take, keep,
    kv1_send, kv1_recv, kv_send, kv_recv, s1_send, s1_recv, s2_send, s2_recv, s3_send, s3_recv,
    w_send, w_recv, own_sem, halo_send, halo_recv, tp_send, tp_recv, in_sem, ready,
):
    z, y = lax.axis_index("sp_0"), lax.axis_index("sp_1")
    fx, tp = lax.axis_index("fs"), lax.axis_index("tp")
    me = z * RING + y
    maj = (z, y)
    axis_of = ("sp_0", "sp_1")
    after = lax.rem(me + 1, RING * RING)
    last = RING - 1

    def at_sp(i):
        return {"sp_0": i // RING, "sp_1": lax.rem(i, RING)}

    def remote(src, dst, send, recv, where):
        return pltpu.make_async_remote_copy(
            src_ref=src, dst_ref=dst, send_sem=send, recv_sem=recv,
            device_id=where, device_id_type=MESH,
        )

    lane = lax.broadcasted_iota(jnp.int32, (ROWS, ROWS), 1)
    sub = lax.broadcasted_iota(jnp.int32, (ROWS, ROWS), 0)
    low = lane < HD
    sub8 = lax.broadcasted_iota(jnp.int32, (8, ROWS), 0)

    ins = [
        pltpu.make_async_copy(src, dst, in_sem.at[i])
        for i, (src, dst) in enumerate((
            (k_in, k_ref), (v_in, v_ref), (g_in, g_ref), (q_in, q_ref), (x_in, x_ref), (w_in, w_ref),
            (r_in, r_ref), (step_in, step_ref), (extra_in, extra_ref), (lane_in, lane_ref),
            (bypass_in, bypass_ref), (xtap_in, xtap_ref), (wtap_in, wtap_ref), (rtap_in, rtap_ref),
            (gate_in, gate_ref), (gain_in, gain_ref),
        ))
    ]
    for copy in ins:
        copy.start()

    def clear_row(row, carry):
        kv[0, row] = jnp.zeros((RING, BLOCK, ROWS), BF16)
        kv[1, y, row] = jnp.zeros((BLOCK, ROWS), BF16)
        return carry

    lax.fori_loop(z + 1, RING, clear_row, 0)

    @pl.when(z < 4)
    def _():
        kv[1, mod8(y + 4), 4:8] = jnp.zeros((4, BLOCK, ROWS), BF16)

    barrier = pltpu.get_barrier_semaphore()

    def greet(peer):
        pl.semaphore_signal(barrier, inc=1, device_id=peer, device_id_type=MESH)

    for d in range(1, RING):
        greet({"sp_1": mod8(y + d)})
    for peer in ({"fs": mod4(fx + 1)}, {"fs": mod4(fx - 1)}, {"tp": 1 - tp}):
        greet(peer)
    for d in range(1, RING):
        pl.when(z + d < RING)(lambda d=d: greet({"sp_0": z + d}))
    pl.when((y == 0) & (z > 0))(lambda: greet(at_sp(me - 1)))

    wide[...] = jnp.zeros_like(wide)
    for copy in ins[0:4]:
        copy.wait()
    kf, vf = k_ref[...].astype(F32), v_ref[...].astype(F32)
    both = (
        jnp.where(low, kf, pltpu.roll(vf, HD, 1)).astype(BF16),
        jnp.where(low, pltpu.roll(kf, HD, 1), vf).astype(BF16),
    )
    gt = g_ref[...]
    hi, mid, lo = split3(gt)
    four = sub8 < 4
    rows0 = jnp.concatenate(
        [jnp.where(four, hi, pltpu.roll(lo, 4, 0)), jnp.where(four, mid, 0.0)], axis=0
    )
    rows1 = jnp.concatenate(
        [jnp.where(four, pltpu.roll(hi, 4, 0), lo), jnp.where(four, pltpu.roll(mid, 4, 0), 0.0)], axis=0
    )
    kv[0, z, y, 0:ROWS] = both[0]
    kv[1, y, z, 0:ROWS] = both[1]
    kv[0, z, y, ROWS:BLOCK] = rows0.astype(BF16)
    kv[1, y, z, ROWS:BLOCK] = rows1.astype(BF16)
    for p in range(4):
        qf = q_ref[:, 128 * p : 128 * p + 128].astype(F32) * 0.125
        qs[2 * p] = jnp.where(low, qf, 0.0).astype(BF16)
        qs[2 * p + 1] = jnp.where(low, pltpu.roll(qf, HD, 1), 0.0).astype(BF16)

    for copy in ins[4:7]:
        copy.wait()
    inner_row = (y < last) | (z == last)
    pl.semaphore_wait(barrier, RING + 2 + z + jnp.where(inner_row, 0, 1))
    for d in range(1, RING):
        @pl.when(z - d >= 0)
        def _():
            pl.semaphore_signal(
                ready.at[z], inc=1, device_id={"sp_0": z - d}, device_id_type=MESH
            )

    halos = []
    for i, (src, dst) in enumerate(((x_ref, hx), (w_ref, hw), (r_ref, hr))):
        halos.append(
            remote(src.at[pl.ds(ROWS - 16, 16)], dst, halo_send.at[i], halo_recv.at[i], at_sp(after))
        )

    def each_halo(do):
        for h in halos:
            do(h)

    pl.when(me < RING * RING - 1)(lambda: each_halo(lambda h: h.start()))

    def first(c, d):
        peer = mod8(y + d) if c == 0 else z + d
        own = kv.at[c, maj[c], maj[1 - c]]
        return remote(own, own, kv1_send.at[c, d], kv1_recv.at[c, maj[1 - c]], {axis_of[1 - c]: peer})

    def first_arrival(c, b):
        slot = kv.at[c, maj[c], b]
        return remote(slot, slot, kv1_send.at[c, 0], kv1_recv.at[c, b], {axis_of[1 - c]: b})

    for d in range(1, RING):
        first(0, d).start()

    right, left = {"fs": mod4(fx + 1)}, {"fs": mod4(fx - 1)}
    owns = [
        pltpu.make_async_copy(w1_ref, wbuf.at[0, fx], own_sem.at[0]),
        pltpu.make_async_copy(w2_ref, wbuf.at[1, fx], own_sem.at[1]),
    ]

    def weights(j, d):
        src = (w1_ref, w2_ref)[j]
        return remote(src, wbuf.at[j, fx], w_send.at[j, d], w_recv.at[j, d], (right, left)[d])

    def weights_arrival(j, d):
        slot = wbuf.at[j, mod4(fx - 1) if d == 0 else mod4(fx + 1)]
        return remote(slot, slot, w_send.at[j, d], w_recv.at[j, d], (right, left)[d])

    def passed_on(j):
        slot = wbuf.at[j, mod4(fx - 1) if j == 0 else mod4(fx + 1)]
        return remote(slot, slot, w_send.at[j, 2], w_recv.at[j, 2], (right, left)[j])

    def passed_arrival(j):
        slot = wbuf.at[j, mod4(fx + 2)]
        return remote(slot, slot, w_send.at[j, 2], w_recv.at[j, 2], (right, left)[j])

    for o in owns:
        o.start()
    for j in range(2):
        for d in range(2):
            weights(j, d).start()

    for d in range(1, RING):
        @pl.when(z + d < RING)
        def _():
            pl.semaphore_wait(ready.at[z + d], 1)
            first(1, d).start()

    for h in range(8):
        c = h // 4
        own = both[c]
        s = dot(qs[h], own, NT) - gt[h : h + 1, :]
        s = jnp.where(lane <= sub, s, NEG)
        m = jnp.max(s, axis=1, keepdims=True)
        p = jnp.exp(s - m)
        m_sc[h] = jnp.broadcast_to(m, (ROWS, ROWS))
        acc_sc[h] = dot(p.astype(BF16), jnp.where(low, 1.0, own.astype(F32)).astype(BF16))

    for copy in ins[7:]:
        copy.wait()

    @pl.when(me > 0)
    def _():
        each_halo(lambda h: h.wait_recv())

    opening = me > 0

    def filtered(rows, halo, taps):
        old = jnp.where(opening, halo[...].astype(F32), 0.0)
        padded = jnp.concatenate([old, rows[...].astype(F32)], axis=0)
        t = taps[...].astype(F32)
        total = t[0:1] * padded[13 : 13 + ROWS]
        for o in range(1, 4):
            total = total + t[o : o + 1] * padded[13 + o : 13 + o + ROWS]
        return silu(total).astype(BF16)

    xs_sc[...] = filtered(x_ref, hx, xtap_ref)
    wr = filtered(w_ref, hw, wtap_ref)
    rd = filtered(r_ref, hr, rtap_ref)
    rd_sc[...] = rd
    raw = step_ref[...]
    step = jnp.maximum(raw, 0.0) + jnp.log1p(jnp.exp(-jnp.abs(raw)))
    on_diagonal = sub8[:, 0:8] == lax.broadcasted_iota(jnp.int32, (8, 8), 1)
    rate = jnp.sum(jnp.where(on_diagonal, lane_ref[...], 0.0), axis=1, keepdims=True)
    cum = step * (-jnp.exp(rate)) + extra_ref[...]
    lane8 = lax.broadcasted_iota(jnp.int32, (8, ROWS), 1)
    for shift in (1, 2, 4, 8, 16, 32, 64):
        cum = cum + jnp.where(lane8 >= shift, pltpu.roll(cum, shift, 1), 0.0)
    end = cum[:, ROWS - 1 : ROWS]
    scale = jnp.exp(end - cum) * step
    wide[0:8] = cum
    wide[8:16] = scale
    wide[16:24] = jnp.broadcast_to(end, (8, ROWS))
    turned = wide[...].T
    inner = dot(rd, wr, NT)
    causal = lane <= sub
    for p in range(4):
        xp = xs_sc[:, 128 * p : 128 * p + 128]
        parts = []
        for e in range(2):
            h = 2 * p + e
            gap = jnp.where(causal, turned[:, h : h + 1] - cum[h : h + 1, :], NEG)
            mix = inner * (jnp.exp(gap) * step[h : h + 1, :])
            parts.append(dot(mix.astype(BF16), xp))
        xf = xp.astype(F32)
        skip = jnp.where(low, bypass_ref[:, 2 * p : 2 * p + 1], bypass_ref[:, 2 * p + 1 : 2 * p + 2])
        ms_sc[:, 128 * p : 128 * p + 128] = jnp.where(low, parts[0], parts[1]) + skip * xf
        ends = jnp.where(low, turned[:, 8 + 2 * p : 9 + 2 * p], turned[:, 9 + 2 * p : 10 + 2 * p])
        ecum_sc[:, 128 * p : 128 * p + 128] = jnp.exp(
            jnp.where(low, turned[:, 2 * p : 2 * p + 1], turned[:, 2 * p + 1 : 2 * p + 2])
        )
        state = dot((xf * ends).astype(BF16), wr, TN)
        for e in range(2):
            h = 2 * p + e
            msg[h, 0:HD] = state[HD * e : HD * e + HD].astype(BF16)

    def decay_rows(total):
        a, b, c3 = split3(total)
        return jnp.concatenate([jnp.where(four, a, c3), b], axis=0).astype(BF16)

    def decay_of(rows):
        f = rows.astype(F32)
        return (f[0:1] + f[8:9]) + f[4:5]

    for h in range(8):
        msg[h, HD:MSG] = decay_rows(jnp.broadcast_to(end[h : h + 1], (8, ROWS)))

    def around(src, dst, send, recv, axis, d):
        me_on = y if axis == "sp_1" else z
        peer = mod8(me_on + d)
        return remote(src(peer), dst.at[me_on], send.at[d], recv.at[RING - d], {axis: peer})

    def around_arrival(dst, send, recv, axis, d):
        me_on = y if axis == "sp_1" else z
        peer = mod8(me_on + d)
        slot = dst.at[peer]
        return remote(slot, slot, send.at[d], recv.at[d], {axis: peer})

    def up_total(d):
        return remote(tot, s2.at[z], s2_send.at[d], s2_recv.at[z], {"sp_0": z + d})

    s1_out = [around(lambda p: msg.at[p], s1, s1_send, s1_recv, "sp_1", d) for d in range(1, RING)]
    for o in s1_out:
        o.start()
    s1[y] = msg[y]

    def bundle(c, row, half):
        return kv.at[c, row, pl.ds(4 * half, 4)]

    def hop(c, d, k):
        away = -(k // 2) if d == 0 else k // 2
        half = (0 if d == 0 else 1) if k == 6 else k % 2
        slot = bundle(c, mod8(maj[c] + away), half)
        to = mod8(maj[c] + (1 if d == 0 else -1))
        return remote(slot, slot, kv_send.at[c, d, k], kv_recv.at[c, d, k], {axis_of[c]: to})

    def hop_arrival(c, d, k):
        away = -(k // 2) - 1 if d == 0 else k // 2 + 1
        half = (0 if d == 0 else 1) if k == 6 else k % 2
        slot = bundle(c, mod8(maj[c] + away), half)
        to = mod8(maj[c] + (1 if d == 0 else -1))
        return remote(slot, slot, kv_send.at[c, d, k], kv_recv.at[c, d, k], {axis_of[c]: to})

    def going(c, d, k):
        half = (0 if d == 0 else 1) if k == 6 else k % 2
        if c == 1:
            return z >= 4 * half
        if d == 0:
            return (z - k // 2 >= 0) & (z < last)
        return mod8(z + k // 2) <= 2 + half

    def coming(c, d, k):
        half = (0 if d == 0 else 1) if k == 6 else k % 2
        if c == 1:
            return z >= 4 * half
        if d == 0:
            return z - 1 - k // 2 >= 0
        return mod8(z + 1 + k // 2) <= 2 + half

    def send(c, d, k):
        pl.when(going(c, d, k))(lambda: hop(c, d, k).start())

    def attend(up, down, half_up, half_down):
        def one(c, carry):
            mine = jnp.where(c == 0, z, y)
            row_u, row_d = mod8(mine + up), mod8(mine + down)
            stride = jnp.where(c == 0, RING, 1)
            inner_stride = jnp.where(c == 0, 1, RING)
            lead_u = row_u * stride + 4 * half_up * inner_stride
            lead_d = row_d * stride + 4 * half_down * inner_stride

            @pl.when(jnp.minimum(lead_u, lead_d) < me)
            def _():
                keys, bias, vals = [], [], []
                for row, half, lead in ((row_u, half_up, lead_u), (row_d, half_down, lead_d)):
                    for b in range(4):
                        rows = kv[c, row, 4 * half + b, 0:ROWS]
                        g = kv[c, row, 4 * half + b, ROWS:BLOCK].astype(F32)
                        g = g[0:8] + g[8:16]
                        g = g + pltpu.roll(g, 4, 0)
                        seen = lead + b * inner_stride < me
                        bias.append(jnp.where(seen, -g, NEG))
                        keys.append(rows)
                        vals.append(jnp.where(low, jnp.ones_like(rows), rows))
                keys = jnp.concatenate(keys, axis=0)
                vals = jnp.concatenate(vals, axis=0)
                bias = jnp.concatenate(bias, axis=1)
                for i in range(4):
                    h = 4 * c + i
                    s = dot(qs[h], keys, NT) + bias[i : i + 1, :]
                    m_old = m_sc[h]
                    m_new = jnp.maximum(m_old, jnp.max(s, axis=1, keepdims=True))
                    m_sc[h] = m_new
                    p = jnp.exp(s - m_new[:, 0:1])
                    acc_sc[h] = acc_sc[h] * jnp.exp(m_old - m_new) + dot(p.astype(BF16), vals)

            return carry

        lax.fori_loop(0, 2, one, 0)

    for half in range(2):
        for c in range(2):
            for b in range(4 * half, 4 * half + 4):
                there = (b != y) if c == 0 else (b < z)
                pl.when(there)(lambda: first_arrival(c, b).wait_recv())
            for d in range(2):
                send(c, d, half)
    attend(0, 0, 0, 1)

    def stage(k):
        if k == 2:
            weights_arrival(0, 0).wait_recv()
            passed_on(0).start()
        if k == 1:
            for d in range(1, RING):
                around_arrival(s1, s1_send, s1_recv, "sp_1", d).wait_recv()
            run = jnp.zeros((HD, ROWS), F32)
            total = jnp.zeros((1, ROWS), F32)
            for j in range(RING):
                pre[j] = run
                cumpre[j] = jnp.broadcast_to(total, (8, ROWS))
                ld = decay_of(s1[j, HD:MSG])
                run = jnp.exp(ld) * run + s1[j, 0:HD].astype(F32)
                total = total + ld
            tot[0:HD] = run.astype(BF16)
            tot[HD:MSG] = decay_rows(jnp.broadcast_to(total, (8, ROWS)))
            for d in range(1, RING):
                pl.when(z + d < RING)(lambda: up_total(d).start())
        if k == 3:
            for j in range(RING - 1):
                slot = s2.at[j]
                come = remote(slot, slot, s2_send.at[0], s2_recv.at[j], {"sp_0": j})
                pl.when(j < z)(lambda: come.wait_recv())
            entering = jnp.zeros((HD, ROWS), F32)
            for j in range(RING - 1):
                later = jnp.exp(decay_of(s2[j, HD:MSG])) * entering + s2[j, 0:HD].astype(F32)
                entering = jnp.where(j < z, later, entering)
            for j in range(RING):
                back[j] = (pre[j] + jnp.exp(cumpre[j, 0:1]) * entering).astype(BF16)
            for d in range(1, RING):
                around(lambda p: back.at[p], carried, s3_send, s3_recv, "sp_1", d).start()
            carried[y] = back[y]
        if k == 5:
            weights_arrival(1, 1).wait_recv()
            passed_on(1).start()
        if k == 6:
            for d in range(1, RING):
                around_arrival(carried, s3_send, s3_recv, "sp_1", d).wait_recv()
            states = jnp.concatenate([carried[h] for h in range(8)], axis=0)
            u = dot(rd_sc[...], states, NT) * ecum_sc[...] + ms_sc[...]
            u = u * silu(gate_ref[...].astype(F32))
            stretch = lax.rsqrt(jnp.mean(u * u, axis=1, keepdims=True) + EPSILON)
            xs_sc[...] = (u * stretch * gain_ref[...]).astype(BF16)

    for k in range(7):
        for c in range(2):
            for d in range(2):
                pl.when(coming(c, d, k))(lambda: hop_arrival(c, d, k).wait_recv())
        for c in range(2):
            if k < 5:
                send(c, 0, k + 2)
            if k < 4:
                send(c, 1, k + 2)
            if k == 5:
                send(c, 1, 6)
        half_up = 0 if k == 6 else k % 2
        half_down = 1 if k == 6 else k % 2
        attend(-(k // 2) - 1, k // 2 + 1, half_up, half_down)
        stage(k)

    attended = []
    for p in range(4):
        a, b = acc_sc[2 * p], acc_sc[2 * p + 1]
        first_half = pltpu.roll(a, HD, 1) / a
        second_half = b / pltpu.roll(b, HD, 1)
        attended.append(jnp.where(low, first_half, second_half).astype(BF16))
    attended = jnp.concatenate(attended, axis=1)
    state_out = xs_sc[...]
    half_rows = ROWS // 2

    def across(n):
        return remote(give.at[n], take.at[n], tp_send.at[n], tp_recv.at[n], {"tp": 1 - tp})

    columns = (fx, mod4(fx - 1), mod4(fx + 1), mod4(fx + 2))
    for n, f in enumerate(columns):
        if n == 0:
            for o in owns:
                o.wait()
        elif n == 1:
            weights_arrival(1, 0).wait_recv()
        elif n == 2:
            weights_arrival(0, 1).wait_recv()
        else:
            passed_arrival(0).wait_recv()
            passed_arrival(1).wait_recv()
        merged = dot(state_out, wbuf[0, f]) + dot(attended, wbuf[1, f])
        top, bottom = merged[0:half_rows], merged[half_rows:ROWS]
        give[n] = jnp.where(tp == 0, bottom, top).astype(BF16)
        across(n).start()
        keep[n] = jnp.where(tp == 0, top, bottom)
    for n, f in enumerate(columns):
        across(n).wait_recv()
        out_ref[:, pl.ds(pl.multiple_of(512 * f, 512), 512)] = (keep[n] + take[n].astype(F32)).astype(BF16)

    for n in range(FS):
        across(n).wait_send()
    pl.when(me < RING * RING - 1)(lambda: each_halo(lambda h: h.wait_send()))
    for d in range(1, RING):
        first(0, d).wait_send()
        around(lambda p: msg.at[p], s1, s1_send, s1_recv, "sp_1", d).wait_send()
        around(lambda p: back.at[p], carried, s3_send, s3_recv, "sp_1", d).wait_send()

        @pl.when(z + d < RING)
        def _():
            first(1, d).wait_send()
            up_total(d).wait_send()
    for k in range(7):
        for c in range(2):
            for d in range(2):
                pl.when(going(c, d, k))(lambda: hop(c, d, k).wait_send())
    for j in range(2):
        for d in range(2):
            weights(j, d).wait_send()
        passed_on(j).wait_send()


def shards(
    state_head_inputs, state_write_vectors, state_read_vectors, state_output_gate,
    presoftplus_steps, extra_decay_log, lane_shrinkage_powers, bypass_coefficient_vector,
    feeder_smoothing_stencil, stored_smoothing_stencil, lookup_smoothing_stencil,
    bundled_rescaling_vector, queries, attention_keys, attention_values, forget_gate_cumsum,
    state_out_weight, attention_out_weight,
):
    vmem = pl.BlockSpec(memory_space=pltpu.VMEM)
    hbm = pl.BlockSpec(memory_space=pltpu.HBM)
    dma = pltpu.SemaphoreType.DMA
    out = pl.pallas_call(
        kernel,
        out_shape=jax.ShapeDtypeStruct((ROWS // 2, 512 * FS), BF16),
        in_specs=[hbm] * 18,
        out_specs=vmem,
        scratch_shapes=[
            pltpu.VMEM((ROWS, 512), BF16), pltpu.VMEM((ROWS, ROWS), BF16), pltpu.VMEM((ROWS, ROWS), BF16),
            pltpu.VMEM((ROWS, 512), BF16), pltpu.VMEM((8, ROWS), F32), pltpu.VMEM((8, ROWS), F32),
            pltpu.VMEM((1, 8), F32), pltpu.VMEM((1, 8), F32),
            pltpu.VMEM((4, 512), BF16), pltpu.VMEM((4, ROWS), BF16), pltpu.VMEM((4, ROWS), BF16),
            pltpu.VMEM((1, 512), F32), pltpu.VMEM((ROWS, 512), BF16), pltpu.VMEM((ROWS, ROWS), BF16),
            pltpu.VMEM((ROWS, ROWS), BF16), pltpu.VMEM((8, ROWS), F32),
            pltpu.VMEM((2, RING, RING, BLOCK, ROWS), BF16),
            pltpu.VMEM((8, ROWS, ROWS), BF16),
            pltpu.VMEM((ROWS, ROWS), F32),
            pltpu.VMEM((16, 512), BF16),
            pltpu.VMEM((16, ROWS), BF16),
            pltpu.VMEM((16, ROWS), BF16),
            pltpu.VMEM((8, ROWS, ROWS), F32),
            pltpu.VMEM((8, ROWS, ROWS), F32),
            pltpu.VMEM((RING, MSG, ROWS), BF16),
            pltpu.VMEM((RING, MSG, ROWS), BF16),
            pltpu.VMEM((MSG, ROWS), BF16),
            pltpu.VMEM((RING, MSG, ROWS), BF16),
            pltpu.VMEM((RING, HD, ROWS), F32),
            pltpu.VMEM((RING, 8, ROWS), F32),
            pltpu.VMEM((RING, HD, ROWS), BF16),
            pltpu.VMEM((RING, HD, ROWS), BF16),
            pltpu.VMEM((ROWS, 512), BF16),
            pltpu.VMEM((ROWS, 512), F32),
            pltpu.VMEM((ROWS, ROWS), BF16),
            pltpu.VMEM((ROWS, 512), F32),
            pltpu.VMEM((2, FS, 512, 512), BF16),
            pltpu.VMEM((FS, ROWS // 2, 512), BF16),
            pltpu.VMEM((FS, ROWS // 2, 512), BF16),
            pltpu.VMEM((FS, ROWS // 2, 512), F32),
            dma((2, RING)), dma((2, RING)),
            dma((2, 2, 7)), dma((2, 2, 7)),
            dma((RING,)), dma((RING,)), dma((RING,)), dma((RING,)), dma((RING,)), dma((RING,)),
            dma((2, 3)), dma((2, 3)), dma((2,)),
            dma((3,)), dma((3,)), dma((FS,)), dma((FS,)), dma((16,)),
            pltpu.SemaphoreType.REGULAR((RING,)),
        ],
        compiler_params=pltpu.CompilerParams(
            collective_id=0, has_side_effects=True, vmem_limit_bytes=60 * 1024 * 1024
        ),
        name="mixer",
    )(
        state_head_inputs[0], state_write_vectors[0], state_read_vectors[0], state_output_gate[0],
        presoftplus_steps[0], extra_decay_log[0],
        lane_shrinkage_powers.reshape(1, -1), bypass_coefficient_vector.reshape(1, -1),
        feeder_smoothing_stencil, stored_smoothing_stencil, lookup_smoothing_stencil,
        bundled_rescaling_vector.reshape(1, -1), queries[0], attention_keys[0], attention_values[0],
        forget_gate_cumsum[0].T, state_out_weight, attention_out_weight,
    )
    return out[None]


def solution(mesh):
    split = Mesh(
        mesh.devices.reshape(8, 8, mesh.shape["fs"], mesh.shape["tp"]), ("sp_0", "sp_1", "fs", "tp")
    )
    placed = (
        P("fs", SP, "tp"),
        P("fs", SP, "tp"),
        P("fs", SP, "tp"),
        P("fs", SP, "tp"),
        P("fs", "tp", SP),
        P("fs", "tp", SP),
        P("tp"),
        P("tp"),
        P(None, "tp"),
        P(None, "tp"),
        P(None, "tp"),
        P("tp"),
        P("fs", SP, "tp"),
        P("fs", SP, "tp"),
        P("fs", SP, "tp"),
        P("fs", SP, "tp"),
        P("tp", "fs"),
        P("tp", "fs"),
    )
    return jax.shard_map(
        shards, mesh=split, in_specs=placed, out_specs=P("fs", SP_TP, None), check_vma=False
    )
```

```python
import jax
import jax.numpy as jnp
from jax import lax
from jax.experimental import pallas as pl
from jax.experimental.pallas import tpu as pltpu
from jax.sharding import Mesh
from jax.sharding import PartitionSpec as P

SP = ("sp_0", "sp_1")
SP_TP = ("sp_0", "sp_1", "tp")
MESH = pl.DeviceIdType.MESH
BF16 = jnp.bfloat16
F32 = jnp.float32

RING = 8
FS = 4
ROWS = 128
HD = 64
BLOCK = ROWS + 16
MSG = HD + 16
EPSILON = 1e-06
NEG = -1e30

NT = (((1,), (1,)), ((), ()))
TN = (((0,), (0,)), ((), ()))


def mod8(i):
    return lax.rem(i + 2 * RING, RING)


def mod4(i):
    return lax.rem(i + 2 * FS, FS)


def dot(a, b, dims=None):
    if dims is None:
        return jnp.dot(a, b, preferred_element_type=F32)
    return lax.dot_general(a, b, dims, preferred_element_type=F32)


def silu(f):
    return f / (1.0 + jnp.exp(-f))


def split3(g):
    hi = g.astype(BF16).astype(F32)
    rest = g - hi
    mid = rest.astype(BF16).astype(F32)
    return hi, mid, rest - mid


def kernel(
    x_in, w_in, r_in, gate_in, step_in, extra_in, lane_in, bypass_in, xtap_in, wtap_in, rtap_in,
    gain_in, q_in, k_in, v_in, g_in, w1_ref, w2_ref,
    out_ref,
    x_ref, w_ref, r_ref, gate_ref, step_ref, extra_ref, lane_ref, bypass_ref, xtap_ref, wtap_ref, rtap_ref,
    gain_ref, q_ref, k_ref, v_ref, g_ref,
    kv, qs, wide, hx, hw, hr, m_sc, acc_sc, msg, s1, tot, s2, pre, cumpre, back, carried,
    xs_sc, ms_sc, rd_sc, ecum_sc, wbuf, give, take, keep,
    kv1_send, kv1_recv, kv_send, kv_recv, s1_send, s1_recv, s2_send, s2_recv, s3_send, s3_recv,
    w_send, w_recv, own_sem, halo_send, halo_recv, tp_send, tp_recv, in_sem, ready,
):
    z, y = lax.axis_index("sp_0"), lax.axis_index("sp_1")
    fx, tp = lax.axis_index("fs"), lax.axis_index("tp")
    me = z * RING + y
    maj = (z, y)
    axis_of = ("sp_0", "sp_1")
    after = lax.rem(me + 1, RING * RING)
    last = RING - 1

    def at_sp(i):
        return {"sp_0": i // RING, "sp_1": lax.rem(i, RING)}

    def remote(src, dst, send, recv, where):
        return pltpu.make_async_remote_copy(
            src_ref=src, dst_ref=dst, send_sem=send, recv_sem=recv,
            device_id=where, device_id_type=MESH,
        )

    lane = lax.broadcasted_iota(jnp.int32, (ROWS, ROWS), 1)
    sub = lax.broadcasted_iota(jnp.int32, (ROWS, ROWS), 0)
    low = lane < HD
    sub8 = lax.broadcasted_iota(jnp.int32, (8, ROWS), 0)

    ins = [
        pltpu.make_async_copy(src, dst, in_sem.at[i])
        for i, (src, dst) in enumerate((
            (k_in, k_ref), (v_in, v_ref), (g_in, g_ref), (q_in, q_ref), (x_in, x_ref), (w_in, w_ref),
            (r_in, r_ref), (step_in, step_ref), (extra_in, extra_ref), (lane_in, lane_ref),
            (bypass_in, bypass_ref), (xtap_in, xtap_ref), (wtap_in, wtap_ref), (rtap_in, rtap_ref),
            (gate_in, gate_ref), (gain_in, gain_ref),
        ))
    ]
    for copy in ins:
        copy.start()

    def clear_row(row, carry):
        kv[0, row] = jnp.zeros((RING, BLOCK, ROWS), BF16)
        kv[1, y, row] = jnp.zeros((BLOCK, ROWS), BF16)
        return carry

    lax.fori_loop(z + 1, RING, clear_row, 0)

    @pl.when(z < 4)
    def _():
        kv[1, mod8(y + 4), 4:8] = jnp.zeros((4, BLOCK, ROWS), BF16)

    barrier = pltpu.get_barrier_semaphore()

    def greet(peer):
        pl.semaphore_signal(barrier, inc=1, device_id=peer, device_id_type=MESH)

    for d in range(1, RING):
        greet({"sp_1": mod8(y + d)})
    for peer in ({"fs": mod4(fx + 1)}, {"fs": mod4(fx - 1)}, {"tp": 1 - tp}):
        greet(peer)
    for d in range(1, RING):
        pl.when(z + d < RING)(lambda d=d: greet({"sp_0": z + d}))
    pl.when((y == 0) & (z > 0))(lambda: greet(at_sp(me - 1)))

    wide[...] = jnp.zeros_like(wide)
    for copy in ins[0:4]:
        copy.wait()
    kf, vt = k_ref[...].astype(F32), v_ref[...].astype(F32).T
    low64 = low[0:HD]
    key_rows = (
        jnp.where(low64, kf[0:HD], pltpu.roll(kf[HD:ROWS], HD, 1)),
        jnp.where(low64, pltpu.roll(kf[0:HD], HD, 1), kf[HD:ROWS]),
    )
    hi, mid, lo = split3(-g_ref[...])
    four = sub8 < 4
    gate_rows = (
        jnp.concatenate(
            [jnp.where(four, hi, pltpu.roll(lo, 4, 0)), jnp.where(four, mid, 0.0)], axis=0
        ),
        jnp.concatenate(
            [jnp.where(four, pltpu.roll(hi, 4, 0), lo), jnp.where(four, pltpu.roll(mid, 4, 0), 0.0)],
            axis=0,
        ),
    )
    for c in range(2):
        spot = (c, maj[c], maj[1 - c])
        kv[spot + (slice(0, HD),)] = key_rows[c].astype(BF16)
        kv[spot + (slice(HD, ROWS),)] = vt[HD * c : HD * c + HD].astype(BF16)
        kv[spot + (slice(ROWS, BLOCK),)] = gate_rows[c].astype(BF16)
    for h in range(8):
        p, e = h // 2, h % 2
        qf = q_ref[:, 128 * p : 128 * p + 128].astype(F32) * 0.125
        turn = pltpu.roll(qf, HD, 1)
        at = slice(ROWS * e, ROWS * e + ROWS)
        picks = jnp.where(lax.rem(lane, 4) == h % 4, 1.0, 0.0).astype(BF16)
        head, other = (qf, turn) if e == 0 else (turn, qf)
        qs[p, 0, at, 0:ROWS] = jnp.where(low, head, 0.0).astype(BF16)
        qs[p, 1, at, 0:ROWS] = jnp.where(low, 0.0, other).astype(BF16)
        for n in range(2):
            qs[p, n, at, ROWS : 2 * ROWS] = picks

    for copy in ins[4:7]:
        copy.wait()
    inner_row = (y < last) | (z == last)
    pl.semaphore_wait(barrier, RING + 2 + z + jnp.where(inner_row, 0, 1))
    for d in range(1, RING):
        @pl.when(z - d >= 0)
        def _():
            pl.semaphore_signal(
                ready.at[z], inc=1, device_id={"sp_0": z - d}, device_id_type=MESH
            )

    halos = []
    for i, (src, dst) in enumerate(((x_ref, hx), (w_ref, hw), (r_ref, hr))):
        halos.append(
            remote(src.at[pl.ds(ROWS - 16, 16)], dst, halo_send.at[i], halo_recv.at[i], at_sp(after))
        )

    def each_halo(do):
        for h in halos:
            do(h)

    pl.when(me < RING * RING - 1)(lambda: each_halo(lambda h: h.start()))

    def first(c, d):
        peer = mod8(y + d) if c == 0 else z + d
        own = kv.at[c, maj[c], maj[1 - c]]
        return remote(own, own, kv1_send.at[c, d], kv1_recv.at[c, maj[1 - c]], {axis_of[1 - c]: peer})

    def first_arrival(c, b):
        slot = kv.at[c, maj[c], b]
        return remote(slot, slot, kv1_send.at[c, 0], kv1_recv.at[c, b], {axis_of[1 - c]: b})

    for d in range(1, RING):
        first(0, d).start()

    right, left = {"fs": mod4(fx + 1)}, {"fs": mod4(fx - 1)}
    owns = [
        pltpu.make_async_copy(w1_ref, wbuf.at[0, fx], own_sem.at[0]),
        pltpu.make_async_copy(w2_ref, wbuf.at[1, fx], own_sem.at[1]),
    ]

    def weights(j, d):
        src = (w1_ref, w2_ref)[j]
        return remote(src, wbuf.at[j, fx], w_send.at[j, d], w_recv.at[j, d], (right, left)[d])

    def weights_arrival(j, d):
        slot = wbuf.at[j, mod4(fx - 1) if d == 0 else mod4(fx + 1)]
        return remote(slot, slot, w_send.at[j, d], w_recv.at[j, d], (right, left)[d])

    def passed_on(j):
        slot = wbuf.at[j, mod4(fx - 1) if j == 0 else mod4(fx + 1)]
        return remote(slot, slot, w_send.at[j, 2], w_recv.at[j, 2], (right, left)[j])

    def passed_arrival(j):
        slot = wbuf.at[j, mod4(fx + 2)]
        return remote(slot, slot, w_send.at[j, 2], w_recv.at[j, 2], (right, left)[j])

    for o in owns:
        o.start()
    for j in range(2):
        for d in range(2):
            weights(j, d).start()

    for d in range(1, RING):
        @pl.when(z + d < RING)
        def _():
            pl.semaphore_wait(ready.at[z + d], 1)
            first(1, d).start()

    ones = jnp.ones((16, ROWS), BF16)
    pair_query = lax.rem(lax.broadcasted_iota(jnp.int32, (HD, 2 * ROWS), 1), ROWS)
    pair_key = lax.broadcasted_iota(jnp.int32, (HD, 2 * ROWS), 0)
    lane_block = lane // 16

    def turned_gates(gates):
        f = jnp.concatenate([g.astype(F32) for g in gates], axis=0)
        if f.shape[0] < ROWS:
            f = jnp.concatenate([f, jnp.zeros((ROWS - f.shape[0], ROWS), F32)], axis=0)
        return f.T

    def scores(keys, gates, p, n):
        return dot(jnp.concatenate([keys, gates], axis=1), qs[p, n], NT)

    for c in range(2):
        own = kv.at[c, maj[c], maj[1 - c]]
        turned = turned_gates([own[ROWS:BLOCK]]).astype(BF16)
        vals = jnp.concatenate([own[HD:ROWS], ones], axis=0)
        for p in (2 * c, 2 * c + 1):
            s0 = scores(own[0:HD], turned[0:HD], p, 0)
            s1_ = scores(own[0:HD], turned[HD:ROWS], p, 1)
            s0 = jnp.where(pair_key <= pair_query, s0, NEG)
            s1_ = jnp.where(pair_key + HD <= pair_query, s1_, NEG)
            m = jnp.maximum(jnp.max(s0, axis=0, keepdims=True), jnp.max(s1_, axis=0, keepdims=True))
            probs = jnp.concatenate([jnp.exp(s0 - m), jnp.exp(s1_ - m)], axis=0).astype(BF16)
            m_sc[p] = jnp.broadcast_to(m, (8, 2 * ROWS))
            acc_sc[p] = dot(vals, probs)

    for copy in ins[7:]:
        copy.wait()

    @pl.when(me > 0)
    def _():
        each_halo(lambda h: h.wait_recv())

    opening = me > 0

    def filtered(rows, halo, taps):
        old = jnp.where(opening, halo[...].astype(F32), 0.0)
        padded = jnp.concatenate([old, rows[...].astype(F32)], axis=0)
        t = taps[...].astype(F32)
        total = t[0:1] * padded[13 : 13 + ROWS]
        for o in range(1, 4):
            total = total + t[o : o + 1] * padded[13 + o : 13 + o + ROWS]
        return silu(total).astype(BF16)

    xs_sc[...] = filtered(x_ref, hx, xtap_ref)
    wr = filtered(w_ref, hw, wtap_ref)
    rd = filtered(r_ref, hr, rtap_ref)
    rd_sc[...] = rd
    raw = step_ref[...]
    step = jnp.maximum(raw, 0.0) + jnp.log1p(jnp.exp(-jnp.abs(raw)))
    on_diagonal = sub8[:, 0:8] == lax.broadcasted_iota(jnp.int32, (8, 8), 1)
    rate = jnp.sum(jnp.where(on_diagonal, lane_ref[...], 0.0), axis=1, keepdims=True)
    cum = step * (-jnp.exp(rate)) + extra_ref[...]
    lane8 = lax.broadcasted_iota(jnp.int32, (8, ROWS), 1)
    for shift in (1, 2, 4, 8, 16, 32, 64):
        cum = cum + jnp.where(lane8 >= shift, pltpu.roll(cum, shift, 1), 0.0)
    end = cum[:, ROWS - 1 : ROWS]
    scale = jnp.exp(end - cum) * step
    wide[0:8] = cum
    wide[8:16] = scale
    wide[16:24] = jnp.broadcast_to(end, (8, ROWS))
    turned = wide[...].T
    inner = dot(rd, wr, NT)
    causal = lane <= sub
    for p in range(4):
        xp = xs_sc[:, 128 * p : 128 * p + 128]
        parts = []
        for e in range(2):
            h = 2 * p + e
            gap = jnp.where(causal, turned[:, h : h + 1] - cum[h : h + 1, :], NEG)
            mix = inner * (jnp.exp(gap) * step[h : h + 1, :])
            parts.append(dot(mix.astype(BF16), xp))
        xf = xp.astype(F32)
        skip = jnp.where(low, bypass_ref[:, 2 * p : 2 * p + 1], bypass_ref[:, 2 * p + 1 : 2 * p + 2])
        ms_sc[:, 128 * p : 128 * p + 128] = jnp.where(low, parts[0], parts[1]) + skip * xf
        ends = jnp.where(low, turned[:, 8 + 2 * p : 9 + 2 * p], turned[:, 9 + 2 * p : 10 + 2 * p])
        ecum_sc[:, 128 * p : 128 * p + 128] = jnp.exp(
            jnp.where(low, turned[:, 2 * p : 2 * p + 1], turned[:, 2 * p + 1 : 2 * p + 2])
        )
        state = dot((xf * ends).astype(BF16), wr, TN)
        for e in range(2):
            h = 2 * p + e
            msg[h, 0:HD] = state[HD * e : HD * e + HD].astype(BF16)

    def decay_rows(total):
        a, b, c3 = split3(total)
        return jnp.concatenate([jnp.where(four, a, c3), b], axis=0).astype(BF16)

    def decay_of(rows):
        f = rows.astype(F32)
        return (f[0:1] + f[8:9]) + f[4:5]

    for h in range(8):
        msg[h, HD:MSG] = decay_rows(jnp.broadcast_to(end[h : h + 1], (8, ROWS)))

    def around(src, dst, send, recv, axis, d):
        me_on = y if axis == "sp_1" else z
        peer = mod8(me_on + d)
        return remote(src(peer), dst.at[me_on], send.at[d], recv.at[RING - d], {axis: peer})

    def around_arrival(dst, send, recv, axis, d):
        me_on = y if axis == "sp_1" else z
        peer = mod8(me_on + d)
        slot = dst.at[peer]
        return remote(slot, slot, send.at[d], recv.at[d], {axis: peer})

    def up_total(d):
        return remote(tot, s2.at[z], s2_send.at[d], s2_recv.at[z], {"sp_0": z + d})

    s1_out = [around(lambda p: msg.at[p], s1, s1_send, s1_recv, "sp_1", d) for d in range(1, RING)]
    for o in s1_out:
        o.start()
    s1[y] = msg[y]

    def bundle(c, row, half):
        return kv.at[c, row, pl.ds(4 * half, 4)]

    def hop(c, d, k):
        away = -(k // 2) if d == 0 else k // 2
        half = (0 if d == 0 else 1) if k == 6 else k % 2
        slot = bundle(c, mod8(maj[c] + away), half)
        to = mod8(maj[c] + (1 if d == 0 else -1))
        return remote(slot, slot, kv_send.at[c, d, k], kv_recv.at[c, d, k], {axis_of[c]: to})

    def hop_arrival(c, d, k):
        away = -(k // 2) - 1 if d == 0 else k // 2 + 1
        half = (0 if d == 0 else 1) if k == 6 else k % 2
        slot = bundle(c, mod8(maj[c] + away), half)
        to = mod8(maj[c] + (1 if d == 0 else -1))
        return remote(slot, slot, kv_send.at[c, d, k], kv_recv.at[c, d, k], {axis_of[c]: to})

    def going(c, d, k):
        half = (0 if d == 0 else 1) if k == 6 else k % 2
        if c == 1:
            return z >= 4 * half
        if d == 0:
            return (z - k // 2 >= 0) & (z < last)
        return mod8(z + k // 2) <= 2 + half

    def coming(c, d, k):
        half = (0 if d == 0 else 1) if k == 6 else k % 2
        if c == 1:
            return z >= 4 * half
        if d == 0:
            return z - 1 - k // 2 >= 0
        return mod8(z + 1 + k // 2) <= 2 + half

    def send(c, d, k):
        pl.when(going(c, d, k))(lambda: hop(c, d, k).start())

    def attend(up, down, half_up, half_down):
        def one(c, carry):
            mine = jnp.where(c == 0, z, y)
            row_u, row_d = mod8(mine + up), mod8(mine + down)
            stride = jnp.where(c == 0, RING, 1)
            inner_stride = jnp.where(c == 0, 1, RING)
            lead_u = row_u * stride + 4 * half_up * inner_stride
            lead_d = row_d * stride + 4 * half_down * inner_stride

            @pl.when(jnp.minimum(lead_u, lead_d) < me)
            def _():
                spots = [(row_u, 4 * half_up + b) for b in range(4)]
                spots += [(row_d, 4 * half_down + b) for b in range(4)]
                leads = [lead_u + b * inner_stride for b in range(4)]
                leads += [lead_d + b * inner_stride for b in range(4)]
                turned = turned_gates([kv[c, r, b, ROWS:BLOCK] for r, b in spots])
                gates = []
                for n, lead in enumerate(leads):
                    off = jnp.where(lead < me, 0.0, NEG)
                    gates.append(jnp.where(lane_block == n, turned + off, 0.0).astype(BF16))
                for part in range(2):
                    at = range(4 * part, 4 * part + 4)
                    keys = jnp.concatenate([kv[(c,) + spots[n] + (slice(0, HD),)] for n in at], axis=0)
                    vals = [kv[(c,) + spots[n] + (slice(HD, ROWS),)] for n in at]
                    vals = jnp.concatenate(
                        [jnp.concatenate(vals, axis=1), jnp.concatenate([ones] * 4, axis=1)], axis=0
                    )
                    gates_0 = jnp.concatenate([gates[n][0:HD] for n in at], axis=0)
                    gates_1 = jnp.concatenate([gates[n][HD:ROWS] for n in at], axis=0)
                    for i in range(2):
                        p = 2 * c + i
                        s0 = scores(keys, gates_0, p, 0)
                        s1_ = scores(keys, gates_1, p, 1)
                        m_old = m_sc[p, 0:1]
                        m = jnp.max(jnp.maximum(s0, s1_), axis=0, keepdims=True)
                        m = jnp.maximum(m, m_old)
                        m_sc[p, 0:1] = m
                        e0, e1 = jnp.exp(s0 - m).astype(BF16), jnp.exp(s1_ - m).astype(BF16)
                        probs = []
                        for b in range(4):
                            probs += [e0[HD * b : HD * b + HD], e1[HD * b : HD * b + HD]]
                        probs = jnp.concatenate(probs, axis=0)
                        acc_sc[p] = acc_sc[p] * jnp.exp(m_old - m) + dot(vals, probs)

            return carry

        lax.fori_loop(0, 2, one, 0)

    for half in range(2):
        for c in range(2):
            for b in range(4 * half, 4 * half + 4):
                there = (b != y) if c == 0 else (b < z)
                pl.when(there)(lambda: first_arrival(c, b).wait_recv())
            for d in range(2):
                send(c, d, half)
    attend(0, 0, 0, 1)

    def stage(k):
        if k == 2:
            weights_arrival(0, 0).wait_recv()
            passed_on(0).start()
        if k == 1:
            for d in range(1, RING):
                around_arrival(s1, s1_send, s1_recv, "sp_1", d).wait_recv()
            run = jnp.zeros((HD, ROWS), F32)
            total = jnp.zeros((1, ROWS), F32)
            for j in range(RING):
                pre[j] = run
                cumpre[j] = jnp.broadcast_to(total, (8, ROWS))
                ld = decay_of(s1[j, HD:MSG])
                run = jnp.exp(ld) * run + s1[j, 0:HD].astype(F32)
                total = total + ld
            tot[0:HD] = run.astype(BF16)
            tot[HD:MSG] = decay_rows(jnp.broadcast_to(total, (8, ROWS)))
            for d in range(1, RING):
                pl.when(z + d < RING)(lambda: up_total(d).start())
        if k == 3:
            for j in range(RING - 1):
                slot = s2.at[j]
                come = remote(slot, slot, s2_send.at[0], s2_recv.at[j], {"sp_0": j})
                pl.when(j < z)(lambda: come.wait_recv())
            entering = jnp.zeros((HD, ROWS), F32)
            for j in range(RING - 1):
                later = jnp.exp(decay_of(s2[j, HD:MSG])) * entering + s2[j, 0:HD].astype(F32)
                entering = jnp.where(j < z, later, entering)
            for j in range(RING):
                back[j] = (pre[j] + jnp.exp(cumpre[j, 0:1]) * entering).astype(BF16)
            for d in range(1, RING):
                around(lambda p: back.at[p], carried, s3_send, s3_recv, "sp_1", d).start()
            carried[y] = back[y]
        if k == 5:
            weights_arrival(1, 1).wait_recv()
            passed_on(1).start()
        if k == 6:
            for d in range(1, RING):
                around_arrival(carried, s3_send, s3_recv, "sp_1", d).wait_recv()
            states = jnp.concatenate([carried[h] for h in range(8)], axis=0)
            u = dot(rd_sc[...], states, NT) * ecum_sc[...] + ms_sc[...]
            u = u * silu(gate_ref[...].astype(F32))
            stretch = lax.rsqrt(jnp.mean(u * u, axis=1, keepdims=True) + EPSILON)
            xs_sc[...] = (u * stretch * gain_ref[...]).astype(BF16)

    for k in range(7):
        for c in range(2):
            for d in range(2):
                pl.when(coming(c, d, k))(lambda: hop_arrival(c, d, k).wait_recv())
        for c in range(2):
            if k < 5:
                send(c, 0, k + 2)
            if k < 4:
                send(c, 1, k + 2)
            if k == 5:
                send(c, 1, 6)
        half_up = 0 if k == 6 else k % 2
        half_down = 1 if k == 6 else k % 2
        attend(-(k // 2) - 1, k // 2 + 1, half_up, half_down)
        stage(k)

    attended = []
    for p in range(4):
        acc = acc_sc[p]
        out = acc[0:HD] / acc[HD : HD + 1]
        out = jnp.concatenate([out[:, 0:ROWS], out[:, ROWS : 2 * ROWS]], axis=0)
        attended.append(out.T.astype(BF16))
    attended = jnp.concatenate(attended, axis=1)
    state_out = xs_sc[...]
    half_rows = ROWS // 2

    def across(n):
        return remote(give.at[n], take.at[n], tp_send.at[n], tp_recv.at[n], {"tp": 1 - tp})

    columns = (fx, mod4(fx - 1), mod4(fx + 1), mod4(fx + 2))
    for n, f in enumerate(columns):
        if n == 0:
            for o in owns:
                o.wait()
        elif n == 1:
            weights_arrival(1, 0).wait_recv()
        elif n == 2:
            weights_arrival(0, 1).wait_recv()
        else:
            passed_arrival(0).wait_recv()
            passed_arrival(1).wait_recv()
        merged = dot(state_out, wbuf[0, f]) + dot(attended, wbuf[1, f])
        top, bottom = merged[0:half_rows], merged[half_rows:ROWS]
        give[n] = jnp.where(tp == 0, bottom, top).astype(BF16)
        across(n).start()
        keep[n] = jnp.where(tp == 0, top, bottom)
    for n, f in enumerate(columns):
        across(n).wait_recv()
        out_ref[:, pl.ds(pl.multiple_of(512 * f, 512), 512)] = (keep[n] + take[n].astype(F32)).astype(BF16)

    for n in range(FS):
        across(n).wait_send()
    pl.when(me < RING * RING - 1)(lambda: each_halo(lambda h: h.wait_send()))
    for d in range(1, RING):
        first(0, d).wait_send()
        around(lambda p: msg.at[p], s1, s1_send, s1_recv, "sp_1", d).wait_send()
        around(lambda p: back.at[p], carried, s3_send, s3_recv, "sp_1", d).wait_send()

        @pl.when(z + d < RING)
        def _():
            first(1, d).wait_send()
            up_total(d).wait_send()
    for k in range(7):
        for c in range(2):
            for d in range(2):
                pl.when(going(c, d, k))(lambda: hop(c, d, k).wait_send())
    for j in range(2):
        for d in range(2):
            weights(j, d).wait_send()
        passed_on(j).wait_send()


def shards(
    state_head_inputs, state_write_vectors, state_read_vectors, state_output_gate,
    presoftplus_steps, extra_decay_log, lane_shrinkage_powers, bypass_coefficient_vector,
    feeder_smoothing_stencil, stored_smoothing_stencil, lookup_smoothing_stencil,
    bundled_rescaling_vector, queries, attention_keys, attention_values, forget_gate_cumsum,
    state_out_weight, attention_out_weight,
):
    vmem = pl.BlockSpec(memory_space=pltpu.VMEM)
    hbm = pl.BlockSpec(memory_space=pltpu.HBM)
    dma = pltpu.SemaphoreType.DMA
    out = pl.pallas_call(
        kernel,
        out_shape=jax.ShapeDtypeStruct((ROWS // 2, 512 * FS), BF16),
        in_specs=[hbm] * 18,
        out_specs=vmem,
        scratch_shapes=[
            pltpu.VMEM((ROWS, 512), BF16), pltpu.VMEM((ROWS, ROWS), BF16), pltpu.VMEM((ROWS, ROWS), BF16),
            pltpu.VMEM((ROWS, 512), BF16), pltpu.VMEM((8, ROWS), F32), pltpu.VMEM((8, ROWS), F32),
            pltpu.VMEM((1, 8), F32), pltpu.VMEM((1, 8), F32),
            pltpu.VMEM((4, 512), BF16), pltpu.VMEM((4, ROWS), BF16), pltpu.VMEM((4, ROWS), BF16),
            pltpu.VMEM((1, 512), F32), pltpu.VMEM((ROWS, 512), BF16), pltpu.VMEM((ROWS, ROWS), BF16),
            pltpu.VMEM((ROWS, ROWS), BF16), pltpu.VMEM((8, ROWS), F32),
            pltpu.VMEM((2, RING, RING, BLOCK, ROWS), BF16),
            pltpu.VMEM((4, 2, 2 * ROWS, 2 * ROWS), BF16),
            pltpu.VMEM((ROWS, ROWS), F32),
            pltpu.VMEM((16, 512), BF16),
            pltpu.VMEM((16, ROWS), BF16),
            pltpu.VMEM((16, ROWS), BF16),
            pltpu.VMEM((4, 8, 2 * ROWS), F32),
            pltpu.VMEM((4, HD + 16, 2 * ROWS), F32),
            pltpu.VMEM((RING, MSG, ROWS), BF16),
            pltpu.VMEM((RING, MSG, ROWS), BF16),
            pltpu.VMEM((MSG, ROWS), BF16),
            pltpu.VMEM((RING, MSG, ROWS), BF16),
            pltpu.VMEM((RING, HD, ROWS), F32),
            pltpu.VMEM((RING, 8, ROWS), F32),
            pltpu.VMEM((RING, HD, ROWS), BF16),
            pltpu.VMEM((RING, HD, ROWS), BF16),
            pltpu.VMEM((ROWS, 512), BF16),
            pltpu.VMEM((ROWS, 512), F32),
            pltpu.VMEM((ROWS, ROWS), BF16),
            pltpu.VMEM((ROWS, 512), F32),
            pltpu.VMEM((2, FS, 512, 512), BF16),
            pltpu.VMEM((FS, ROWS // 2, 512), BF16),
            pltpu.VMEM((FS, ROWS // 2, 512), BF16),
            pltpu.VMEM((FS, ROWS // 2, 512), F32),
            dma((2, RING)), dma((2, RING)),
            dma((2, 2, 7)), dma((2, 2, 7)),
            dma((RING,)), dma((RING,)), dma((RING,)), dma((RING,)), dma((RING,)), dma((RING,)),
            dma((2, 3)), dma((2, 3)), dma((2,)),
            dma((3,)), dma((3,)), dma((FS,)), dma((FS,)), dma((16,)),
            pltpu.SemaphoreType.REGULAR((RING,)),
        ],
        compiler_params=pltpu.CompilerParams(
            collective_id=0, has_side_effects=True, vmem_limit_bytes=60 * 1024 * 1024
        ),
        name="mixer",
    )(
        state_head_inputs[0], state_write_vectors[0], state_read_vectors[0], state_output_gate[0],
        presoftplus_steps[0], extra_decay_log[0],
        lane_shrinkage_powers.reshape(1, -1), bypass_coefficient_vector.reshape(1, -1),
        feeder_smoothing_stencil, stored_smoothing_stencil, lookup_smoothing_stencil,
        bundled_rescaling_vector.reshape(1, -1), queries[0], attention_keys[0], attention_values[0],
        forget_gate_cumsum[0].T, state_out_weight, attention_out_weight,
    )
    return out[None]


def solution(mesh):
    split = Mesh(
        mesh.devices.reshape(8, 8, mesh.shape["fs"], mesh.shape["tp"]), ("sp_0", "sp_1", "fs", "tp")
    )
    placed = (
        P("fs", SP, "tp"),
        P("fs", SP, "tp"),
        P("fs", SP, "tp"),
        P("fs", SP, "tp"),
        P("fs", "tp", SP),
        P("fs", "tp", SP),
        P("tp"),
        P("tp"),
        P(None, "tp"),
        P(None, "tp"),
        P(None, "tp"),
        P("tp"),
        P("fs", SP, "tp"),
        P("fs", SP, "tp"),
        P("fs", SP, "tp"),
        P("fs", SP, "tp"),
        P("tp", "fs"),
        P("tp", "fs"),
    )
    return jax.shard_map(
        shards, mesh=split, in_specs=placed, out_specs=P("fs", SP_TP, None), check_vma=False
    )
```

```python
import jax
import jax.numpy as jnp
from jax import lax
from jax.experimental import pallas as pl
from jax.experimental.pallas import tpu as pltpu
from jax.sharding import Mesh
from jax.sharding import PartitionSpec as P

SP = ("sp_0", "sp_1")
SP_TP = ("sp_0", "sp_1", "tp")
MESH = pl.DeviceIdType.MESH
BF16 = jnp.bfloat16
F32 = jnp.float32

RING = 8
FS = 4
ROWS = 128
HD = 64
BLOCK = ROWS + 16
MSG = HD + 16
EPSILON = 1e-06
NEG = -1e30

NT = (((1,), (1,)), ((), ()))
TN = (((0,), (0,)), ((), ()))


def mod8(i):
    return lax.rem(i + 2 * RING, RING)


def mod4(i):
    return lax.rem(i + 2 * FS, FS)


def dot(a, b, dims=None):
    if dims is None:
        return jnp.dot(a, b, preferred_element_type=F32)
    return lax.dot_general(a, b, dims, preferred_element_type=F32)


def silu(f):
    return f / (1.0 + jnp.exp(-f))


def split3(g):
    hi = g.astype(BF16).astype(F32)
    rest = g - hi
    mid = rest.astype(BF16).astype(F32)
    return hi, mid, rest - mid


def kernel(
    x_in, w_in, r_in, gate_in, step_in, extra_in, lane_in, bypass_in, xtap_in, wtap_in, rtap_in,
    gain_in, q_in, k_in, v_in, g_in, w1_ref, w2_ref,
    out_ref,
    x_ref, w_ref, r_ref, gate_ref, step_ref, extra_ref, lane_ref, bypass_ref, xtap_ref, wtap_ref, rtap_ref,
    gain_ref, q_ref, k_ref, v_ref, g_ref,
    kv, qs, wide, hx, hw, hr, m_sc, acc_sc, msg, s1, tot, s2, pre, cumpre, back, carried,
    xs_sc, ms_sc, rd_sc, ecum_sc, wbuf, give, take, keep, ob,
    kv1_send, kv1_recv, kv_send, kv_recv, s1_send, s1_recv, s2_send, s2_recv, s3_send, s3_recv,
    w_send, w_recv, own_sem, halo_send, halo_recv, tp_send, tp_recv, in_sem, out_sem, ready, ready_row,
):
    z, y = lax.axis_index("sp_0"), lax.axis_index("sp_1")
    fx, tp = lax.axis_index("fs"), lax.axis_index("tp")
    me = z * RING + y
    maj = (z, y)
    axis_of = ("sp_0", "sp_1")
    after = lax.rem(me + 1, RING * RING)
    last = RING - 1

    def at_sp(i):
        return {"sp_0": i // RING, "sp_1": lax.rem(i, RING)}

    def remote(src, dst, send, recv, where):
        return pltpu.make_async_remote_copy(
            src_ref=src, dst_ref=dst, send_sem=send, recv_sem=recv,
            device_id=where, device_id_type=MESH,
        )

    lane = lax.broadcasted_iota(jnp.int32, (ROWS, ROWS), 1)
    sub = lax.broadcasted_iota(jnp.int32, (ROWS, ROWS), 0)
    low = lane < HD
    sub8 = lax.broadcasted_iota(jnp.int32, (8, ROWS), 0)

    ins = [
        pltpu.make_async_copy(src, dst, in_sem.at[i])
        for i, (src, dst) in enumerate((
            (k_in, k_ref), (v_in, v_ref), (g_in, g_ref), (q_in, q_ref), (x_in, x_ref), (w_in, w_ref),
            (r_in, r_ref), (step_in, step_ref), (extra_in, extra_ref), (lane_in, lane_ref),
            (bypass_in, bypass_ref), (xtap_in, xtap_ref), (wtap_in, wtap_ref), (rtap_in, rtap_ref),
            (gate_in, gate_ref), (gain_in, gain_ref),
        ))
    ]
    for copy in ins:
        copy.start()

    def clear_row(row, carry):
        kv[0, row] = jnp.zeros((RING, BLOCK, ROWS), BF16)
        kv[1, y, row] = jnp.zeros((BLOCK, ROWS), BF16)
        return carry

    lax.fori_loop(z + 1, RING, clear_row, 0)

    @pl.when(z < 4)
    def _():
        kv[1, mod8(y + 4), 4:8] = jnp.zeros((4, BLOCK, ROWS), BF16)

    barrier = pltpu.get_barrier_semaphore()

    def greet(peer):
        pl.semaphore_signal(barrier, inc=1, device_id=peer, device_id_type=MESH)

    for peer in ({"fs": mod4(fx + 1)}, {"fs": mod4(fx - 1)}, {"tp": 1 - tp}):
        greet(peer)
    for d in range(1, RING):
        pl.when(z + d < RING)(lambda d=d: greet({"sp_0": z + d}))
        pl.when(y + d < RING)(lambda d=d: greet({"sp_1": y + d}))
    pl.when((y == 0) & (z > 0))(lambda: greet(at_sp(me - 1)))

    wide[...] = jnp.zeros_like(wide)
    for copy in ins[0:4]:
        copy.wait()
    kf, vt = k_ref[...].astype(F32), v_ref[...].astype(F32).T
    low64 = low[0:HD]
    key_rows = (
        jnp.where(low64, kf[0:HD], pltpu.roll(kf[HD:ROWS], HD, 1)),
        jnp.where(low64, pltpu.roll(kf[0:HD], HD, 1), kf[HD:ROWS]),
    )
    hi, mid, lo = split3(-g_ref[...])
    four = sub8 < 4
    gate_rows = (
        jnp.concatenate(
            [jnp.where(four, hi, pltpu.roll(lo, 4, 0)), jnp.where(four, mid, 0.0)], axis=0
        ),
        jnp.concatenate(
            [jnp.where(four, pltpu.roll(hi, 4, 0), lo), jnp.where(four, pltpu.roll(mid, 4, 0), 0.0)],
            axis=0,
        ),
    )
    for c in range(2):
        spot = (c, maj[c], maj[1 - c])
        kv[spot + (slice(0, HD),)] = key_rows[c].astype(BF16)
        kv[spot + (slice(HD, ROWS),)] = vt[HD * c : HD * c + HD].astype(BF16)
        kv[spot + (slice(ROWS, BLOCK),)] = gate_rows[c].astype(BF16)
    for h in range(8):
        p, e = h // 2, h % 2
        qf = q_ref[:, 128 * p : 128 * p + 128].astype(F32) * 0.125
        turn = pltpu.roll(qf, HD, 1)
        at = slice(ROWS * e, ROWS * e + ROWS)
        picks = jnp.where(lax.rem(lane, 4) == h % 4, 1.0, 0.0).astype(BF16)
        head, other = (qf, turn) if e == 0 else (turn, qf)
        qs[p, 0, at, 0:ROWS] = jnp.where(low, head, 0.0).astype(BF16)
        qs[p, 1, at, 0:ROWS] = jnp.where(low, 0.0, other).astype(BF16)
        for n in range(2):
            qs[p, n, at, ROWS : 2 * ROWS] = picks

    for copy in ins[4:7]:
        copy.wait()
    inner_row = (y < last) | (z == last)
    pl.semaphore_wait(barrier, 3 + z + y + jnp.where(inner_row, 0, 1))
    for d in range(1, RING):
        @pl.when(z - d >= 0)
        def _():
            pl.semaphore_signal(
                ready.at[z], inc=1, device_id={"sp_0": z - d}, device_id_type=MESH
            )

        @pl.when(y - d >= 0)
        def _():
            pl.semaphore_signal(
                ready_row.at[y], inc=1, device_id={"sp_1": y - d}, device_id_type=MESH
            )

    right, left = {"fs": mod4(fx + 1)}, {"fs": mod4(fx - 1)}
    owns = [
        pltpu.make_async_copy(w1_ref, wbuf.at[0, fx], own_sem.at[0]),
        pltpu.make_async_copy(w2_ref, wbuf.at[1, fx], own_sem.at[1]),
    ]

    def weights(j, d):
        src = (w1_ref, w2_ref)[j]
        return remote(src, wbuf.at[j, fx], w_send.at[j, d], w_recv.at[j, d], (right, left)[d])

    def weights_arrival(j, d):
        slot = wbuf.at[j, mod4(fx - 1) if d == 0 else mod4(fx + 1)]
        return remote(slot, slot, w_send.at[j, d], w_recv.at[j, d], (right, left)[d])

    def passed_on(j):
        slot = wbuf.at[j, mod4(fx - 1) if j == 0 else mod4(fx + 1)]
        return remote(slot, slot, w_send.at[j, 2], w_recv.at[j, 2], (right, left)[j])

    def passed_arrival(j):
        slot = wbuf.at[j, mod4(fx + 2)]
        return remote(slot, slot, w_send.at[j, 2], w_recv.at[j, 2], (right, left)[j])

    for o in owns:
        o.start()
    for j, d in ((0, 0), (1, 1), (1, 0), (0, 1)):
        weights(j, d).start()

    for d in range(1, RING):
        pl.when(y + d < RING)(lambda: pl.semaphore_wait(ready_row.at[y + d], 1))

    halos = []
    for i, (src, dst) in enumerate(((x_ref, hx), (w_ref, hw), (r_ref, hr))):
        halos.append(
            remote(src.at[pl.ds(ROWS - 16, 16)], dst, halo_send.at[i], halo_recv.at[i], at_sp(after))
        )

    def each_halo(do):
        for h in halos:
            do(h)

    pl.when(me < RING * RING - 1)(lambda: each_halo(lambda h: h.start()))

    def first(c, d):
        peer = mod8(y + d) if c == 0 else z + d
        own = kv.at[c, maj[c], maj[1 - c]]
        return remote(own, own, kv1_send.at[c, d], kv1_recv.at[c, maj[1 - c]], {axis_of[1 - c]: peer})

    def first_arrival(c, b):
        slot = kv.at[c, maj[c], b]
        return remote(slot, slot, kv1_send.at[c, 0], kv1_recv.at[c, b], {axis_of[1 - c]: b})

    for d in range(1, RING):
        first(0, d).start()

    for d in range(1, RING):
        @pl.when(z + d < RING)
        def _():
            pl.semaphore_wait(ready.at[z + d], 1)
            first(1, d).start()

    ones = jnp.ones((16, ROWS), BF16)
    pair_query = lax.rem(lax.broadcasted_iota(jnp.int32, (HD, 2 * ROWS), 1), ROWS)
    pair_key = lax.broadcasted_iota(jnp.int32, (HD, 2 * ROWS), 0)
    lane_block = lane // 16

    def turned_gates(gates):
        f = jnp.concatenate([g.astype(F32) for g in gates], axis=0)
        if f.shape[0] < ROWS:
            f = jnp.concatenate([f, jnp.zeros((ROWS - f.shape[0], ROWS), F32)], axis=0)
        return f.T

    def scores(keys, gates, p, n):
        return dot(jnp.concatenate([keys, gates], axis=1), qs[p, n], NT)

    for c in range(2):
        own = kv.at[c, maj[c], maj[1 - c]]
        turned = turned_gates([own[ROWS:BLOCK]]).astype(BF16)
        vals = jnp.concatenate([own[HD:ROWS], ones], axis=0)
        for p in (2 * c, 2 * c + 1):
            s0 = scores(own[0:HD], turned[0:HD], p, 0)
            s1_ = scores(own[0:HD], turned[HD:ROWS], p, 1)
            s0 = jnp.where(pair_key <= pair_query, s0, NEG)
            s1_ = jnp.where(pair_key + HD <= pair_query, s1_, NEG)
            m = jnp.maximum(jnp.max(s0, axis=0, keepdims=True), jnp.max(s1_, axis=0, keepdims=True))
            probs = jnp.concatenate([jnp.exp(s0 - m), jnp.exp(s1_ - m)], axis=0).astype(BF16)
            m_sc[p] = jnp.broadcast_to(m, (8, 2 * ROWS))
            acc_sc[p] = dot(vals, probs)

    for copy in ins[7:]:
        copy.wait()

    @pl.when(me > 0)
    def _():
        each_halo(lambda h: h.wait_recv())

    opening = me > 0

    def filtered(rows, halo, taps):
        old = jnp.where(opening, halo[...].astype(F32), 0.0)
        padded = jnp.concatenate([old, rows[...].astype(F32)], axis=0)
        t = taps[...].astype(F32)
        total = t[0:1] * padded[13 : 13 + ROWS]
        for o in range(1, 4):
            total = total + t[o : o + 1] * padded[13 + o : 13 + o + ROWS]
        return silu(total).astype(BF16)

    xs_sc[...] = filtered(x_ref, hx, xtap_ref)
    wr = filtered(w_ref, hw, wtap_ref)
    rd = filtered(r_ref, hr, rtap_ref)
    rd_sc[...] = rd
    raw = step_ref[...]
    step = jnp.maximum(raw, 0.0) + jnp.log1p(jnp.exp(-jnp.abs(raw)))
    on_diagonal = sub8[:, 0:8] == lax.broadcasted_iota(jnp.int32, (8, 8), 1)
    rate = jnp.sum(jnp.where(on_diagonal, lane_ref[...], 0.0), axis=1, keepdims=True)
    cum = step * (-jnp.exp(rate)) + extra_ref[...]
    lane8 = lax.broadcasted_iota(jnp.int32, (8, ROWS), 1)
    for shift in (1, 2, 4, 8, 16, 32, 64):
        cum = cum + jnp.where(lane8 >= shift, pltpu.roll(cum, shift, 1), 0.0)
    end = cum[:, ROWS - 1 : ROWS]
    scale = jnp.exp(end - cum) * step
    wide[0:8] = cum
    wide[8:16] = scale
    wide[16:24] = jnp.broadcast_to(end, (8, ROWS))
    turned = wide[...].T
    inner = dot(rd, wr, NT)
    causal = lane <= sub
    for p in range(4):
        xp = xs_sc[:, 128 * p : 128 * p + 128]
        parts = []
        for e in range(2):
            h = 2 * p + e
            gap = jnp.where(causal, turned[:, h : h + 1] - cum[h : h + 1, :], NEG)
            mix = inner * (jnp.exp(gap) * step[h : h + 1, :])
            parts.append(dot(mix.astype(BF16), xp))
        xf = xp.astype(F32)
        skip = jnp.where(low, bypass_ref[:, 2 * p : 2 * p + 1], bypass_ref[:, 2 * p + 1 : 2 * p + 2])
        ms_sc[:, 128 * p : 128 * p + 128] = jnp.where(low, parts[0], parts[1]) + skip * xf
        ends = jnp.where(low, turned[:, 8 + 2 * p : 9 + 2 * p], turned[:, 9 + 2 * p : 10 + 2 * p])
        ecum_sc[:, 128 * p : 128 * p + 128] = jnp.exp(
            jnp.where(low, turned[:, 2 * p : 2 * p + 1], turned[:, 2 * p + 1 : 2 * p + 2])
        )
        state = dot((xf * ends).astype(BF16), wr, TN)
        for e in range(2):
            h = 2 * p + e
            msg[h, 0:HD] = state[HD * e : HD * e + HD].astype(BF16)

    def decay_rows(total):
        a, b, c3 = split3(total)
        return jnp.concatenate([jnp.where(four, a, c3), b], axis=0).astype(BF16)

    def decay_of(rows):
        f = rows.astype(F32)
        return (f[0:1] + f[8:9]) + f[4:5]

    for h in range(8):
        msg[h, HD:MSG] = decay_rows(jnp.broadcast_to(end[h : h + 1], (8, ROWS)))

    def around(src, dst, send, recv, axis, d):
        me_on = y if axis == "sp_1" else z
        peer = mod8(me_on + d)
        return remote(src(peer), dst.at[me_on], send.at[d], recv.at[RING - d], {axis: peer})

    def around_arrival(dst, send, recv, axis, d):
        me_on = y if axis == "sp_1" else z
        peer = mod8(me_on + d)
        slot = dst.at[peer]
        return remote(slot, slot, send.at[d], recv.at[d], {axis: peer})

    def up_total(d):
        return remote(tot, s2.at[z], s2_send.at[d], s2_recv.at[z], {"sp_0": z + d})

    s1_out = [around(lambda p: msg.at[p], s1, s1_send, s1_recv, "sp_1", d) for d in range(1, RING)]
    for o in s1_out:
        o.start()
    s1[y] = msg[y]

    def bundle(c, row, half):
        return kv.at[c, row, pl.ds(4 * half, 4)]

    def hop(c, d, k):
        away = -(k // 2) if d == 0 else k // 2
        half = (0 if d == 0 else 1) if k == 6 else k % 2
        slot = bundle(c, mod8(maj[c] + away), half)
        to = mod8(maj[c] + (1 if d == 0 else -1))
        return remote(slot, slot, kv_send.at[c, d, k], kv_recv.at[c, d, k], {axis_of[c]: to})

    def hop_arrival(c, d, k):
        away = -(k // 2) - 1 if d == 0 else k // 2 + 1
        half = (0 if d == 0 else 1) if k == 6 else k % 2
        slot = bundle(c, mod8(maj[c] + away), half)
        to = mod8(maj[c] + (1 if d == 0 else -1))
        return remote(slot, slot, kv_send.at[c, d, k], kv_recv.at[c, d, k], {axis_of[c]: to})

    def going(c, d, k):
        half = (0 if d == 0 else 1) if k == 6 else k % 2
        if c == 1:
            return z >= 4 * half
        if d == 0:
            return (z - k // 2 >= 0) & (z < last)
        return mod8(z + k // 2) <= 2 + half

    def coming(c, d, k):
        half = (0 if d == 0 else 1) if k == 6 else k % 2
        if c == 1:
            return z >= 4 * half
        if d == 0:
            return z - 1 - k // 2 >= 0
        return mod8(z + 1 + k // 2) <= 2 + half

    def send(c, d, k):
        pl.when(going(c, d, k))(lambda: hop(c, d, k).start())

    def attend(head, up, down, half_up, half_down):
        def one(c, carry):
            mine = jnp.where(c == 0, z, y)
            row_u, row_d = mod8(mine + up), mod8(mine + down)
            stride = jnp.where(c == 0, RING, 1)
            inner_stride = jnp.where(c == 0, 1, RING)
            lead_u = row_u * stride + 4 * half_up * inner_stride
            lead_d = row_d * stride + 4 * half_down * inner_stride

            @pl.when(jnp.minimum(lead_u, lead_d) < me)
            def _():
                spots = [(row_u, 4 * half_up + b) for b in range(4)]
                spots += [(row_d, 4 * half_down + b) for b in range(4)]
                leads = [lead_u + b * inner_stride for b in range(4)]
                leads += [lead_d + b * inner_stride for b in range(4)]
                turned = turned_gates([kv[c, r, b, ROWS:BLOCK] for r, b in spots])
                gates = []
                for n, lead in enumerate(leads):
                    off = jnp.where(lead < me, 0.0, NEG)
                    gates.append(jnp.where(lane_block == n, turned + off, 0.0).astype(BF16))
                for part in range(1):
                    at = range(8)
                    keys = jnp.concatenate([kv[(c,) + spots[n] + (slice(0, HD),)] for n in at], axis=0)
                    vals = [kv[(c,) + spots[n] + (slice(HD, ROWS),)] for n in at]
                    vals = jnp.concatenate(
                        [jnp.concatenate(vals, axis=1), jnp.concatenate([ones] * len(at), axis=1)], axis=0
                    )
                    gates_0 = jnp.concatenate([gates[n][0:HD] for n in at], axis=0)
                    gates_1 = jnp.concatenate([gates[n][HD:ROWS] for n in at], axis=0)
                    for i in range(2):
                        p = 2 * c + i
                        s0 = scores(keys, gates_0, p, 0)
                        s1_ = scores(keys, gates_1, p, 1)
                        m_old = m_sc[p, 0:1]
                        m = jnp.max(jnp.maximum(s0, s1_), axis=0, keepdims=True)
                        m = jnp.maximum(m, m_old)
                        m_sc[p, 0:1] = m
                        e0, e1 = jnp.exp(s0 - m).astype(BF16), jnp.exp(s1_ - m).astype(BF16)
                        probs = []
                        for b in range(len(at)):
                            probs += [e0[HD * b : HD * b + HD], e1[HD * b : HD * b + HD]]
                        probs = jnp.concatenate(probs, axis=0)
                        acc_sc[p] = acc_sc[p] * jnp.exp(m_old - m) + dot(vals, probs)

            return carry

        one(head, 0)

    def arrive(c, half):
        for b in range(4 * half, 4 * half + 4):
            there = (b != y) if c == 0 else (b < z)
            pl.when(there)(lambda: first_arrival(c, b).wait_recv())
        for d in range(2):
            send(c, d, half)

    arrive(1, 0)
    arrive(1, 1)
    attend(1, 0, 0, 0, 1)
    arrive(0, 0)
    arrive(0, 1)
    attend(0, 0, 0, 0, 1)

    def stage(k):
        if k == 0:
            weights_arrival(0, 0).wait_recv()
            passed_on(0).start()
            weights_arrival(1, 1).wait_recv()
            passed_on(1).start()
        if k == -1:
            for d in range(1, RING):
                around_arrival(s1, s1_send, s1_recv, "sp_1", d).wait_recv()
            run = jnp.zeros((HD, ROWS), F32)
            total = jnp.zeros((1, ROWS), F32)
            for j in range(RING):
                pre[j] = run
                cumpre[j] = jnp.broadcast_to(total, (8, ROWS))
                ld = decay_of(s1[j, HD:MSG])
                run = jnp.exp(ld) * run + s1[j, 0:HD].astype(F32)
                total = total + ld
            tot[0:HD] = run.astype(BF16)
            tot[HD:MSG] = decay_rows(jnp.broadcast_to(total, (8, ROWS)))
            for d in range(1, RING):
                pl.when(z + d < RING)(lambda: up_total(d).start())
        if k == 2:
            for j in range(RING - 1):
                slot = s2.at[j]
                come = remote(slot, slot, s2_send.at[0], s2_recv.at[j], {"sp_0": j})
                pl.when(j < z)(lambda: come.wait_recv())
            entering = jnp.zeros((HD, ROWS), F32)
            for j in range(RING - 1):
                later = jnp.exp(decay_of(s2[j, HD:MSG])) * entering + s2[j, 0:HD].astype(F32)
                entering = jnp.where(j < z, later, entering)
            for j in range(RING):
                back[j] = (pre[j] + jnp.exp(cumpre[j, 0:1]) * entering).astype(BF16)
            for d in range(1, RING):
                around(lambda p: back.at[p], carried, s3_send, s3_recv, "sp_1", d).start()
            carried[y] = back[y]
        if k == 5:
            for d in range(1, RING):
                around_arrival(carried, s3_send, s3_recv, "sp_1", d).wait_recv()
            states = jnp.concatenate([carried[h] for h in range(8)], axis=0)
            u = dot(rd_sc[...], states, NT) * ecum_sc[...] + ms_sc[...]
            u = u * silu(gate_ref[...].astype(F32))
            stretch = lax.rsqrt(jnp.mean(u * u, axis=1, keepdims=True) + EPSILON)
            xs_sc[...] = (u * stretch * gain_ref[...]).astype(BF16)

    stage(-1)
    for k in range(7):
        half_up = 0 if k == 6 else k % 2
        half_down = 1 if k == 6 else k % 2
        for c in (1, 0):
            for d in range(2):
                pl.when(coming(c, d, k))(lambda: hop_arrival(c, d, k).wait_recv())
            if k < 5:
                send(c, 0, k + 2)
            if k < 4:
                send(c, 1, k + 2)
            if k == 5:
                send(c, 1, 6)
            attend(c, -(k // 2) - 1, k // 2 + 1, half_up, half_down)
        stage(k)

    attended = []
    for p in range(4):
        acc = acc_sc[p]
        out = acc[0:HD] / acc[HD : HD + 1]
        out = jnp.concatenate([out[:, 0:ROWS], out[:, ROWS : 2 * ROWS]], axis=0)
        attended.append(out.T.astype(BF16))
    attended = jnp.concatenate(attended, axis=1)
    state_out = xs_sc[...]
    half_rows = ROWS // 2

    def across(n):
        return remote(give.at[n], take.at[n], tp_send.at[n], tp_recv.at[n], {"tp": 1 - tp})

    def written(n, f):
        return pltpu.make_async_copy(
            ob.at[n], out_ref.at[:, pl.ds(pl.multiple_of(512 * f, 512), 512)], out_sem.at[n]
        )

    columns = (fx, mod4(fx - 1), mod4(fx + 1), mod4(fx + 2))
    for n, f in enumerate(columns):
        if n == 0:
            for o in owns:
                o.wait()
        elif n == 1:
            weights_arrival(1, 0).wait_recv()
        elif n == 2:
            weights_arrival(0, 1).wait_recv()
        else:
            passed_arrival(0).wait_recv()
            passed_arrival(1).wait_recv()
        merged = dot(state_out, wbuf[0, f]) + dot(attended, wbuf[1, f])
        top, bottom = merged[0:half_rows], merged[half_rows:ROWS]
        give[n] = jnp.where(tp == 0, bottom, top).astype(BF16)
        across(n).start()
        keep[n] = jnp.where(tp == 0, top, bottom)
    for n, f in enumerate(columns):
        across(n).wait_recv()
        ob[n] = (keep[n] + take[n].astype(F32)).astype(BF16)
        written(n, f).start()
    for n, f in enumerate(columns):
        written(n, f).wait()

    for n in range(FS):
        across(n).wait_send()
    pl.when(me < RING * RING - 1)(lambda: each_halo(lambda h: h.wait_send()))
    for d in range(1, RING):
        first(0, d).wait_send()
        around(lambda p: msg.at[p], s1, s1_send, s1_recv, "sp_1", d).wait_send()
        around(lambda p: back.at[p], carried, s3_send, s3_recv, "sp_1", d).wait_send()

        @pl.when(z + d < RING)
        def _():
            first(1, d).wait_send()
            up_total(d).wait_send()
    for k in range(7):
        for c in range(2):
            for d in range(2):
                pl.when(going(c, d, k))(lambda: hop(c, d, k).wait_send())
    for j in range(2):
        for d in range(2):
            weights(j, d).wait_send()
        passed_on(j).wait_send()


def shards(
    state_head_inputs, state_write_vectors, state_read_vectors, state_output_gate,
    presoftplus_steps, extra_decay_log, lane_shrinkage_powers, bypass_coefficient_vector,
    feeder_smoothing_stencil, stored_smoothing_stencil, lookup_smoothing_stencil,
    bundled_rescaling_vector, queries, attention_keys, attention_values, forget_gate_cumsum,
    state_out_weight, attention_out_weight,
):
    hbm = pl.BlockSpec(memory_space=pltpu.HBM)
    dma = pltpu.SemaphoreType.DMA
    out = pl.pallas_call(
        kernel,
        out_shape=jax.ShapeDtypeStruct((ROWS // 2, 512 * FS), BF16),
        in_specs=[hbm] * 18,
        out_specs=hbm,
        scratch_shapes=[
            pltpu.VMEM((ROWS, 512), BF16), pltpu.VMEM((ROWS, ROWS), BF16), pltpu.VMEM((ROWS, ROWS), BF16),
            pltpu.VMEM((ROWS, 512), BF16), pltpu.VMEM((8, ROWS), F32), pltpu.VMEM((8, ROWS), F32),
            pltpu.VMEM((1, 8), F32), pltpu.VMEM((1, 8), F32),
            pltpu.VMEM((4, 512), BF16), pltpu.VMEM((4, ROWS), BF16), pltpu.VMEM((4, ROWS), BF16),
            pltpu.VMEM((1, 512), F32), pltpu.VMEM((ROWS, 512), BF16), pltpu.VMEM((ROWS, ROWS), BF16),
            pltpu.VMEM((ROWS, ROWS), BF16), pltpu.VMEM((8, ROWS), F32),
            pltpu.VMEM((2, RING, RING, BLOCK, ROWS), BF16),
            pltpu.VMEM((4, 2, 2 * ROWS, 2 * ROWS), BF16),
            pltpu.VMEM((ROWS, ROWS), F32),
            pltpu.VMEM((16, 512), BF16),
            pltpu.VMEM((16, ROWS), BF16),
            pltpu.VMEM((16, ROWS), BF16),
            pltpu.VMEM((4, 8, 2 * ROWS), F32),
            pltpu.VMEM((4, HD + 16, 2 * ROWS), F32),
            pltpu.VMEM((RING, MSG, ROWS), BF16),
            pltpu.VMEM((RING, MSG, ROWS), BF16),
            pltpu.VMEM((MSG, ROWS), BF16),
            pltpu.VMEM((RING, MSG, ROWS), BF16),
            pltpu.VMEM((RING, HD, ROWS), F32),
            pltpu.VMEM((RING, 8, ROWS), F32),
            pltpu.VMEM((RING, HD, ROWS), BF16),
            pltpu.VMEM((RING, HD, ROWS), BF16),
            pltpu.VMEM((ROWS, 512), BF16),
            pltpu.VMEM((ROWS, 512), F32),
            pltpu.VMEM((ROWS, ROWS), BF16),
            pltpu.VMEM((ROWS, 512), F32),
            pltpu.VMEM((2, FS, 512, 512), BF16),
            pltpu.VMEM((FS, ROWS // 2, 512), BF16),
            pltpu.VMEM((FS, ROWS // 2, 512), BF16),
            pltpu.VMEM((FS, ROWS // 2, 512), F32),
            pltpu.VMEM((FS, ROWS // 2, 512), BF16),
            dma((2, RING)), dma((2, RING)),
            dma((2, 2, 7)), dma((2, 2, 7)),
            dma((RING,)), dma((RING,)), dma((RING,)), dma((RING,)), dma((RING,)), dma((RING,)),
            dma((2, 3)), dma((2, 3)), dma((2,)),
            dma((3,)), dma((3,)), dma((FS,)), dma((FS,)), dma((16,)), dma((FS,)),
            pltpu.SemaphoreType.REGULAR((RING,)), pltpu.SemaphoreType.REGULAR((RING,)),
        ],
        compiler_params=pltpu.CompilerParams(
            collective_id=0, has_side_effects=True, vmem_limit_bytes=60 * 1024 * 1024
        ),
        name="mixer",
    )(
        state_head_inputs[0], state_write_vectors[0], state_read_vectors[0], state_output_gate[0],
        presoftplus_steps[0], extra_decay_log[0],
        lane_shrinkage_powers.reshape(1, -1), bypass_coefficient_vector.reshape(1, -1),
        feeder_smoothing_stencil, stored_smoothing_stencil, lookup_smoothing_stencil,
        bundled_rescaling_vector.reshape(1, -1), queries[0], attention_keys[0], attention_values[0],
        forget_gate_cumsum[0].T, state_out_weight, attention_out_weight,
    )
    return out[None]


def solution(mesh):
    split = Mesh(
        mesh.devices.reshape(8, 8, mesh.shape["fs"], mesh.shape["tp"]), ("sp_0", "sp_1", "fs", "tp")
    )
    placed = (
        P("fs", SP, "tp"),
        P("fs", SP, "tp"),
        P("fs", SP, "tp"),
        P("fs", SP, "tp"),
        P("fs", "tp", SP),
        P("fs", "tp", SP),
        P("tp"),
        P("tp"),
        P(None, "tp"),
        P(None, "tp"),
        P(None, "tp"),
        P("tp"),
        P("fs", SP, "tp"),
        P("fs", SP, "tp"),
        P("fs", SP, "tp"),
        P("fs", SP, "tp"),
        P("tp", "fs"),
        P("tp", "fs"),
    )
    return jax.shard_map(
        shards, mesh=split, in_specs=placed, out_specs=P("fs", SP_TP, None), check_vma=False
    )
```

```python
import jax
import jax.numpy as jnp
from jax import lax
from jax.experimental import pallas as pl
from jax.experimental.pallas import tpu as pltpu
from jax.sharding import Mesh
from jax.sharding import PartitionSpec as P

SP = ("sp_0", "sp_1")
SP_TP = ("sp_0", "sp_1", "tp")
MESH = pl.DeviceIdType.MESH
BF16 = jnp.bfloat16
F32 = jnp.float32

RING = 8
FS = 4
ROWS = 128
HD = 64
BLOCK = ROWS + 16
MSG = HD + 16
EPSILON = 1e-06
NEG = -1e30

NT = (((1,), (1,)), ((), ()))
TN = (((0,), (0,)), ((), ()))


def mod8(i):
    return lax.rem(i + 2 * RING, RING)


def mod4(i):
    return lax.rem(i + 2 * FS, FS)


def dot(a, b, dims=None):
    if dims is None:
        return jnp.dot(a, b, preferred_element_type=F32)
    return lax.dot_general(a, b, dims, preferred_element_type=F32)


def silu(f):
    return f / (1.0 + jnp.exp(-f))


def split3(g):
    hi = g.astype(BF16).astype(F32)
    rest = g - hi
    mid = rest.astype(BF16).astype(F32)
    return hi, mid, rest - mid


def kernel(
    x_in, w_in, r_in, gate_in, step_in, extra_in, lane_in, bypass_in, xtap_in, wtap_in, rtap_in,
    gain_in, q_in, k_in, v_in, g_in, w1_ref, w2_ref,
    out_ref,
    x_ref, w_ref, r_ref, gate_ref, step_ref, extra_ref, lane_ref, bypass_ref, xtap_ref, wtap_ref, rtap_ref,
    gain_ref, q_ref, k_ref, v_ref, g_ref,
    kv, qs, wide, hx, hw, hr, m_sc, acc_sc, msg, s1, tot, s2, pre, cumpre, back, carried,
    xs_sc, ms_sc, rd_sc, ecum_sc, wbuf, give, take, keep, ob, early,
    kv1_send, kv1_recv, kv_send, kv_recv, s1_send, s1_recv, s2_send, s2_recv, s3_send, s3_recv,
    w_send, w_recv, own_sem, halo_send, halo_recv, tp_send, tp_recv, in_sem, out_sem, ready, ready_row,
):
    z, y = lax.axis_index("sp_0"), lax.axis_index("sp_1")
    fx, tp = lax.axis_index("fs"), lax.axis_index("tp")
    me = z * RING + y
    maj = (z, y)
    axis_of = ("sp_0", "sp_1")
    after = lax.rem(me + 1, RING * RING)
    last = RING - 1

    def at_sp(i):
        return {"sp_0": i // RING, "sp_1": lax.rem(i, RING)}

    def remote(src, dst, send, recv, where):
        return pltpu.make_async_remote_copy(
            src_ref=src, dst_ref=dst, send_sem=send, recv_sem=recv,
            device_id=where, device_id_type=MESH,
        )

    lane = lax.broadcasted_iota(jnp.int32, (ROWS, ROWS), 1)
    sub = lax.broadcasted_iota(jnp.int32, (ROWS, ROWS), 0)
    low = lane < HD
    sub8 = lax.broadcasted_iota(jnp.int32, (8, ROWS), 0)

    ins = [
        pltpu.make_async_copy(src, dst, in_sem.at[i])
        for i, (src, dst) in enumerate((
            (k_in, k_ref), (v_in, v_ref), (g_in, g_ref), (q_in, q_ref), (x_in, x_ref), (w_in, w_ref),
            (r_in, r_ref), (step_in, step_ref), (extra_in, extra_ref), (lane_in, lane_ref),
            (bypass_in, bypass_ref), (xtap_in, xtap_ref), (wtap_in, wtap_ref), (rtap_in, rtap_ref),
            (gate_in, gate_ref), (gain_in, gain_ref),
        ))
    ]
    for copy in ins:
        copy.start()

    def clear_row(row, carry):
        kv[0, row] = jnp.zeros((RING, BLOCK, ROWS), BF16)
        kv[1, y, row] = jnp.zeros((BLOCK, ROWS), BF16)
        return carry

    lax.fori_loop(z + 1, RING, clear_row, 0)

    @pl.when(z < 4)
    def _():
        kv[1, mod8(y + 4), 4:8] = jnp.zeros((4, BLOCK, ROWS), BF16)

    barrier = pltpu.get_barrier_semaphore()

    def greet(peer):
        pl.semaphore_signal(barrier, inc=1, device_id=peer, device_id_type=MESH)

    for peer in ({"fs": mod4(fx + 1)}, {"fs": mod4(fx - 1)}, {"tp": 1 - tp}):
        greet(peer)
    for d in range(1, RING):
        pl.when(z + d < RING)(lambda d=d: greet({"sp_0": z + d}))
        pl.when(y + d < RING)(lambda d=d: greet({"sp_1": y + d}))
    pl.when((y == 0) & (z > 0))(lambda: greet(at_sp(me - 1)))

    inner_row = (y < last) | (z == last)
    pl.semaphore_wait(barrier, 3 + z + y + jnp.where(inner_row, 0, 1))
    for d in range(1, RING):
        @pl.when(z - d >= 0)
        def _():
            pl.semaphore_signal(
                ready.at[z], inc=1, device_id={"sp_0": z - d}, device_id_type=MESH
            )

        @pl.when(y - d >= 0)
        def _():
            pl.semaphore_signal(
                ready_row.at[y], inc=1, device_id={"sp_1": y - d}, device_id_type=MESH
            )

    right, left = {"fs": mod4(fx + 1)}, {"fs": mod4(fx - 1)}
    owns = [
        pltpu.make_async_copy(w1_ref, wbuf.at[0, fx], own_sem.at[0]),
        pltpu.make_async_copy(w2_ref, wbuf.at[1, fx], own_sem.at[1]),
    ]

    def weights(j, d):
        src = (w1_ref, w2_ref)[j]
        return remote(src, wbuf.at[j, fx], w_send.at[j, d], w_recv.at[j, d], (right, left)[d])

    def weights_arrival(j, d):
        slot = wbuf.at[j, mod4(fx - 1) if d == 0 else mod4(fx + 1)]
        return remote(slot, slot, w_send.at[j, d], w_recv.at[j, d], (right, left)[d])

    def passed_on(j):
        slot = wbuf.at[j, mod4(fx - 1) if j == 0 else mod4(fx + 1)]
        return remote(slot, slot, w_send.at[j, 2], w_recv.at[j, 2], (right, left)[j])

    def passed_arrival(j):
        slot = wbuf.at[j, mod4(fx + 2)]
        return remote(slot, slot, w_send.at[j, 2], w_recv.at[j, 2], (right, left)[j])

    for o in owns:
        o.start()
    for j, d in ((0, 0), (1, 1), (1, 0), (0, 1)):
        weights(j, d).start()

    wide[...] = jnp.zeros_like(wide)
    for copy in ins[0:4]:
        copy.wait()
    kf, vt = k_ref[...].astype(F32), v_ref[...].astype(F32).T
    low64 = low[0:HD]
    key_rows = (
        jnp.where(low64, kf[0:HD], pltpu.roll(kf[HD:ROWS], HD, 1)),
        jnp.where(low64, pltpu.roll(kf[0:HD], HD, 1), kf[HD:ROWS]),
    )
    hi, mid, lo = split3(-g_ref[...])
    four = sub8 < 4
    gate_rows = (
        jnp.concatenate(
            [jnp.where(four, hi, pltpu.roll(lo, 4, 0)), jnp.where(four, mid, 0.0)], axis=0
        ),
        jnp.concatenate(
            [jnp.where(four, pltpu.roll(hi, 4, 0), lo), jnp.where(four, pltpu.roll(mid, 4, 0), 0.0)],
            axis=0,
        ),
    )
    for c in range(2):
        spot = (c, maj[c], maj[1 - c])
        kv[spot + (slice(0, HD),)] = key_rows[c].astype(BF16)
        kv[spot + (slice(HD, ROWS),)] = vt[HD * c : HD * c + HD].astype(BF16)
        kv[spot + (slice(ROWS, BLOCK),)] = gate_rows[c].astype(BF16)
    for h in range(8):
        p, e = h // 2, h % 2
        qf = q_ref[:, 128 * p : 128 * p + 128].astype(F32) * 0.125
        turn = pltpu.roll(qf, HD, 1)
        at = slice(ROWS * e, ROWS * e + ROWS)
        picks = jnp.where(lax.rem(lane, 4) == h % 4, 1.0, 0.0).astype(BF16)
        head, other = (qf, turn) if e == 0 else (turn, qf)
        qs[p, 0, at, 0:ROWS] = jnp.where(low, head, 0.0).astype(BF16)
        qs[p, 1, at, 0:ROWS] = jnp.where(low, 0.0, other).astype(BF16)
        for n in range(2):
            qs[p, n, at, ROWS : 2 * ROWS] = picks

    for copy in ins[4:7]:
        copy.wait()
    for d in range(1, RING):
        pl.when(y + d < RING)(lambda: pl.semaphore_wait(ready_row.at[y + d], 1))

    halos = []
    for i, (src, dst) in enumerate(((x_ref, hx), (w_ref, hw), (r_ref, hr))):
        halos.append(
            remote(src.at[pl.ds(ROWS - 16, 16)], dst, halo_send.at[i], halo_recv.at[i], at_sp(after))
        )

    def each_halo(do):
        for h in halos:
            do(h)

    pl.when(me < RING * RING - 1)(lambda: each_halo(lambda h: h.start()))

    def first(c, d):
        peer = mod8(y + d) if c == 0 else z + d
        own = kv.at[c, maj[c], maj[1 - c]]
        return remote(own, own, kv1_send.at[c, d], kv1_recv.at[c, maj[1 - c]], {axis_of[1 - c]: peer})

    def first_arrival(c, b):
        slot = kv.at[c, maj[c], b]
        return remote(slot, slot, kv1_send.at[c, 0], kv1_recv.at[c, b], {axis_of[1 - c]: b})

    def relayed(i):
        from_left = (i == 3) | ((i == 4) & (tp == 0))
        block = mod8(jnp.where(from_left, y - 2, y + 2))
        peer = mod8(y + 1) if i == 3 else mod8(y - 1) if i == 5 else mod8(jnp.where(from_left, y + 2, y - 2))
        slot = kv.at[0, z, block]
        return remote(slot, slot, kv1_send.at[0, i], kv1_recv.at[0, block], {"sp_1": peer})

    for d in (1, 7, 2, 6):
        first(0, d).start()

    for d in range(1, RING):
        @pl.when(z + d < RING)
        def _():
            pl.semaphore_wait(ready.at[z + d], 1)
            first(1, d).start()

    ones = jnp.ones((16, ROWS), BF16)
    pair_query = lax.rem(lax.broadcasted_iota(jnp.int32, (HD, 2 * ROWS), 1), ROWS)
    pair_key = lax.broadcasted_iota(jnp.int32, (HD, 2 * ROWS), 0)
    lane_block = lane // 16

    def turned_gates(gates):
        f = jnp.concatenate([g.astype(F32) for g in gates], axis=0)
        if f.shape[0] < ROWS:
            f = jnp.concatenate([f, jnp.zeros((ROWS - f.shape[0], ROWS), F32)], axis=0)
        return f.T

    def scores(keys, gates, p, n):
        return dot(jnp.concatenate([keys, gates], axis=1), qs[p, n], NT)

    for c in range(2):
        own = kv.at[c, maj[c], maj[1 - c]]
        turned = turned_gates([own[ROWS:BLOCK]]).astype(BF16)
        vals = jnp.concatenate([own[HD:ROWS], ones], axis=0)
        for p in (2 * c, 2 * c + 1):
            s0 = scores(own[0:HD], turned[0:HD], p, 0)
            s1_ = scores(own[0:HD], turned[HD:ROWS], p, 1)
            s0 = jnp.where(pair_key <= pair_query, s0, NEG)
            s1_ = jnp.where(pair_key + HD <= pair_query, s1_, NEG)
            m = jnp.maximum(jnp.max(s0, axis=0, keepdims=True), jnp.max(s1_, axis=0, keepdims=True))
            probs = jnp.concatenate([jnp.exp(s0 - m), jnp.exp(s1_ - m)], axis=0).astype(BF16)
            m_sc[p] = jnp.broadcast_to(m, (8, 2 * ROWS))
            acc_sc[p] = dot(vals, probs)

    for copy in ins[7:]:
        copy.wait()

    @pl.when(me > 0)
    def _():
        each_halo(lambda h: h.wait_recv())

    opening = me > 0

    def filtered(rows, halo, taps):
        old = jnp.where(opening, halo[...].astype(F32), 0.0)
        padded = jnp.concatenate([old, rows[...].astype(F32)], axis=0)
        t = taps[...].astype(F32)
        total = t[0:1] * padded[13 : 13 + ROWS]
        for o in range(1, 4):
            total = total + t[o : o + 1] * padded[13 + o : 13 + o + ROWS]
        return silu(total).astype(BF16)

    xs_sc[...] = filtered(x_ref, hx, xtap_ref)
    wr = filtered(w_ref, hw, wtap_ref)
    rd = filtered(r_ref, hr, rtap_ref)
    rd_sc[...] = rd
    raw = step_ref[...]
    step = jnp.maximum(raw, 0.0) + jnp.log1p(jnp.exp(-jnp.abs(raw)))
    on_diagonal = sub8[:, 0:8] == lax.broadcasted_iota(jnp.int32, (8, 8), 1)
    rate = jnp.sum(jnp.where(on_diagonal, lane_ref[...], 0.0), axis=1, keepdims=True)
    cum = step * (-jnp.exp(rate)) + extra_ref[...]
    lane8 = lax.broadcasted_iota(jnp.int32, (8, ROWS), 1)
    for shift in (1, 2, 4, 8, 16, 32, 64):
        cum = cum + jnp.where(lane8 >= shift, pltpu.roll(cum, shift, 1), 0.0)
    end = cum[:, ROWS - 1 : ROWS]
    scale = jnp.exp(end - cum) * step
    wide[0:8] = cum
    wide[8:16] = scale
    wide[16:24] = jnp.broadcast_to(end, (8, ROWS))
    turned = wide[...].T
    inner = dot(rd, wr, NT)
    causal = lane <= sub
    for p in range(4):
        xp = xs_sc[:, 128 * p : 128 * p + 128]
        parts = []
        for e in range(2):
            h = 2 * p + e
            gap = jnp.where(causal, turned[:, h : h + 1] - cum[h : h + 1, :], NEG)
            mix = inner * (jnp.exp(gap) * step[h : h + 1, :])
            parts.append(dot(mix.astype(BF16), xp))
        xf = xp.astype(F32)
        skip = jnp.where(low, bypass_ref[:, 2 * p : 2 * p + 1], bypass_ref[:, 2 * p + 1 : 2 * p + 2])
        ms_sc[:, 128 * p : 128 * p + 128] = jnp.where(low, parts[0], parts[1]) + skip * xf
        ends = jnp.where(low, turned[:, 8 + 2 * p : 9 + 2 * p], turned[:, 9 + 2 * p : 10 + 2 * p])
        ecum_sc[:, 128 * p : 128 * p + 128] = jnp.exp(
            jnp.where(low, turned[:, 2 * p : 2 * p + 1], turned[:, 2 * p + 1 : 2 * p + 2])
        )
        state = dot((xf * ends).astype(BF16), wr, TN)
        for e in range(2):
            h = 2 * p + e
            msg[h, 0:HD] = state[HD * e : HD * e + HD].astype(BF16)

    def decay_rows(total):
        a, b, c3 = split3(total)
        return jnp.concatenate([jnp.where(four, a, c3), b], axis=0).astype(BF16)

    def decay_of(rows):
        f = rows.astype(F32)
        return (f[0:1] + f[8:9]) + f[4:5]

    for h in range(8):
        msg[h, HD:MSG] = decay_rows(jnp.broadcast_to(end[h : h + 1], (8, ROWS)))

    def around(src, dst, send, recv, axis, d):
        me_on = y if axis == "sp_1" else z
        peer = mod8(me_on + d)
        return remote(src(peer), dst.at[me_on], send.at[d], recv.at[RING - d], {axis: peer})

    def around_arrival(dst, send, recv, axis, d):
        me_on = y if axis == "sp_1" else z
        peer = mod8(me_on + d)
        slot = dst.at[peer]
        return remote(slot, slot, send.at[d], recv.at[d], {axis: peer})

    def up_total(d):
        return remote(tot, s2.at[z], s2_send.at[d], s2_recv.at[z], {"sp_0": z + d})

    for d in (2, 6):
        first_arrival(0, mod8(y + d)).wait_recv()
    for i in (3, 5, 4):
        relayed(i).start()

    s1_out = [around(lambda p: msg.at[p], s1, s1_send, s1_recv, "sp_1", d) for d in range(1, RING)]
    for o in s1_out:
        o.start()
    s1[y] = msg[y]

    def bundle(c, row, half):
        return kv.at[c, row, pl.ds(4 * half, 4)]

    def hop(c, d, k):
        away = -(k // 2) if d == 0 else k // 2
        half = (0 if d == 0 else 1) if k == 6 else k % 2
        slot = bundle(c, mod8(maj[c] + away), half)
        to = mod8(maj[c] + (1 if d == 0 else -1))
        return remote(slot, slot, kv_send.at[c, d, k], kv_recv.at[c, d, k], {axis_of[c]: to})

    def hop_arrival(c, d, k):
        away = -(k // 2) - 1 if d == 0 else k // 2 + 1
        half = (0 if d == 0 else 1) if k == 6 else k % 2
        slot = bundle(c, mod8(maj[c] + away), half)
        to = mod8(maj[c] + (1 if d == 0 else -1))
        return remote(slot, slot, kv_send.at[c, d, k], kv_recv.at[c, d, k], {axis_of[c]: to})

    def going(c, d, k):
        half = (0 if d == 0 else 1) if k == 6 else k % 2
        if c == 1:
            return z >= 4 * half
        if d == 0:
            return (z - k // 2 >= 0) & (z < last)
        return mod8(z + k // 2) <= 2 + half

    def coming(c, d, k):
        half = (0 if d == 0 else 1) if k == 6 else k % 2
        if c == 1:
            return z >= 4 * half
        if d == 0:
            return z - 1 - k // 2 >= 0
        return mod8(z + 1 + k // 2) <= 2 + half

    def send(c, d, k):
        pl.when(going(c, d, k))(lambda: hop(c, d, k).start())

    def attend(head, up, down, half_up, half_down):
        def one(c, carry):
            mine = jnp.where(c == 0, z, y)
            row_u, row_d = mod8(mine + up), mod8(mine + down)
            stride = jnp.where(c == 0, RING, 1)
            inner_stride = jnp.where(c == 0, 1, RING)
            lead_u = row_u * stride + 4 * half_up * inner_stride
            lead_d = row_d * stride + 4 * half_down * inner_stride

            @pl.when(jnp.minimum(lead_u, lead_d) < me)
            def _():
                spots = [(row_u, 4 * half_up + b) for b in range(4)]
                spots += [(row_d, 4 * half_down + b) for b in range(4)]
                leads = [lead_u + b * inner_stride for b in range(4)]
                leads += [lead_d + b * inner_stride for b in range(4)]
                turned = turned_gates([kv[c, r, b, ROWS:BLOCK] for r, b in spots])
                gates = []
                for n, lead in enumerate(leads):
                    off = jnp.where(lead < me, 0.0, NEG)
                    gates.append(jnp.where(lane_block == n, turned + off, 0.0).astype(BF16))
                for part in range(1):
                    at = range(8)
                    keys = jnp.concatenate([kv[(c,) + spots[n] + (slice(0, HD),)] for n in at], axis=0)
                    vals = [kv[(c,) + spots[n] + (slice(HD, ROWS),)] for n in at]
                    vals = jnp.concatenate(
                        [jnp.concatenate(vals, axis=1), jnp.concatenate([ones] * len(at), axis=1)], axis=0
                    )
                    gates_0 = jnp.concatenate([gates[n][0:HD] for n in at], axis=0)
                    gates_1 = jnp.concatenate([gates[n][HD:ROWS] for n in at], axis=0)
                    for i in range(2):
                        p = 2 * c + i
                        s0 = scores(keys, gates_0, p, 0)
                        s1_ = scores(keys, gates_1, p, 1)
                        m_old = m_sc[p, 0:1]
                        m = jnp.max(jnp.maximum(s0, s1_), axis=0, keepdims=True)
                        m = jnp.maximum(m, m_old)
                        m_sc[p, 0:1] = m
                        e0, e1 = jnp.exp(s0 - m).astype(BF16), jnp.exp(s1_ - m).astype(BF16)
                        probs = []
                        for b in range(len(at)):
                            probs += [e0[HD * b : HD * b + HD], e1[HD * b : HD * b + HD]]
                        probs = jnp.concatenate(probs, axis=0)
                        acc_sc[p] = acc_sc[p] * jnp.exp(m_old - m) + dot(vals, probs)

            return carry

        one(head, 0)

    def arrive(c, half):
        for b in range(4 * half, 4 * half + 4):
            there = (b != y) & (b != mod8(y + 2)) & (b != mod8(y - 2)) if c == 0 else (b < z)
            pl.when(there)(lambda: first_arrival(c, b).wait_recv())
        for d in range(2):
            send(c, d, half)

    arrive(1, 0)
    arrive(1, 1)
    attend(1, 0, 0, 0, 1)
    arrive(0, 0)
    arrive(0, 1)
    attend(0, 0, 0, 0, 1)

    def stage(k):
        if k == 0:
            weights_arrival(0, 0).wait_recv()
            passed_on(0).start()
            weights_arrival(1, 1).wait_recv()
            passed_on(1).start()
        if k == 0:
            for d in range(1, RING):
                around_arrival(s1, s1_send, s1_recv, "sp_1", d).wait_recv()
            run = jnp.zeros((HD, ROWS), F32)
            total = jnp.zeros((1, ROWS), F32)
            for j in range(RING):
                pre[j] = run
                cumpre[j] = jnp.broadcast_to(total, (8, ROWS))
                ld = decay_of(s1[j, HD:MSG])
                run = jnp.exp(ld) * run + s1[j, 0:HD].astype(F32)
                total = total + ld
            tot[0:HD] = run.astype(BF16)
            tot[HD:MSG] = decay_rows(jnp.broadcast_to(total, (8, ROWS)))
            for d in range(1, RING):
                pl.when(z + d < RING)(lambda: up_total(d).start())
        if k == 2:
            for j in range(RING - 1):
                slot = s2.at[j]
                come = remote(slot, slot, s2_send.at[0], s2_recv.at[j], {"sp_0": j})
                pl.when(j < z)(lambda: come.wait_recv())
            entering = jnp.zeros((HD, ROWS), F32)
            for j in range(RING - 1):
                later = jnp.exp(decay_of(s2[j, HD:MSG])) * entering + s2[j, 0:HD].astype(F32)
                entering = jnp.where(j < z, later, entering)
            for j in range(RING):
                back[j] = (pre[j] + jnp.exp(cumpre[j, 0:1]) * entering).astype(BF16)
            for d in range(1, RING):
                around(lambda p: back.at[p], carried, s3_send, s3_recv, "sp_1", d).start()
            carried[y] = back[y]
        if k == 5:
            for d in range(1, RING):
                around_arrival(carried, s3_send, s3_recv, "sp_1", d).wait_recv()
            states = jnp.concatenate([carried[h] for h in range(8)], axis=0)
            u = dot(rd_sc[...], states, NT) * ecum_sc[...] + ms_sc[...]
            u = u * silu(gate_ref[...].astype(F32))
            stretch = lax.rsqrt(jnp.mean(u * u, axis=1, keepdims=True) + EPSILON)
            xs_sc[...] = (u * stretch * gain_ref[...]).astype(BF16)
            for o in owns:
                o.wait()
            weights_arrival(0, 1).wait_recv()
            for n, f in enumerate((fx, mod4(fx - 1), mod4(fx + 1))):
                early[n] = dot(xs_sc[...], wbuf[0, f])

    for k in range(7):
        half_up = 0 if k == 6 else k % 2
        half_down = 1 if k == 6 else k % 2
        for c in (1, 0):
            for d in range(2):
                pl.when(coming(c, d, k))(lambda: hop_arrival(c, d, k).wait_recv())
            if k < 5:
                send(c, 0, k + 2)
            if k < 4:
                send(c, 1, k + 2)
            if k == 5:
                send(c, 1, 6)
            attend(c, -(k // 2) - 1, k // 2 + 1, half_up, half_down)
        stage(k)

    attended = []
    for p in range(4):
        acc = acc_sc[p]
        out = acc[0:HD] / acc[HD : HD + 1]
        out = jnp.concatenate([out[:, 0:ROWS], out[:, ROWS : 2 * ROWS]], axis=0)
        attended.append(out.T.astype(BF16))
    attended = jnp.concatenate(attended, axis=1)
    state_out = xs_sc[...]
    half_rows = ROWS // 2

    def across(n):
        return remote(give.at[n], take.at[n], tp_send.at[n], tp_recv.at[n], {"tp": 1 - tp})

    def written(n, f):
        return pltpu.make_async_copy(
            ob.at[n], out_ref.at[:, pl.ds(pl.multiple_of(512 * f, 512), 512)], out_sem.at[n]
        )

    columns = (fx, mod4(fx - 1), mod4(fx + 1), mod4(fx + 2))
    for n, f in enumerate(columns):
        if n == 1:
            weights_arrival(1, 0).wait_recv()
        if n == 3:
            passed_arrival(0).wait_recv()
            passed_arrival(1).wait_recv()
        merged = (early[n] if n < 3 else dot(state_out, wbuf[0, f])) + dot(attended, wbuf[1, f])
        top, bottom = merged[0:half_rows], merged[half_rows:ROWS]
        give[n] = jnp.where(tp == 0, bottom, top).astype(BF16)
        across(n).start()
        keep[n] = jnp.where(tp == 0, top, bottom)
    pl.when(me < RING * RING - 1)(lambda: each_halo(lambda h: h.wait_send()))
    for d in range(1, RING):
        (first(0, d) if d in (1, 2, 6, 7) else relayed(d)).wait_send()
        around(lambda p: msg.at[p], s1, s1_send, s1_recv, "sp_1", d).wait_send()
        around(lambda p: back.at[p], carried, s3_send, s3_recv, "sp_1", d).wait_send()

        @pl.when(z + d < RING)
        def _():
            first(1, d).wait_send()
            up_total(d).wait_send()
    for k in range(7):
        for c in range(2):
            for d in range(2):
                pl.when(going(c, d, k))(lambda: hop(c, d, k).wait_send())
    for j in range(2):
        for d in range(2):
            weights(j, d).wait_send()
        passed_on(j).wait_send()

    for n, f in enumerate(columns):
        across(n).wait_recv()
        ob[n] = (keep[n] + take[n].astype(F32)).astype(BF16)
        written(n, f).start()
    for n, f in enumerate(columns):
        written(n, f).wait()
    for n in range(FS):
        across(n).wait_send()


def shards(
    state_head_inputs, state_write_vectors, state_read_vectors, state_output_gate,
    presoftplus_steps, extra_decay_log, lane_shrinkage_powers, bypass_coefficient_vector,
    feeder_smoothing_stencil, stored_smoothing_stencil, lookup_smoothing_stencil,
    bundled_rescaling_vector, queries, attention_keys, attention_values, forget_gate_cumsum,
    state_out_weight, attention_out_weight,
):
    hbm = pl.BlockSpec(memory_space=pltpu.HBM)
    dma = pltpu.SemaphoreType.DMA
    out = pl.pallas_call(
        kernel,
        out_shape=jax.ShapeDtypeStruct((ROWS // 2, 512 * FS), BF16),
        in_specs=[hbm] * 18,
        out_specs=hbm,
        scratch_shapes=[
            pltpu.VMEM((ROWS, 512), BF16), pltpu.VMEM((ROWS, ROWS), BF16), pltpu.VMEM((ROWS, ROWS), BF16),
            pltpu.VMEM((ROWS, 512), BF16), pltpu.VMEM((8, ROWS), F32), pltpu.VMEM((8, ROWS), F32),
            pltpu.VMEM((1, 8), F32), pltpu.VMEM((1, 8), F32),
            pltpu.VMEM((4, 512), BF16), pltpu.VMEM((4, ROWS), BF16), pltpu.VMEM((4, ROWS), BF16),
            pltpu.VMEM((1, 512), F32), pltpu.VMEM((ROWS, 512), BF16), pltpu.VMEM((ROWS, ROWS), BF16),
            pltpu.VMEM((ROWS, ROWS), BF16), pltpu.VMEM((8, ROWS), F32),
            pltpu.VMEM((2, RING, RING, BLOCK, ROWS), BF16),
            pltpu.VMEM((4, 2, 2 * ROWS, 2 * ROWS), BF16),
            pltpu.VMEM((ROWS, ROWS), F32),
            pltpu.VMEM((16, 512), BF16),
            pltpu.VMEM((16, ROWS), BF16),
            pltpu.VMEM((16, ROWS), BF16),
            pltpu.VMEM((4, 8, 2 * ROWS), F32),
            pltpu.VMEM((4, HD + 16, 2 * ROWS), F32),
            pltpu.VMEM((RING, MSG, ROWS), BF16),
            pltpu.VMEM((RING, MSG, ROWS), BF16),
            pltpu.VMEM((MSG, ROWS), BF16),
            pltpu.VMEM((RING, MSG, ROWS), BF16),
            pltpu.VMEM((RING, HD, ROWS), F32),
            pltpu.VMEM((RING, 8, ROWS), F32),
            pltpu.VMEM((RING, HD, ROWS), BF16),
            pltpu.VMEM((RING, HD, ROWS), BF16),
            pltpu.VMEM((ROWS, 512), BF16),
            pltpu.VMEM((ROWS, 512), F32),
            pltpu.VMEM((ROWS, ROWS), BF16),
            pltpu.VMEM((ROWS, 512), F32),
            pltpu.VMEM((2, FS, 512, 512), BF16),
            pltpu.VMEM((FS, ROWS // 2, 512), BF16),
            pltpu.VMEM((FS, ROWS // 2, 512), BF16),
            pltpu.VMEM((FS, ROWS // 2, 512), F32),
            pltpu.VMEM((FS, ROWS // 2, 512), BF16),
            pltpu.VMEM((3, ROWS, 512), F32),
            dma((2, RING)), dma((2, RING)),
            dma((2, 2, 7)), dma((2, 2, 7)),
            dma((RING,)), dma((RING,)), dma((RING,)), dma((RING,)), dma((RING,)), dma((RING,)),
            dma((2, 3)), dma((2, 3)), dma((2,)),
            dma((3,)), dma((3,)), dma((FS,)), dma((FS,)), dma((16,)), dma((FS,)),
            pltpu.SemaphoreType.REGULAR((RING,)), pltpu.SemaphoreType.REGULAR((RING,)),
        ],
        compiler_params=pltpu.CompilerParams(
            collective_id=0, has_side_effects=True, vmem_limit_bytes=60 * 1024 * 1024
        ),
        name="mixer",
    )(
        state_head_inputs[0], state_write_vectors[0], state_read_vectors[0], state_output_gate[0],
        presoftplus_steps[0], extra_decay_log[0],
        lane_shrinkage_powers.reshape(1, -1), bypass_coefficient_vector.reshape(1, -1),
        feeder_smoothing_stencil, stored_smoothing_stencil, lookup_smoothing_stencil,
        bundled_rescaling_vector.reshape(1, -1), queries[0], attention_keys[0], attention_values[0],
        forget_gate_cumsum[0].T, state_out_weight, attention_out_weight,
    )
    return out[None]


def solution(mesh):
    split = Mesh(
        mesh.devices.reshape(8, 8, mesh.shape["fs"], mesh.shape["tp"]), ("sp_0", "sp_1", "fs", "tp")
    )
    placed = (
        P("fs", SP, "tp"),
        P("fs", SP, "tp"),
        P("fs", SP, "tp"),
        P("fs", SP, "tp"),
        P("fs", "tp", SP),
        P("fs", "tp", SP),
        P("tp"),
        P("tp"),
        P(None, "tp"),
        P(None, "tp"),
        P(None, "tp"),
        P("tp"),
        P("fs", SP, "tp"),
        P("fs", SP, "tp"),
        P("fs", SP, "tp"),
        P("fs", SP, "tp"),
        P("tp", "fs"),
        P("tp", "fs"),
    )
    return jax.shard_map(
        shards, mesh=split, in_specs=placed, out_specs=P("fs", SP_TP, None), check_vma=False
    )
```

```python
import jax
import jax.numpy as jnp
from jax import lax
from jax.experimental import pallas as pl
from jax.experimental.pallas import tpu as pltpu
from jax.sharding import Mesh
from jax.sharding import PartitionSpec as P

SP = ("sp_0", "sp_1")
SP_TP = ("sp_0", "sp_1", "tp")
MESH = pl.DeviceIdType.MESH
BF16 = jnp.bfloat16
F32 = jnp.float32

RING = 8
FS = 4
ROWS = 128
HD = 64
BLOCK = ROWS + 16
MSG = HD + 16
EPSILON = 1e-06
NEG = -1e30

NT = (((1,), (1,)), ((), ()))
TN = (((0,), (0,)), ((), ()))


def mod8(i):
    return lax.rem(i + 2 * RING, RING)


def mod4(i):
    return lax.rem(i + 2 * FS, FS)


def dot(a, b, dims=None):
    if dims is None:
        return jnp.dot(a, b, preferred_element_type=F32)
    return lax.dot_general(a, b, dims, preferred_element_type=F32)


def silu(f):
    return f / (1.0 + jnp.exp(-f))


def split3(g):
    hi = g.astype(BF16).astype(F32)
    rest = g - hi
    mid = rest.astype(BF16).astype(F32)
    return hi, mid, rest - mid


def kernel(
    x_in, w_in, r_in, gate_in, step_in, extra_in, lane_in, bypass_in, xtap_in, wtap_in, rtap_in,
    gain_in, q_in, k_in, v_in, g_in, w1_ref, w2_ref,
    keep_out, take_out,
    x_ref, w_ref, r_ref, gate_ref, step_ref, extra_ref, lane_ref, bypass_ref, xtap_ref, wtap_ref, rtap_ref,
    gain_ref, q_ref, k_ref, v_ref, g_ref,
    kv, qs, wide, hx, hw, hr, m_sc, acc_sc, msg, s1, tot, s2, pre, cumpre, back, carried,
    xs_sc, ms_sc, rd_sc, ecum_sc, wbuf, give, keep, early,
    kv1_send, kv1_recv, kv_send, kv_recv, s1_send, s1_recv, s2_send, s2_recv, s3_send, s3_recv,
    w_send, w_recv, own_sem, halo_send, halo_recv, tp_send, tp_recv, in_sem, out_sem, ready, ready_row,
):
    z, y = lax.axis_index("sp_0"), lax.axis_index("sp_1")
    fx, tp = lax.axis_index("fs"), lax.axis_index("tp")
    me = z * RING + y
    maj = (z, y)
    axis_of = ("sp_0", "sp_1")
    after = lax.rem(me + 1, RING * RING)
    last = RING - 1

    def at_sp(i):
        return {"sp_0": i // RING, "sp_1": lax.rem(i, RING)}

    def remote(src, dst, send, recv, where):
        return pltpu.make_async_remote_copy(
            src_ref=src, dst_ref=dst, send_sem=send, recv_sem=recv,
            device_id=where, device_id_type=MESH,
        )

    lane = lax.broadcasted_iota(jnp.int32, (ROWS, ROWS), 1)
    sub = lax.broadcasted_iota(jnp.int32, (ROWS, ROWS), 0)
    low = lane < HD
    sub8 = lax.broadcasted_iota(jnp.int32, (8, ROWS), 0)

    ins = [
        pltpu.make_async_copy(src, dst, in_sem.at[i])
        for i, (src, dst) in enumerate((
            (k_in, k_ref), (v_in, v_ref), (g_in, g_ref), (q_in, q_ref), (x_in, x_ref), (w_in, w_ref),
            (r_in, r_ref), (step_in, step_ref), (extra_in, extra_ref), (lane_in, lane_ref),
            (bypass_in, bypass_ref), (xtap_in, xtap_ref), (wtap_in, wtap_ref), (rtap_in, rtap_ref),
            (gate_in, gate_ref), (gain_in, gain_ref),
        ))
    ]
    for copy in ins:
        copy.start()

    def clear_row(row, carry):
        kv[0, row] = jnp.zeros((RING, BLOCK, ROWS), BF16)
        kv[1, y, row] = jnp.zeros((BLOCK, ROWS), BF16)
        return carry

    lax.fori_loop(z + 1, RING, clear_row, 0)

    @pl.when(z < 4)
    def _():
        kv[1, mod8(y + 4), 4:8] = jnp.zeros((4, BLOCK, ROWS), BF16)

    barrier = pltpu.get_barrier_semaphore()

    def greet(peer):
        pl.semaphore_signal(barrier, inc=1, device_id=peer, device_id_type=MESH)

    for peer in ({"fs": mod4(fx + 1)}, {"fs": mod4(fx - 1)}, {"tp": 1 - tp}):
        greet(peer)
    for d in range(1, RING):
        pl.when(z + d < RING)(lambda d=d: greet({"sp_0": z + d}))
        pl.when(y + d < RING)(lambda d=d: greet({"sp_1": y + d}))
    pl.when((y == 0) & (z > 0))(lambda: greet(at_sp(me - 1)))

    inner_row = (y < last) | (z == last)
    pl.semaphore_wait(barrier, 3 + z + y + jnp.where(inner_row, 0, 1))
    for d in range(1, RING):
        @pl.when(z - d >= 0)
        def _():
            pl.semaphore_signal(
                ready.at[z], inc=1, device_id={"sp_0": z - d}, device_id_type=MESH
            )

        @pl.when(y - d >= 0)
        def _():
            pl.semaphore_signal(
                ready_row.at[y], inc=1, device_id={"sp_1": y - d}, device_id_type=MESH
            )

    right, left = {"fs": mod4(fx + 1)}, {"fs": mod4(fx - 1)}
    owns = [
        pltpu.make_async_copy(w1_ref, wbuf.at[0, fx], own_sem.at[0]),
        pltpu.make_async_copy(w2_ref, wbuf.at[1, fx], own_sem.at[1]),
    ]

    def weights(j, d):
        src = (w1_ref, w2_ref)[j]
        return remote(src, wbuf.at[j, fx], w_send.at[j, d], w_recv.at[j, d], (right, left)[d])

    def weights_arrival(j, d):
        slot = wbuf.at[j, mod4(fx - 1) if d == 0 else mod4(fx + 1)]
        return remote(slot, slot, w_send.at[j, d], w_recv.at[j, d], (right, left)[d])

    def passed_on(j):
        slot = wbuf.at[j, mod4(fx - 1) if j == 0 else mod4(fx + 1)]
        return remote(slot, slot, w_send.at[j, 2], w_recv.at[j, 2], (right, left)[j])

    def passed_arrival(j):
        slot = wbuf.at[j, mod4(fx + 2)]
        return remote(slot, slot, w_send.at[j, 2], w_recv.at[j, 2], (right, left)[j])

    for o in owns:
        o.start()
    for j, d in ((0, 0), (1, 1), (1, 0), (0, 1)):
        weights(j, d).start()

    wide[...] = jnp.zeros_like(wide)
    for copy in ins[0:4]:
        copy.wait()
    kf, vt = k_ref[...].astype(F32), v_ref[...].astype(F32).T
    low64 = low[0:HD]
    key_rows = (
        jnp.where(low64, kf[0:HD], pltpu.roll(kf[HD:ROWS], HD, 1)),
        jnp.where(low64, pltpu.roll(kf[0:HD], HD, 1), kf[HD:ROWS]),
    )
    hi, mid, lo = split3(-g_ref[...])
    four = sub8 < 4
    gate_rows = (
        jnp.concatenate(
            [jnp.where(four, hi, pltpu.roll(lo, 4, 0)), jnp.where(four, mid, 0.0)], axis=0
        ),
        jnp.concatenate(
            [jnp.where(four, pltpu.roll(hi, 4, 0), lo), jnp.where(four, pltpu.roll(mid, 4, 0), 0.0)],
            axis=0,
        ),
    )
    for c in range(2):
        spot = (c, maj[c], maj[1 - c])
        kv[spot + (slice(0, HD),)] = key_rows[c].astype(BF16)
        kv[spot + (slice(HD, ROWS),)] = vt[HD * c : HD * c + HD].astype(BF16)
        kv[spot + (slice(ROWS, BLOCK),)] = gate_rows[c].astype(BF16)
    for h in range(8):
        p, e = h // 2, h % 2
        qf = q_ref[:, 128 * p : 128 * p + 128].astype(F32) * 0.125
        turn = pltpu.roll(qf, HD, 1)
        at = slice(ROWS * e, ROWS * e + ROWS)
        picks = jnp.where(lax.rem(lane, 4) == h % 4, 1.0, 0.0).astype(BF16)
        head, other = (qf, turn) if e == 0 else (turn, qf)
        qs[p, 0, at, 0:ROWS] = jnp.where(low, head, 0.0).astype(BF16)
        qs[p, 1, at, 0:ROWS] = jnp.where(low, 0.0, other).astype(BF16)
        for n in range(2):
            qs[p, n, at, ROWS : 2 * ROWS] = picks

    for copy in ins[4:7]:
        copy.wait()
    for d in range(1, RING):
        pl.when(y + d < RING)(lambda: pl.semaphore_wait(ready_row.at[y + d], 1))

    halos = []
    for i, (src, dst) in enumerate(((x_ref, hx), (w_ref, hw), (r_ref, hr))):
        halos.append(
            remote(src.at[pl.ds(ROWS - 16, 16)], dst, halo_send.at[i], halo_recv.at[i], at_sp(after))
        )

    def each_halo(do):
        for h in halos:
            do(h)

    pl.when(me < RING * RING - 1)(lambda: each_halo(lambda h: h.start()))

    def first(c, d):
        peer = mod8(y + d) if c == 0 else z + d
        own = kv.at[c, maj[c], maj[1 - c]]
        return remote(own, own, kv1_send.at[c, d], kv1_recv.at[c, maj[1 - c]], {axis_of[1 - c]: peer})

    def first_arrival(c, b):
        slot = kv.at[c, maj[c], b]
        return remote(slot, slot, kv1_send.at[c, 0], kv1_recv.at[c, b], {axis_of[1 - c]: b})

    def relayed(i):
        from_left = (i == 3) | ((i == 4) & (tp == 0))
        block = mod8(jnp.where(from_left, y - 2, y + 2))
        peer = mod8(y + 1) if i == 3 else mod8(y - 1) if i == 5 else mod8(jnp.where(from_left, y + 2, y - 2))
        slot = kv.at[0, z, block]
        return remote(slot, slot, kv1_send.at[0, i], kv1_recv.at[0, block], {"sp_1": peer})

    for d in (1, 7, 2, 6):
        first(0, d).start()

    for d in range(1, RING):
        @pl.when(z + d < RING)
        def _():
            pl.semaphore_wait(ready.at[z + d], 1)
            first(1, d).start()

    ones = jnp.ones((16, ROWS), BF16)
    pair_query = lax.rem(lax.broadcasted_iota(jnp.int32, (HD, 2 * ROWS), 1), ROWS)
    pair_key = lax.broadcasted_iota(jnp.int32, (HD, 2 * ROWS), 0)
    lane_block = lane // 16

    def turned_gates(gates):
        f = jnp.concatenate([g.astype(F32) for g in gates], axis=0)
        if f.shape[0] < ROWS:
            f = jnp.concatenate([f, jnp.zeros((ROWS - f.shape[0], ROWS), F32)], axis=0)
        return f.T

    def scores(keys, gates, p, n):
        return dot(jnp.concatenate([keys, gates], axis=1), qs[p, n], NT)

    for c in range(2):
        own = kv.at[c, maj[c], maj[1 - c]]
        turned = turned_gates([own[ROWS:BLOCK]]).astype(BF16)
        vals = jnp.concatenate([own[HD:ROWS], ones], axis=0)
        for p in (2 * c, 2 * c + 1):
            s0 = scores(own[0:HD], turned[0:HD], p, 0)
            s1_ = scores(own[0:HD], turned[HD:ROWS], p, 1)
            s0 = jnp.where(pair_key <= pair_query, s0, NEG)
            s1_ = jnp.where(pair_key + HD <= pair_query, s1_, NEG)
            m = jnp.maximum(jnp.max(s0, axis=0, keepdims=True), jnp.max(s1_, axis=0, keepdims=True))
            probs = jnp.concatenate([jnp.exp(s0 - m), jnp.exp(s1_ - m)], axis=0).astype(BF16)
            m_sc[p] = jnp.broadcast_to(m, (8, 2 * ROWS))
            acc_sc[p] = dot(vals, probs)

    for copy in ins[7:]:
        copy.wait()

    @pl.when(me > 0)
    def _():
        each_halo(lambda h: h.wait_recv())

    opening = me > 0

    def filtered(rows, halo, taps):
        old = jnp.where(opening, halo[...].astype(F32), 0.0)
        padded = jnp.concatenate([old, rows[...].astype(F32)], axis=0)
        t = taps[...].astype(F32)
        total = t[0:1] * padded[13 : 13 + ROWS]
        for o in range(1, 4):
            total = total + t[o : o + 1] * padded[13 + o : 13 + o + ROWS]
        return silu(total).astype(BF16)

    xs_sc[...] = filtered(x_ref, hx, xtap_ref)
    wr = filtered(w_ref, hw, wtap_ref)
    rd = filtered(r_ref, hr, rtap_ref)
    rd_sc[...] = rd
    raw = step_ref[...]
    step = jnp.maximum(raw, 0.0) + jnp.log1p(jnp.exp(-jnp.abs(raw)))
    on_diagonal = sub8[:, 0:8] == lax.broadcasted_iota(jnp.int32, (8, 8), 1)
    rate = jnp.sum(jnp.where(on_diagonal, lane_ref[...], 0.0), axis=1, keepdims=True)
    cum = step * (-jnp.exp(rate)) + extra_ref[...]
    lane8 = lax.broadcasted_iota(jnp.int32, (8, ROWS), 1)
    for shift in (1, 2, 4, 8, 16, 32, 64):
        cum = cum + jnp.where(lane8 >= shift, pltpu.roll(cum, shift, 1), 0.0)
    end = cum[:, ROWS - 1 : ROWS]
    scale = jnp.exp(end - cum) * step
    wide[0:8] = cum
    wide[8:16] = scale
    wide[16:24] = jnp.broadcast_to(end, (8, ROWS))
    turned = wide[...].T
    inner = dot(rd, wr, NT)
    causal = lane <= sub
    for p in range(4):
        xp = xs_sc[:, 128 * p : 128 * p + 128]
        parts = []
        for e in range(2):
            h = 2 * p + e
            gap = jnp.where(causal, turned[:, h : h + 1] - cum[h : h + 1, :], NEG)
            mix = inner * (jnp.exp(gap) * step[h : h + 1, :])
            parts.append(dot(mix.astype(BF16), xp))
        xf = xp.astype(F32)
        skip = jnp.where(low, bypass_ref[:, 2 * p : 2 * p + 1], bypass_ref[:, 2 * p + 1 : 2 * p + 2])
        ms_sc[:, 128 * p : 128 * p + 128] = jnp.where(low, parts[0], parts[1]) + skip * xf
        ends = jnp.where(low, turned[:, 8 + 2 * p : 9 + 2 * p], turned[:, 9 + 2 * p : 10 + 2 * p])
        ecum_sc[:, 128 * p : 128 * p + 128] = jnp.exp(
            jnp.where(low, turned[:, 2 * p : 2 * p + 1], turned[:, 2 * p + 1 : 2 * p + 2])
        )
        state = dot((xf * ends).astype(BF16), wr, TN)
        for e in range(2):
            h = 2 * p + e
            msg[h, 0:HD] = state[HD * e : HD * e + HD].astype(BF16)

    def decay_rows(total):
        a, b, c3 = split3(total)
        return jnp.concatenate([jnp.where(four, a, c3), b], axis=0).astype(BF16)

    def decay_of(rows):
        f = rows.astype(F32)
        return (f[0:1] + f[8:9]) + f[4:5]

    for h in range(8):
        msg[h, HD:MSG] = decay_rows(jnp.broadcast_to(end[h : h + 1], (8, ROWS)))

    def around(src, dst, send, recv, axis, d):
        me_on = y if axis == "sp_1" else z
        peer = mod8(me_on + d)
        return remote(src(peer), dst.at[me_on], send.at[d], recv.at[RING - d], {axis: peer})

    def around_arrival(dst, send, recv, axis, d):
        me_on = y if axis == "sp_1" else z
        peer = mod8(me_on + d)
        slot = dst.at[peer]
        return remote(slot, slot, send.at[d], recv.at[d], {axis: peer})

    def up_total(d):
        return remote(tot, s2.at[z], s2_send.at[d], s2_recv.at[z], {"sp_0": z + d})

    for d in (2, 6):
        first_arrival(0, mod8(y + d)).wait_recv()
    for i in (3, 5, 4):
        relayed(i).start()

    s1_out = [around(lambda p: msg.at[p], s1, s1_send, s1_recv, "sp_1", d) for d in range(1, RING)]
    for o in s1_out:
        o.start()
    s1[y] = msg[y]

    def bundle(c, row, half):
        return kv.at[c, row, pl.ds(4 * half, 4)]

    def hop(c, d, k):
        away = -(k // 2) if d == 0 else k // 2
        half = (0 if d == 0 else 1) if k == 6 else k % 2
        slot = bundle(c, mod8(maj[c] + away), half)
        to = mod8(maj[c] + (1 if d == 0 else -1))
        return remote(slot, slot, kv_send.at[c, d, k], kv_recv.at[c, d, k], {axis_of[c]: to})

    def hop_arrival(c, d, k):
        away = -(k // 2) - 1 if d == 0 else k // 2 + 1
        half = (0 if d == 0 else 1) if k == 6 else k % 2
        slot = bundle(c, mod8(maj[c] + away), half)
        to = mod8(maj[c] + (1 if d == 0 else -1))
        return remote(slot, slot, kv_send.at[c, d, k], kv_recv.at[c, d, k], {axis_of[c]: to})

    def going(c, d, k):
        half = (0 if d == 0 else 1) if k == 6 else k % 2
        if c == 1:
            return z >= 4 * half
        if d == 0:
            return (z - k // 2 >= 0) & (z < last)
        return mod8(z + k // 2) <= 2 + half

    def coming(c, d, k):
        half = (0 if d == 0 else 1) if k == 6 else k % 2
        if c == 1:
            return z >= 4 * half
        if d == 0:
            return z - 1 - k // 2 >= 0
        return mod8(z + 1 + k // 2) <= 2 + half

    def send(c, d, k):
        pl.when(going(c, d, k))(lambda: hop(c, d, k).start())

    def attend(head, up, down, half_up, half_down):
        def one(c, carry):
            mine = jnp.where(c == 0, z, y)
            row_u, row_d = mod8(mine + up), mod8(mine + down)
            stride = jnp.where(c == 0, RING, 1)
            inner_stride = jnp.where(c == 0, 1, RING)
            lead_u = row_u * stride + 4 * half_up * inner_stride
            lead_d = row_d * stride + 4 * half_down * inner_stride

            @pl.when(jnp.minimum(lead_u, lead_d) < me)
            def _():
                spots = [(row_u, 4 * half_up + b) for b in range(4)]
                spots += [(row_d, 4 * half_down + b) for b in range(4)]
                leads = [lead_u + b * inner_stride for b in range(4)]
                leads += [lead_d + b * inner_stride for b in range(4)]
                turned = turned_gates([kv[c, r, b, ROWS:BLOCK] for r, b in spots])
                gates = []
                for n, lead in enumerate(leads):
                    off = jnp.where(lead < me, 0.0, NEG)
                    gates.append(jnp.where(lane_block == n, turned + off, 0.0).astype(BF16))
                for part in range(1):
                    at = range(8)
                    keys = jnp.concatenate([kv[(c,) + spots[n] + (slice(0, HD),)] for n in at], axis=0)
                    vals = [kv[(c,) + spots[n] + (slice(HD, ROWS),)] for n in at]
                    vals = jnp.concatenate(
                        [jnp.concatenate(vals, axis=1), jnp.concatenate([ones] * len(at), axis=1)], axis=0
                    )
                    gates_0 = jnp.concatenate([gates[n][0:HD] for n in at], axis=0)
                    gates_1 = jnp.concatenate([gates[n][HD:ROWS] for n in at], axis=0)
                    for i in range(2):
                        p = 2 * c + i
                        s0 = scores(keys, gates_0, p, 0)
                        s1_ = scores(keys, gates_1, p, 1)
                        m_old = m_sc[p, 0:1]
                        m = jnp.max(jnp.maximum(s0, s1_), axis=0, keepdims=True)
                        m = jnp.maximum(m, m_old)
                        m_sc[p, 0:1] = m
                        e0, e1 = jnp.exp(s0 - m).astype(BF16), jnp.exp(s1_ - m).astype(BF16)
                        probs = []
                        for b in range(len(at)):
                            probs += [e0[HD * b : HD * b + HD], e1[HD * b : HD * b + HD]]
                        probs = jnp.concatenate(probs, axis=0)
                        acc_sc[p] = acc_sc[p] * jnp.exp(m_old - m) + dot(vals, probs)

            return carry

        one(head, 0)

    def arrive(c, half):
        for b in range(4 * half, 4 * half + 4):
            there = (b != y) & (b != mod8(y + 2)) & (b != mod8(y - 2)) if c == 0 else (b < z)
            pl.when(there)(lambda: first_arrival(c, b).wait_recv())
        for d in range(2):
            send(c, d, half)

    arrive(1, 0)
    arrive(1, 1)
    attend(1, 0, 0, 0, 1)
    arrive(0, 0)
    arrive(0, 1)
    attend(0, 0, 0, 0, 1)

    def stage(k):
        if k == 0:
            weights_arrival(0, 0).wait_recv()
            passed_on(0).start()
            weights_arrival(1, 1).wait_recv()
            passed_on(1).start()
        if k == 0:
            for d in range(1, RING):
                around_arrival(s1, s1_send, s1_recv, "sp_1", d).wait_recv()
            run = jnp.zeros((HD, ROWS), F32)
            total = jnp.zeros((1, ROWS), F32)
            for j in range(RING):
                pre[j] = run
                cumpre[j] = jnp.broadcast_to(total, (8, ROWS))
                ld = decay_of(s1[j, HD:MSG])
                run = jnp.exp(ld) * run + s1[j, 0:HD].astype(F32)
                total = total + ld
            tot[0:HD] = run.astype(BF16)
            tot[HD:MSG] = decay_rows(jnp.broadcast_to(total, (8, ROWS)))
            for d in range(1, RING):
                pl.when(z + d < RING)(lambda: up_total(d).start())
        if k == 4:
            for j in range(RING - 1):
                slot = s2.at[j]
                come = remote(slot, slot, s2_send.at[0], s2_recv.at[j], {"sp_0": j})
                pl.when(j < z)(lambda: come.wait_recv())
            entering = jnp.zeros((HD, ROWS), F32)
            for j in range(RING - 1):
                later = jnp.exp(decay_of(s2[j, HD:MSG])) * entering + s2[j, 0:HD].astype(F32)
                entering = jnp.where(j < z, later, entering)
            for j in range(RING):
                back[j] = (pre[j] + jnp.exp(cumpre[j, 0:1]) * entering).astype(BF16)
            for d in range(1, RING):
                around(lambda p: back.at[p], carried, s3_send, s3_recv, "sp_1", d).start()
            carried[y] = back[y]
        if k == 6:
            for d in range(1, RING):
                around_arrival(carried, s3_send, s3_recv, "sp_1", d).wait_recv()
            states = jnp.concatenate([carried[h] for h in range(8)], axis=0)
            u = dot(rd_sc[...], states, NT) * ecum_sc[...] + ms_sc[...]
            u = u * silu(gate_ref[...].astype(F32))
            stretch = lax.rsqrt(jnp.mean(u * u, axis=1, keepdims=True) + EPSILON)
            xs_sc[...] = (u * stretch * gain_ref[...]).astype(BF16)
            for o in owns:
                o.wait()
            weights_arrival(0, 1).wait_recv()
            for n, f in enumerate((fx, mod4(fx - 1), mod4(fx + 1))):
                early[n] = dot(xs_sc[...], wbuf[0, f])

    for k in range(7):
        half_up = 0 if k == 6 else k % 2
        half_down = 1 if k == 6 else k % 2
        for c in (1, 0):
            for d in range(2):
                pl.when(coming(c, d, k))(lambda: hop_arrival(c, d, k).wait_recv())
            if k < 5:
                send(c, 0, k + 2)
            if k < 4:
                send(c, 1, k + 2)
            if k == 5:
                send(c, 1, 6)
            attend(c, -(k // 2) - 1, k // 2 + 1, half_up, half_down)
        stage(k)

    attended = []
    for p in range(4):
        acc = acc_sc[p]
        out = acc[0:HD] / acc[HD : HD + 1]
        out = jnp.concatenate([out[:, 0:ROWS], out[:, ROWS : 2 * ROWS]], axis=0)
        attended.append(out.T.astype(BF16))
    attended = jnp.concatenate(attended, axis=1)
    state_out = xs_sc[...]
    half_rows = ROWS // 2

    def across(n, f):
        slot = take_out.at[:, pl.ds(pl.multiple_of(512 * f, 512), 512)]
        return remote(give.at[n], slot, tp_send.at[n], tp_recv.at[n], {"tp": 1 - tp})

    def written(n, f):
        slot = keep_out.at[:, pl.ds(pl.multiple_of(512 * f, 512), 512)]
        return pltpu.make_async_copy(keep.at[n], slot, out_sem.at[n])

    columns = (fx, mod4(fx - 1), mod4(fx + 1), mod4(fx + 2))
    for n, f in enumerate(columns):
        if n == 1:
            weights_arrival(1, 0).wait_recv()
        if n == 3:
            passed_arrival(0).wait_recv()
            passed_arrival(1).wait_recv()
        merged = (early[n] if n < 3 else dot(state_out, wbuf[0, f])) + dot(attended, wbuf[1, f])
        top, bottom = merged[0:half_rows], merged[half_rows:ROWS]
        give[n] = jnp.where(tp == 0, bottom, top).astype(BF16)
        keep[n] = jnp.where(tp == 0, top, bottom)
        across(n, f).start()
        written(n, f).start()
    pl.when(me < RING * RING - 1)(lambda: each_halo(lambda h: h.wait_send()))
    for d in range(1, RING):
        (first(0, d) if d in (1, 2, 6, 7) else relayed(d)).wait_send()
        around(lambda p: msg.at[p], s1, s1_send, s1_recv, "sp_1", d).wait_send()
        around(lambda p: back.at[p], carried, s3_send, s3_recv, "sp_1", d).wait_send()

        @pl.when(z + d < RING)
        def _():
            first(1, d).wait_send()
            up_total(d).wait_send()
    for k in range(7):
        for c in range(2):
            for d in range(2):
                pl.when(going(c, d, k))(lambda: hop(c, d, k).wait_send())
    for j in range(2):
        for d in range(2):
            weights(j, d).wait_send()
        passed_on(j).wait_send()

    for n, f in enumerate(columns):
        written(n, f).wait()
        across(n, f).wait_send()
        across(n, f).wait_recv()


def shards(
    state_head_inputs, state_write_vectors, state_read_vectors, state_output_gate,
    presoftplus_steps, extra_decay_log, lane_shrinkage_powers, bypass_coefficient_vector,
    feeder_smoothing_stencil, stored_smoothing_stencil, lookup_smoothing_stencil,
    bundled_rescaling_vector, queries, attention_keys, attention_values, forget_gate_cumsum,
    state_out_weight, attention_out_weight,
):
    hbm = pl.BlockSpec(memory_space=pltpu.HBM)
    dma = pltpu.SemaphoreType.DMA
    kept, taken = pl.pallas_call(
        kernel,
        out_shape=(
            jax.ShapeDtypeStruct((ROWS // 2, 512 * FS), F32),
            jax.ShapeDtypeStruct((ROWS // 2, 512 * FS), BF16),
        ),
        in_specs=[hbm] * 18,
        out_specs=(hbm, hbm),
        scratch_shapes=[
            pltpu.VMEM((ROWS, 512), BF16), pltpu.VMEM((ROWS, ROWS), BF16), pltpu.VMEM((ROWS, ROWS), BF16),
            pltpu.VMEM((ROWS, 512), BF16), pltpu.VMEM((8, ROWS), F32), pltpu.VMEM((8, ROWS), F32),
            pltpu.VMEM((1, 8), F32), pltpu.VMEM((1, 8), F32),
            pltpu.VMEM((4, 512), BF16), pltpu.VMEM((4, ROWS), BF16), pltpu.VMEM((4, ROWS), BF16),
            pltpu.VMEM((1, 512), F32), pltpu.VMEM((ROWS, 512), BF16), pltpu.VMEM((ROWS, ROWS), BF16),
            pltpu.VMEM((ROWS, ROWS), BF16), pltpu.VMEM((8, ROWS), F32),
            pltpu.VMEM((2, RING, RING, BLOCK, ROWS), BF16),
            pltpu.VMEM((4, 2, 2 * ROWS, 2 * ROWS), BF16),
            pltpu.VMEM((ROWS, ROWS), F32),
            pltpu.VMEM((16, 512), BF16),
            pltpu.VMEM((16, ROWS), BF16),
            pltpu.VMEM((16, ROWS), BF16),
            pltpu.VMEM((4, 8, 2 * ROWS), F32),
            pltpu.VMEM((4, HD + 16, 2 * ROWS), F32),
            pltpu.VMEM((RING, MSG, ROWS), BF16),
            pltpu.VMEM((RING, MSG, ROWS), BF16),
            pltpu.VMEM((MSG, ROWS), BF16),
            pltpu.VMEM((RING, MSG, ROWS), BF16),
            pltpu.VMEM((RING, HD, ROWS), F32),
            pltpu.VMEM((RING, 8, ROWS), F32),
            pltpu.VMEM((RING, HD, ROWS), BF16),
            pltpu.VMEM((RING, HD, ROWS), BF16),
            pltpu.VMEM((ROWS, 512), BF16),
            pltpu.VMEM((ROWS, 512), F32),
            pltpu.VMEM((ROWS, ROWS), BF16),
            pltpu.VMEM((ROWS, 512), F32),
            pltpu.VMEM((2, FS, 512, 512), BF16),
            pltpu.VMEM((FS, ROWS // 2, 512), BF16),
            pltpu.VMEM((FS, ROWS // 2, 512), F32),
            pltpu.VMEM((3, ROWS, 512), F32),
            dma((2, RING)), dma((2, RING)),
            dma((2, 2, 7)), dma((2, 2, 7)),
            dma((RING,)), dma((RING,)), dma((RING,)), dma((RING,)), dma((RING,)), dma((RING,)),
            dma((2, 3)), dma((2, 3)), dma((2,)),
            dma((3,)), dma((3,)), dma((FS,)), dma((FS,)), dma((16,)), dma((FS,)),
            pltpu.SemaphoreType.REGULAR((RING,)), pltpu.SemaphoreType.REGULAR((RING,)),
        ],
        compiler_params=pltpu.CompilerParams(
            collective_id=0, has_side_effects=True, vmem_limit_bytes=60 * 1024 * 1024
        ),
        name="mixer",
    )(
        state_head_inputs[0], state_write_vectors[0], state_read_vectors[0], state_output_gate[0],
        presoftplus_steps[0], extra_decay_log[0],
        lane_shrinkage_powers.reshape(1, -1), bypass_coefficient_vector.reshape(1, -1),
        feeder_smoothing_stencil, stored_smoothing_stencil, lookup_smoothing_stencil,
        bundled_rescaling_vector.reshape(1, -1), queries[0], attention_keys[0], attention_values[0],
        forget_gate_cumsum[0].T, state_out_weight, attention_out_weight,
    )
    return (kept + taken.astype(F32)).astype(BF16)[None]


def solution(mesh):
    split = Mesh(
        mesh.devices.reshape(8, 8, mesh.shape["fs"], mesh.shape["tp"]), ("sp_0", "sp_1", "fs", "tp")
    )
    placed = (
        P("fs", SP, "tp"),
        P("fs", SP, "tp"),
        P("fs", SP, "tp"),
        P("fs", SP, "tp"),
        P("fs", "tp", SP),
        P("fs", "tp", SP),
        P("tp"),
        P("tp"),
        P(None, "tp"),
        P(None, "tp"),
        P(None, "tp"),
        P("tp"),
        P("fs", SP, "tp"),
        P("fs", SP, "tp"),
        P("fs", SP, "tp"),
        P("fs", SP, "tp"),
        P("tp", "fs"),
        P("tp", "fs"),
    )
    return jax.shard_map(
        shards, mesh=split, in_specs=placed, out_specs=P("fs", SP_TP, None), check_vma=False
    )
```

```python
import jax
import jax.numpy as jnp
from jax import lax
from jax.experimental import pallas as pl
from jax.experimental.pallas import tpu as pltpu
from jax.sharding import Mesh
from jax.sharding import PartitionSpec as P

SP = ("sp_0", "sp_1")
SP_TP = ("sp_0", "sp_1", "tp")
MESH = pl.DeviceIdType.MESH
BF16 = jnp.bfloat16
F32 = jnp.float32

RING = 8
FS = 4
ROWS = 128
HD = 64
BLOCK = ROWS + 16
MSG = HD + 16
EPSILON = 1e-06
NEG = -1e30

NT = (((1,), (1,)), ((), ()))
TN = (((0,), (0,)), ((), ()))


def mod8(i):
    return lax.rem(i + 2 * RING, RING)


def mod4(i):
    return lax.rem(i + 2 * FS, FS)


def dot(a, b, dims=None):
    if dims is None:
        return jnp.dot(a, b, preferred_element_type=F32)
    return lax.dot_general(a, b, dims, preferred_element_type=F32)


def silu(f):
    return f / (1.0 + jnp.exp(-f))


def split3(g):
    hi = g.astype(BF16).astype(F32)
    rest = g - hi
    mid = rest.astype(BF16).astype(F32)
    return hi, mid, rest - mid


def kernel(
    x_in, w_in, r_in, gate_in, step_in, extra_in, lane_in, bypass_in, xtap_in, wtap_in, rtap_in,
    gain_in, q_in, k_in, v_in, g_in, w1_ref, w2_ref,
    keep_out, take_out,
    x_ref, w_ref, r_ref, gate_ref, step_ref, extra_ref, lane_ref, bypass_ref, xtap_ref, wtap_ref, rtap_ref,
    gain_ref, q_ref, k_ref, v_ref, g_ref,
    kv, qs, wide, hx, hw, hr, m_sc, acc_sc, msg, s1, tot, s2, pre, cumpre, back, carried,
    xs_sc, ms_sc, rd_sc, ecum_sc, wbuf, give, keep, early,
    kv1_send, kv1_recv, kv_send, kv_recv, s1_send, s1_recv, s2_send, s2_recv, s3_send, s3_recv,
    w_send, w_recv, own_sem, halo_send, halo_recv, tp_send, tp_recv, in_sem, out_sem, ready, ready_row,
):
    z, y = lax.axis_index("sp_0"), lax.axis_index("sp_1")
    fx, tp = lax.axis_index("fs"), lax.axis_index("tp")
    me = z * RING + y
    maj = (z, y)
    axis_of = ("sp_0", "sp_1")
    after = lax.rem(me + 1, RING * RING)
    last = RING - 1

    def at_sp(i):
        return {"sp_0": i // RING, "sp_1": lax.rem(i, RING)}

    def remote(src, dst, send, recv, where):
        return pltpu.make_async_remote_copy(
            src_ref=src, dst_ref=dst, send_sem=send, recv_sem=recv,
            device_id=where, device_id_type=MESH,
        )

    lane = lax.broadcasted_iota(jnp.int32, (ROWS, ROWS), 1)
    sub = lax.broadcasted_iota(jnp.int32, (ROWS, ROWS), 0)
    low = lane < HD
    sub8 = lax.broadcasted_iota(jnp.int32, (8, ROWS), 0)

    ins = [
        pltpu.make_async_copy(src, dst, in_sem.at[i])
        for i, (src, dst) in enumerate((
            (k_in, k_ref), (v_in, v_ref), (g_in, g_ref), (q_in, q_ref), (x_in, x_ref), (w_in, w_ref),
            (r_in, r_ref), (step_in, step_ref), (extra_in, extra_ref), (lane_in, lane_ref),
            (bypass_in, bypass_ref), (xtap_in, xtap_ref), (wtap_in, wtap_ref), (rtap_in, rtap_ref),
            (gate_in, gate_ref), (gain_in, gain_ref),
        ))
    ]
    for copy in ins:
        copy.start()

    def clear_row(row, carry):
        kv[0, row] = jnp.zeros((RING, BLOCK, ROWS), BF16)
        kv[1, y, row] = jnp.zeros((BLOCK, ROWS), BF16)
        return carry

    lax.fori_loop(z + 1, RING, clear_row, 0)

    @pl.when(z < 4)
    def _():
        kv[1, mod8(y + 4), 4:8] = jnp.zeros((4, BLOCK, ROWS), BF16)

    barrier = pltpu.get_barrier_semaphore()

    def greet(peer):
        pl.semaphore_signal(barrier, inc=1, device_id=peer, device_id_type=MESH)

    for peer in ({"fs": mod4(fx + 1)}, {"fs": mod4(fx - 1)}, {"tp": 1 - tp}):
        greet(peer)
    for d in range(1, RING):
        pl.when(z + d < RING)(lambda d=d: greet({"sp_0": z + d}))
        pl.when(y + d < RING)(lambda d=d: greet({"sp_1": y + d}))
    pl.when((y == 0) & (z > 0))(lambda: greet(at_sp(me - 1)))

    inner_row = (y < last) | (z == last)
    pl.semaphore_wait(barrier, 3 + z + y + jnp.where(inner_row, 0, 1))
    for d in range(1, RING):
        @pl.when(z - d >= 0)
        def _():
            pl.semaphore_signal(
                ready.at[z], inc=1, device_id={"sp_0": z - d}, device_id_type=MESH
            )

        @pl.when(y - d >= 0)
        def _():
            pl.semaphore_signal(
                ready_row.at[y], inc=1, device_id={"sp_1": y - d}, device_id_type=MESH
            )

    right, left = {"fs": mod4(fx + 1)}, {"fs": mod4(fx - 1)}
    owns = [
        pltpu.make_async_copy(w1_ref, wbuf.at[0, fx], own_sem.at[0]),
        pltpu.make_async_copy(w2_ref, wbuf.at[1, fx], own_sem.at[1]),
    ]

    def weights(j, d):
        src = (w1_ref, w2_ref)[j]
        return remote(src, wbuf.at[j, fx], w_send.at[j, d], w_recv.at[j, d], (right, left)[d])

    def weights_arrival(j, d):
        slot = wbuf.at[j, mod4(fx - 1) if d == 0 else mod4(fx + 1)]
        return remote(slot, slot, w_send.at[j, d], w_recv.at[j, d], (right, left)[d])

    def passed_on(j):
        slot = wbuf.at[j, mod4(fx - 1) if j == 0 else mod4(fx + 1)]
        return remote(slot, slot, w_send.at[j, 2], w_recv.at[j, 2], (right, left)[j])

    def passed_arrival(j):
        slot = wbuf.at[j, mod4(fx + 2)]
        return remote(slot, slot, w_send.at[j, 2], w_recv.at[j, 2], (right, left)[j])

    for o in owns:
        o.start()
    for j, d in ((0, 0), (1, 1), (1, 0), (0, 1)):
        weights(j, d).start()

    wide[...] = jnp.zeros_like(wide)
    for copy in ins[0:4] + ins[7:10]:
        copy.wait()
    kf, vt = k_ref[...].astype(F32), v_ref[...].astype(F32).T
    low64 = low[0:HD]
    key_rows = (
        jnp.where(low64, kf[0:HD], pltpu.roll(kf[HD:ROWS], HD, 1)),
        jnp.where(low64, pltpu.roll(kf[0:HD], HD, 1), kf[HD:ROWS]),
    )
    hi, mid, lo = split3(-g_ref[...])
    four = sub8 < 4
    raw = step_ref[...]
    step = jnp.maximum(raw, 0.0) + jnp.log1p(jnp.exp(-jnp.abs(raw)))
    on_diagonal = sub8[:, 0:8] == lax.broadcasted_iota(jnp.int32, (8, 8), 1)
    rate = jnp.sum(jnp.where(on_diagonal, lane_ref[...], 0.0), axis=1, keepdims=True)
    cum = step * (-jnp.exp(rate)) + extra_ref[...]
    lane8 = lax.broadcasted_iota(jnp.int32, (8, ROWS), 1)
    for shift in (1, 2, 4, 8, 16, 32, 64):
        cum = cum + jnp.where(lane8 >= shift, pltpu.roll(cum, shift, 1), 0.0)
    end = cum[:, ROWS - 1 : ROWS]
    ends = jnp.sum(jnp.where(sub8 == lane8, end, 0.0), axis=0, keepdims=True)
    spare = jnp.zeros((8, ROWS), F32)
    for i, piece in enumerate(split3(ends)):
        spare = jnp.where(sub8 == 4 + i, piece, spare)
    gate_rows = (
        jnp.concatenate(
            [jnp.where(four, hi, pltpu.roll(lo, 4, 0)), jnp.where(four, mid, spare)], axis=0
        ),
        jnp.concatenate(
            [jnp.where(four, pltpu.roll(hi, 4, 0), lo), jnp.where(four, pltpu.roll(mid, 4, 0), 0.0)],
            axis=0,
        ),
    )
    for c in range(2):
        spot = (c, maj[c], maj[1 - c])
        kv[spot + (slice(0, HD),)] = key_rows[c].astype(BF16)
        kv[spot + (slice(HD, ROWS),)] = vt[HD * c : HD * c + HD].astype(BF16)
        kv[spot + (slice(ROWS, BLOCK),)] = gate_rows[c].astype(BF16)
    for h in range(8):
        p, e = h // 2, h % 2
        qf = q_ref[:, 128 * p : 128 * p + 128].astype(F32) * 0.125
        turn = pltpu.roll(qf, HD, 1)
        at = slice(ROWS * e, ROWS * e + ROWS)
        picks = (lax.rem(lane, 4) == h % 4) & (lax.rem(lane, 16) < 12)
        picks = jnp.where(picks, 1.0, 0.0).astype(BF16)
        head, other = (qf, turn) if e == 0 else (turn, qf)
        qs[p, 0, at, 0:ROWS] = jnp.where(low, head, 0.0).astype(BF16)
        qs[p, 1, at, 0:ROWS] = jnp.where(low, 0.0, other).astype(BF16)
        for n in range(2):
            qs[p, n, at, ROWS : 2 * ROWS] = picks

    for copy in ins[4:7]:
        copy.wait()
    for d in range(1, RING):
        pl.when(y + d < RING)(lambda: pl.semaphore_wait(ready_row.at[y + d], 1))

    halos = []
    for i, (src, dst) in enumerate(((x_ref, hx), (w_ref, hw), (r_ref, hr))):
        halos.append(
            remote(src.at[pl.ds(ROWS - 16, 16)], dst, halo_send.at[i], halo_recv.at[i], at_sp(after))
        )

    def each_halo(do):
        for h in halos:
            do(h)

    pl.when(me < RING * RING - 1)(lambda: each_halo(lambda h: h.start()))

    def first(c, d):
        peer = mod8(y + d) if c == 0 else z + d
        own = kv.at[c, maj[c], maj[1 - c]]
        return remote(own, own, kv1_send.at[c, d], kv1_recv.at[c, maj[1 - c]], {axis_of[1 - c]: peer})

    def first_arrival(c, b):
        slot = kv.at[c, maj[c], b]
        return remote(slot, slot, kv1_send.at[c, 0], kv1_recv.at[c, b], {axis_of[1 - c]: b})

    def relayed(i):
        from_left = (i == 3) | ((i == 4) & (tp == 0))
        block = mod8(jnp.where(from_left, y - 2, y + 2))
        peer = mod8(y + 1) if i == 3 else mod8(y - 1) if i == 5 else mod8(jnp.where(from_left, y + 2, y - 2))
        slot = kv.at[0, z, block]
        return remote(slot, slot, kv1_send.at[0, i], kv1_recv.at[0, block], {"sp_1": peer})

    for d in (1, 7, 2, 6):
        first(0, d).start()

    for d in range(1, RING):
        @pl.when(z + d < RING)
        def _():
            pl.semaphore_wait(ready.at[z + d], 1)
            first(1, d).start()

    ones = jnp.ones((16, ROWS), BF16)
    pair_query = lax.rem(lax.broadcasted_iota(jnp.int32, (HD, 2 * ROWS), 1), ROWS)
    pair_key = lax.broadcasted_iota(jnp.int32, (HD, 2 * ROWS), 0)
    lane_block = lane // 16

    def turned_gates(gates):
        f = jnp.concatenate([g.astype(F32) for g in gates], axis=0)
        if f.shape[0] < ROWS:
            f = jnp.concatenate([f, jnp.zeros((ROWS - f.shape[0], ROWS), F32)], axis=0)
        return f.T

    def scores(keys, gates, p, n):
        return dot(jnp.concatenate([keys, gates], axis=1), qs[p, n], NT)

    for c in range(2):
        own = kv.at[c, maj[c], maj[1 - c]]
        turned = turned_gates([own[ROWS:BLOCK]]).astype(BF16)
        vals = jnp.concatenate([own[HD:ROWS], ones], axis=0)
        for p in (2 * c, 2 * c + 1):
            s0 = scores(own[0:HD], turned[0:HD], p, 0)
            s1_ = scores(own[0:HD], turned[HD:ROWS], p, 1)
            s0 = jnp.where(pair_key <= pair_query, s0, NEG)
            s1_ = jnp.where(pair_key + HD <= pair_query, s1_, NEG)
            m = jnp.maximum(jnp.max(s0, axis=0, keepdims=True), jnp.max(s1_, axis=0, keepdims=True))
            probs = jnp.concatenate([jnp.exp(s0 - m), jnp.exp(s1_ - m)], axis=0).astype(BF16)
            m_sc[p] = jnp.broadcast_to(m, (8, 2 * ROWS))
            acc_sc[p] = dot(vals, probs)

    for copy in ins[10:]:
        copy.wait()

    @pl.when(me > 0)
    def _():
        each_halo(lambda h: h.wait_recv())

    opening = me > 0

    def filtered(rows, halo, taps):
        old = jnp.where(opening, halo[...].astype(F32), 0.0)
        padded = jnp.concatenate([old, rows[...].astype(F32)], axis=0)
        t = taps[...].astype(F32)
        total = t[0:1] * padded[13 : 13 + ROWS]
        for o in range(1, 4):
            total = total + t[o : o + 1] * padded[13 + o : 13 + o + ROWS]
        return silu(total).astype(BF16)

    xs_sc[...] = filtered(x_ref, hx, xtap_ref)
    wr = filtered(w_ref, hw, wtap_ref)
    rd = filtered(r_ref, hr, rtap_ref)
    rd_sc[...] = rd
    scale = jnp.exp(end - cum) * step
    wide[0:8] = cum
    wide[8:16] = scale
    wide[16:24] = jnp.broadcast_to(end, (8, ROWS))
    turned = wide[...].T
    inner = dot(rd, wr, NT)
    causal = lane <= sub
    for p in range(4):
        xp = xs_sc[:, 128 * p : 128 * p + 128]
        parts = []
        for e in range(2):
            h = 2 * p + e
            gap = jnp.where(causal, turned[:, h : h + 1] - cum[h : h + 1, :], NEG)
            mix = inner * (jnp.exp(gap) * step[h : h + 1, :])
            parts.append(dot(mix.astype(BF16), xp))
        xf = xp.astype(F32)
        skip = jnp.where(low, bypass_ref[:, 2 * p : 2 * p + 1], bypass_ref[:, 2 * p + 1 : 2 * p + 2])
        ms_sc[:, 128 * p : 128 * p + 128] = jnp.where(low, parts[0], parts[1]) + skip * xf
        ends = jnp.where(low, turned[:, 8 + 2 * p : 9 + 2 * p], turned[:, 9 + 2 * p : 10 + 2 * p])
        ecum_sc[:, 128 * p : 128 * p + 128] = jnp.exp(
            jnp.where(low, turned[:, 2 * p : 2 * p + 1], turned[:, 2 * p + 1 : 2 * p + 2])
        )
        state = dot((xf * ends).astype(BF16), wr, TN)
        for e in range(2):
            h = 2 * p + e
            msg[h] = state[HD * e : HD * e + HD].astype(BF16)

    def decay_rows(total):
        a, b, c3 = split3(total)
        return jnp.concatenate([jnp.where(four, a, c3), b], axis=0).astype(BF16)

    def decay_of(rows):
        f = rows.astype(F32)
        return (f[0:1] + f[8:9]) + f[4:5]

    def around(src, dst, send, recv, axis, d):
        me_on = y if axis == "sp_1" else z
        peer = mod8(me_on + d)
        return remote(src(peer), dst.at[me_on], send.at[d], recv.at[RING - d], {axis: peer})

    def around_arrival(dst, send, recv, axis, d):
        me_on = y if axis == "sp_1" else z
        peer = mod8(me_on + d)
        slot = dst.at[peer]
        return remote(slot, slot, send.at[d], recv.at[d], {axis: peer})

    def up_total(d):
        return remote(tot, s2.at[z], s2_send.at[d], s2_recv.at[z], {"sp_0": z + d})

    for d in (2, 6):
        first_arrival(0, mod8(y + d)).wait_recv()
    for i in (3, 5, 4):
        relayed(i).start()

    s1_out = [around(lambda p: msg.at[p], s1, s1_send, s1_recv, "sp_1", d) for d in range(1, RING)]
    for o in s1_out:
        o.start()
    s1[y] = msg[y]

    def bundle(c, row, half):
        return kv.at[c, row, pl.ds(4 * half, 4)]

    def hop(c, d, k):
        away = -(k // 2) if d == 0 else k // 2
        half = (0 if d == 0 else 1) if k == 6 else k % 2
        slot = bundle(c, mod8(maj[c] + away), half)
        to = mod8(maj[c] + (1 if d == 0 else -1))
        return remote(slot, slot, kv_send.at[c, d, k], kv_recv.at[c, d, k], {axis_of[c]: to})

    def hop_arrival(c, d, k):
        away = -(k // 2) - 1 if d == 0 else k // 2 + 1
        half = (0 if d == 0 else 1) if k == 6 else k % 2
        slot = bundle(c, mod8(maj[c] + away), half)
        to = mod8(maj[c] + (1 if d == 0 else -1))
        return remote(slot, slot, kv_send.at[c, d, k], kv_recv.at[c, d, k], {axis_of[c]: to})

    def going(c, d, k):
        half = (0 if d == 0 else 1) if k == 6 else k % 2
        if c == 1:
            return z >= 4 * half
        if d == 0:
            return (z - k // 2 >= 0) & (z < last)
        return mod8(z + k // 2) <= 2 + half

    def coming(c, d, k):
        half = (0 if d == 0 else 1) if k == 6 else k % 2
        if c == 1:
            return z >= 4 * half
        if d == 0:
            return z - 1 - k // 2 >= 0
        return mod8(z + 1 + k // 2) <= 2 + half

    def send(c, d, k):
        pl.when(going(c, d, k))(lambda: hop(c, d, k).start())

    def attend(head, up, down, half_up, half_down):
        def one(c, carry):
            mine = jnp.where(c == 0, z, y)
            row_u, row_d = mod8(mine + up), mod8(mine + down)
            stride = jnp.where(c == 0, RING, 1)
            inner_stride = jnp.where(c == 0, 1, RING)
            lead_u = row_u * stride + 4 * half_up * inner_stride
            lead_d = row_d * stride + 4 * half_down * inner_stride

            @pl.when(jnp.minimum(lead_u, lead_d) < me)
            def _():
                spots = [(row_u, 4 * half_up + b) for b in range(4)]
                spots += [(row_d, 4 * half_down + b) for b in range(4)]
                leads = [lead_u + b * inner_stride for b in range(4)]
                leads += [lead_d + b * inner_stride for b in range(4)]
                turned = turned_gates([kv[c, r, b, ROWS:BLOCK] for r, b in spots])
                gates = []
                for n, lead in enumerate(leads):
                    off = jnp.where(lead < me, 0.0, NEG)
                    gates.append(jnp.where(lane_block == n, turned + off, 0.0).astype(BF16))
                for part in range(1):
                    at = range(8)
                    keys = jnp.concatenate([kv[(c,) + spots[n] + (slice(0, HD),)] for n in at], axis=0)
                    vals = [kv[(c,) + spots[n] + (slice(HD, ROWS),)] for n in at]
                    vals = jnp.concatenate(
                        [jnp.concatenate(vals, axis=1), jnp.concatenate([ones] * len(at), axis=1)], axis=0
                    )
                    gates_0 = jnp.concatenate([gates[n][0:HD] for n in at], axis=0)
                    gates_1 = jnp.concatenate([gates[n][HD:ROWS] for n in at], axis=0)
                    for i in range(2):
                        p = 2 * c + i
                        s0 = scores(keys, gates_0, p, 0)
                        s1_ = scores(keys, gates_1, p, 1)
                        m_old = m_sc[p, 0:1]
                        m = jnp.max(jnp.maximum(s0, s1_), axis=0, keepdims=True)
                        m = jnp.maximum(m, m_old)
                        m_sc[p, 0:1] = m
                        e0, e1 = jnp.exp(s0 - m).astype(BF16), jnp.exp(s1_ - m).astype(BF16)
                        probs = []
                        for b in range(len(at)):
                            probs += [e0[HD * b : HD * b + HD], e1[HD * b : HD * b + HD]]
                        probs = jnp.concatenate(probs, axis=0)
                        acc_sc[p] = acc_sc[p] * jnp.exp(m_old - m) + dot(vals, probs)

            return carry

        one(head, 0)

    def arrive(c, half):
        for b in range(4 * half, 4 * half + 4):
            there = (b != y) & (b != mod8(y + 2)) & (b != mod8(y - 2)) if c == 0 else (b < z)
            pl.when(there)(lambda: first_arrival(c, b).wait_recv())
        for d in range(2):
            send(c, d, half)

    arrive(1, 0)
    arrive(1, 1)
    attend(1, 0, 0, 0, 1)
    arrive(0, 0)
    arrive(0, 1)
    attend(0, 0, 0, 0, 1)

    def stage(k):
        if k == 0:
            weights_arrival(0, 0).wait_recv()
            passed_on(0).start()
            weights_arrival(1, 1).wait_recv()
            passed_on(1).start()
        if k == 0:
            for d in range(1, RING):
                around_arrival(s1, s1_send, s1_recv, "sp_1", d).wait_recv()
            run = jnp.zeros((HD, ROWS), F32)
            total = jnp.zeros((1, ROWS), F32)
            for j in range(RING):
                pre[j] = run
                cumpre[j] = jnp.broadcast_to(total, (8, ROWS))
                g = kv[0, z, j, ROWS:BLOCK].astype(F32)
                ld = (g[12:13] + g[13:14]) + g[14:15]
                ld = jnp.sum(jnp.where(lane[0:1] == y, ld, 0.0), axis=1, keepdims=True)
                ld = jnp.broadcast_to(ld, (1, ROWS))
                run = jnp.exp(ld) * run + s1[j].astype(F32)
                total = total + ld
            tot[0:HD] = run.astype(BF16)
            tot[HD:MSG] = decay_rows(jnp.broadcast_to(total, (8, ROWS)))
            for d in range(1, RING):
                pl.when(z + d < RING)(lambda: up_total(d).start())
        if k == 4:
            for j in range(RING - 1):
                slot = s2.at[j]
                come = remote(slot, slot, s2_send.at[0], s2_recv.at[j], {"sp_0": j})
                pl.when(j < z)(lambda: come.wait_recv())
            entering = jnp.zeros((HD, ROWS), F32)
            for j in range(RING - 1):
                later = jnp.exp(decay_of(s2[j, HD:MSG])) * entering + s2[j, 0:HD].astype(F32)
                entering = jnp.where(j < z, later, entering)
            for j in range(RING):
                back[j] = (pre[j] + jnp.exp(cumpre[j, 0:1]) * entering).astype(BF16)
            for d in range(1, RING):
                around(lambda p: back.at[p], carried, s3_send, s3_recv, "sp_1", d).start()
            carried[y] = back[y]
        if k == 6:
            for d in range(1, RING):
                around_arrival(carried, s3_send, s3_recv, "sp_1", d).wait_recv()
            states = jnp.concatenate([carried[h] for h in range(8)], axis=0)
            u = dot(rd_sc[...], states, NT) * ecum_sc[...] + ms_sc[...]
            u = u * silu(gate_ref[...].astype(F32))
            stretch = lax.rsqrt(jnp.mean(u * u, axis=1, keepdims=True) + EPSILON)
            xs_sc[...] = (u * stretch * gain_ref[...]).astype(BF16)
            for o in owns:
                o.wait()
            weights_arrival(0, 1).wait_recv()
            for n, f in enumerate((fx, mod4(fx - 1), mod4(fx + 1))):
                early[n] = dot(xs_sc[...], wbuf[0, f])

    for k in range(7):
        half_up = 0 if k == 6 else k % 2
        half_down = 1 if k == 6 else k % 2
        for c in (0, 1):
            for d in range(2):
                pl.when(coming(c, d, k))(lambda: hop_arrival(c, d, k).wait_recv())
            if k < 5:
                send(c, 0, k + 2)
            if k < 4:
                send(c, 1, k + 2)
            if k == 5:
                send(c, 1, 6)
            attend(c, -(k // 2) - 1, k // 2 + 1, half_up, half_down)
        stage(k)

    attended = []
    for p in range(4):
        acc = acc_sc[p]
        out = acc[0:HD] / acc[HD : HD + 1]
        out = jnp.concatenate([out[:, 0:ROWS], out[:, ROWS : 2 * ROWS]], axis=0)
        attended.append(out.T.astype(BF16))
    attended = jnp.concatenate(attended, axis=1)
    state_out = xs_sc[...]
    half_rows = ROWS // 2

    def across(n, f):
        slot = take_out.at[:, pl.ds(pl.multiple_of(512 * f, 512), 512)]
        return remote(give.at[n], slot, tp_send.at[n], tp_recv.at[n], {"tp": 1 - tp})

    def written(n, f):
        slot = keep_out.at[:, pl.ds(pl.multiple_of(512 * f, 512), 512)]
        return pltpu.make_async_copy(keep.at[n], slot, out_sem.at[n])

    columns = (fx, mod4(fx - 1), mod4(fx + 1), mod4(fx + 2))
    for n, f in enumerate(columns):
        if n == 1:
            weights_arrival(1, 0).wait_recv()
        if n == 3:
            passed_arrival(0).wait_recv()
            passed_arrival(1).wait_recv()
        merged = (early[n] if n < 3 else dot(state_out, wbuf[0, f])) + dot(attended, wbuf[1, f])
        top, bottom = merged[0:half_rows], merged[half_rows:ROWS]
        give[n] = jnp.where(tp == 0, bottom, top).astype(BF16)
        keep[n] = jnp.where(tp == 0, top, bottom)
        across(n, f).start()
        written(n, f).start()
    pl.when(me < RING * RING - 1)(lambda: each_halo(lambda h: h.wait_send()))
    for d in range(1, RING):
        (first(0, d) if d in (1, 2, 6, 7) else relayed(d)).wait_send()
        around(lambda p: msg.at[p], s1, s1_send, s1_recv, "sp_1", d).wait_send()
        around(lambda p: back.at[p], carried, s3_send, s3_recv, "sp_1", d).wait_send()

        @pl.when(z + d < RING)
        def _():
            first(1, d).wait_send()
            up_total(d).wait_send()
    for k in range(7):
        for c in range(2):
            for d in range(2):
                pl.when(going(c, d, k))(lambda: hop(c, d, k).wait_send())
    for j in range(2):
        for d in range(2):
            weights(j, d).wait_send()
        passed_on(j).wait_send()

    for n, f in enumerate(columns):
        written(n, f).wait()
        across(n, f).wait_send()
        across(n, f).wait_recv()


def shards(
    state_head_inputs, state_write_vectors, state_read_vectors, state_output_gate,
    presoftplus_steps, extra_decay_log, lane_shrinkage_powers, bypass_coefficient_vector,
    feeder_smoothing_stencil, stored_smoothing_stencil, lookup_smoothing_stencil,
    bundled_rescaling_vector, queries, attention_keys, attention_values, forget_gate_cumsum,
    state_out_weight, attention_out_weight,
):
    hbm = pl.BlockSpec(memory_space=pltpu.HBM)
    dma = pltpu.SemaphoreType.DMA
    kept, taken = pl.pallas_call(
        kernel,
        out_shape=(
            jax.ShapeDtypeStruct((ROWS // 2, 512 * FS), F32),
            jax.ShapeDtypeStruct((ROWS // 2, 512 * FS), BF16),
        ),
        in_specs=[hbm] * 18,
        out_specs=(hbm, hbm),
        scratch_shapes=[
            pltpu.VMEM((ROWS, 512), BF16), pltpu.VMEM((ROWS, ROWS), BF16), pltpu.VMEM((ROWS, ROWS), BF16),
            pltpu.VMEM((ROWS, 512), BF16), pltpu.VMEM((8, ROWS), F32), pltpu.VMEM((8, ROWS), F32),
            pltpu.VMEM((1, 8), F32), pltpu.VMEM((1, 8), F32),
            pltpu.VMEM((4, 512), BF16), pltpu.VMEM((4, ROWS), BF16), pltpu.VMEM((4, ROWS), BF16),
            pltpu.VMEM((1, 512), F32), pltpu.VMEM((ROWS, 512), BF16), pltpu.VMEM((ROWS, ROWS), BF16),
            pltpu.VMEM((ROWS, ROWS), BF16), pltpu.VMEM((8, ROWS), F32),
            pltpu.VMEM((2, RING, RING, BLOCK, ROWS), BF16),
            pltpu.VMEM((4, 2, 2 * ROWS, 2 * ROWS), BF16),
            pltpu.VMEM((ROWS, ROWS), F32),
            pltpu.VMEM((16, 512), BF16),
            pltpu.VMEM((16, ROWS), BF16),
            pltpu.VMEM((16, ROWS), BF16),
            pltpu.VMEM((4, 8, 2 * ROWS), F32),
            pltpu.VMEM((4, HD + 16, 2 * ROWS), F32),
            pltpu.VMEM((RING, HD, ROWS), BF16),
            pltpu.VMEM((RING, HD, ROWS), BF16),
            pltpu.VMEM((MSG, ROWS), BF16),
            pltpu.VMEM((RING, MSG, ROWS), BF16),
            pltpu.VMEM((RING, HD, ROWS), F32),
            pltpu.VMEM((RING, 8, ROWS), F32),
            pltpu.VMEM((RING, HD, ROWS), BF16),
            pltpu.VMEM((RING, HD, ROWS), BF16),
            pltpu.VMEM((ROWS, 512), BF16),
            pltpu.VMEM((ROWS, 512), F32),
            pltpu.VMEM((ROWS, ROWS), BF16),
            pltpu.VMEM((ROWS, 512), F32),
            pltpu.VMEM((2, FS, 512, 512), BF16),
            pltpu.VMEM((FS, ROWS // 2, 512), BF16),
            pltpu.VMEM((FS, ROWS // 2, 512), F32),
            pltpu.VMEM((3, ROWS, 512), F32),
            dma((2, RING)), dma((2, RING)),
            dma((2, 2, 7)), dma((2, 2, 7)),
            dma((RING,)), dma((RING,)), dma((RING,)), dma((RING,)), dma((RING,)), dma((RING,)),
            dma((2, 3)), dma((2, 3)), dma((2,)),
            dma((3,)), dma((3,)), dma((FS,)), dma((FS,)), dma((16,)), dma((FS,)),
            pltpu.SemaphoreType.REGULAR((RING,)), pltpu.SemaphoreType.REGULAR((RING,)),
        ],
        compiler_params=pltpu.CompilerParams(
            collective_id=0, has_side_effects=True, vmem_limit_bytes=60 * 1024 * 1024
        ),
        name="mixer",
    )(
        state_head_inputs[0], state_write_vectors[0], state_read_vectors[0], state_output_gate[0],
        presoftplus_steps[0], extra_decay_log[0],
        lane_shrinkage_powers.reshape(1, -1), bypass_coefficient_vector.reshape(1, -1),
        feeder_smoothing_stencil, stored_smoothing_stencil, lookup_smoothing_stencil,
        bundled_rescaling_vector.reshape(1, -1), queries[0], attention_keys[0], attention_values[0],
        forget_gate_cumsum[0].T, state_out_weight, attention_out_weight,
    )
    return (kept + taken.astype(F32)).astype(BF16)[None]


def solution(mesh):
    split = Mesh(
        mesh.devices.reshape(8, 8, mesh.shape["fs"], mesh.shape["tp"]), ("sp_0", "sp_1", "fs", "tp")
    )
    placed = (
        P("fs", SP, "tp"),
        P("fs", SP, "tp"),
        P("fs", SP, "tp"),
        P("fs", SP, "tp"),
        P("fs", "tp", SP),
        P("fs", "tp", SP),
        P("tp"),
        P("tp"),
        P(None, "tp"),
        P(None, "tp"),
        P(None, "tp"),
        P("tp"),
        P("fs", SP, "tp"),
        P("fs", SP, "tp"),
        P("fs", SP, "tp"),
        P("fs", SP, "tp"),
        P("tp", "fs"),
        P("tp", "fs"),
    )
    return jax.shard_map(
        shards, mesh=split, in_specs=placed, out_specs=P("fs", SP_TP, None), check_vma=False
    )
```

```python
import jax
import jax.numpy as jnp
from jax import lax
from jax.experimental import pallas as pl
from jax.experimental.pallas import tpu as pltpu
from jax.sharding import Mesh
from jax.sharding import PartitionSpec as P

SP = ("sp_0", "sp_1")
SP_TP = ("sp_0", "sp_1", "tp")
MESH = pl.DeviceIdType.MESH
BF16 = jnp.bfloat16
F32 = jnp.float32

RING = 8
FS = 4
ROWS = 128
HD = 64
BLOCK = ROWS + 16
MSG = HD + 16
EPSILON = 1e-06
NEG = -1e30

NT = (((1,), (1,)), ((), ()))
TN = (((0,), (0,)), ((), ()))


def mod8(i):
    return lax.rem(i + 2 * RING, RING)


def mod4(i):
    return lax.rem(i + 2 * FS, FS)


def dot(a, b, dims=None):
    if dims is None:
        return jnp.dot(a, b, preferred_element_type=F32)
    return lax.dot_general(a, b, dims, preferred_element_type=F32)


def silu(f):
    return f / (1.0 + jnp.exp(-f))


def split3(g):
    hi = g.astype(BF16).astype(F32)
    rest = g - hi
    mid = rest.astype(BF16).astype(F32)
    return hi, mid, rest - mid


def kernel(
    x_in, w_in, r_in, gate_in, step_in, extra_in, lane_in, bypass_in, xtap_in, wtap_in, rtap_in,
    gain_in, q_in, k_in, v_in, g_in, w1_ref, w2_ref,
    keep_out, take_out,
    x_ref, w_ref, r_ref, gate_ref, step_ref, extra_ref, lane_ref, bypass_ref, xtap_ref, wtap_ref, rtap_ref,
    gain_ref, q_ref, k_ref, v_ref, g_ref,
    kv, qs, wide, hx, hw, hr, m_sc, acc_sc, msg, s1, tot, s2, pre, cumpre, back, carried,
    xs_sc, ms_sc, rd_sc, ecum_sc, wbuf, give, keep, early,
    kv1_send, kv1_recv, kv_send, kv_recv, s1_send, s1_recv, s2_send, s2_recv, s3_send, s3_recv,
    w_send, w_recv, own_sem, halo_send, halo_recv, tp_send, tp_recv, in_sem, out_sem, ready, ready_row,
):
    z, y = lax.axis_index("sp_0"), lax.axis_index("sp_1")
    fx, tp = lax.axis_index("fs"), lax.axis_index("tp")
    me = z * RING + y
    maj = (z, y)
    axis_of = ("sp_0", "sp_1")
    after = lax.rem(me + 1, RING * RING)
    last = RING - 1

    def at_sp(i):
        return {"sp_0": i // RING, "sp_1": lax.rem(i, RING)}

    def remote(src, dst, send, recv, where):
        return pltpu.make_async_remote_copy(
            src_ref=src, dst_ref=dst, send_sem=send, recv_sem=recv,
            device_id=where, device_id_type=MESH,
        )

    lane = lax.broadcasted_iota(jnp.int32, (ROWS, ROWS), 1)
    sub = lax.broadcasted_iota(jnp.int32, (ROWS, ROWS), 0)
    low = lane < HD
    sub8 = lax.broadcasted_iota(jnp.int32, (8, ROWS), 0)

    ins = [
        pltpu.make_async_copy(src, dst, in_sem.at[i])
        for i, (src, dst) in enumerate((
            (k_in, k_ref), (v_in, v_ref), (g_in, g_ref), (q_in, q_ref), (x_in, x_ref), (w_in, w_ref),
            (r_in, r_ref), (step_in, step_ref), (extra_in, extra_ref), (lane_in, lane_ref),
            (bypass_in, bypass_ref), (xtap_in, xtap_ref), (wtap_in, wtap_ref), (rtap_in, rtap_ref),
            (gate_in, gate_ref), (gain_in, gain_ref),
        ))
    ]
    for copy in ins:
        copy.start()

    def clear_row(row, carry):
        kv[0, row] = jnp.zeros((RING, BLOCK, ROWS), BF16)
        kv[1, y, row] = jnp.zeros((BLOCK, ROWS), BF16)
        return carry

    lax.fori_loop(z + 1, RING, clear_row, 0)

    @pl.when(z < 4)
    def _():
        kv[1, mod8(y + 4), 4:8] = jnp.zeros((4, BLOCK, ROWS), BF16)

    barrier = pltpu.get_barrier_semaphore()

    def greet(peer):
        pl.semaphore_signal(barrier, inc=1, device_id=peer, device_id_type=MESH)

    for peer in ({"fs": mod4(fx + 1)}, {"fs": mod4(fx - 1)}, {"tp": 1 - tp}):
        greet(peer)
    for d in range(1, RING):
        pl.when(z + d < RING)(lambda d=d: greet({"sp_0": z + d}))
        pl.when(y + d < RING)(lambda d=d: greet({"sp_1": y + d}))
    pl.when((y == 0) & (z > 0))(lambda: greet(at_sp(me - 1)))

    inner_row = (y < last) | (z == last)
    pl.semaphore_wait(barrier, 3 + z + y + jnp.where(inner_row, 0, 1))
    for d in range(1, RING):
        @pl.when(z - d >= 0)
        def _():
            pl.semaphore_signal(
                ready.at[z], inc=1, device_id={"sp_0": z - d}, device_id_type=MESH
            )

        @pl.when(y - d >= 0)
        def _():
            pl.semaphore_signal(
                ready_row.at[y], inc=1, device_id={"sp_1": y - d}, device_id_type=MESH
            )

    right, left = {"fs": mod4(fx + 1)}, {"fs": mod4(fx - 1)}
    owns = [
        pltpu.make_async_copy(w1_ref, wbuf.at[0, fx], own_sem.at[0]),
        pltpu.make_async_copy(w2_ref, wbuf.at[1, fx], own_sem.at[1]),
    ]

    def weights(j, d):
        src = (w1_ref, w2_ref)[j]
        return remote(src, wbuf.at[j, fx], w_send.at[j, d], w_recv.at[j, d], (right, left)[d])

    def weights_arrival(j, d):
        slot = wbuf.at[j, mod4(fx - 1) if d == 0 else mod4(fx + 1)]
        return remote(slot, slot, w_send.at[j, d], w_recv.at[j, d], (right, left)[d])

    def passed_on(j):
        slot = wbuf.at[j, mod4(fx - 1) if j == 0 else mod4(fx + 1)]
        return remote(slot, slot, w_send.at[j, 2], w_recv.at[j, 2], (right, left)[j])

    def passed_arrival(j):
        slot = wbuf.at[j, mod4(fx + 2)]
        return remote(slot, slot, w_send.at[j, 2], w_recv.at[j, 2], (right, left)[j])

    for o in owns:
        o.start()
    for j, d in ((0, 0), (1, 1), (1, 0), (0, 1)):
        weights(j, d).start()

    wide[...] = jnp.zeros_like(wide)
    for copy in ins[0:4] + ins[7:10]:
        copy.wait()
    kf, vt = k_ref[...].astype(F32), v_ref[...].astype(F32).T
    low64 = low[0:HD]
    key_rows = (
        jnp.where(low64, kf[0:HD], pltpu.roll(kf[HD:ROWS], HD, 1)),
        jnp.where(low64, pltpu.roll(kf[0:HD], HD, 1), kf[HD:ROWS]),
    )
    hi, mid, lo = split3(-g_ref[...])
    four = sub8 < 4
    raw = step_ref[...]
    step = jnp.maximum(raw, 0.0) + jnp.log1p(jnp.exp(-jnp.abs(raw)))
    on_diagonal = sub8[:, 0:8] == lax.broadcasted_iota(jnp.int32, (8, 8), 1)
    rate = jnp.sum(jnp.where(on_diagonal, lane_ref[...], 0.0), axis=1, keepdims=True)
    cum = step * (-jnp.exp(rate)) + extra_ref[...]
    lane8 = lax.broadcasted_iota(jnp.int32, (8, ROWS), 1)
    for shift in (1, 2, 4, 8, 16, 32, 64):
        cum = cum + jnp.where(lane8 >= shift, pltpu.roll(cum, shift, 1), 0.0)
    end = cum[:, ROWS - 1 : ROWS]
    ends = jnp.sum(jnp.where(sub8 == lane8, end, 0.0), axis=0, keepdims=True)
    spare = jnp.zeros((8, ROWS), F32)
    for i, piece in enumerate(split3(ends)):
        spare = jnp.where(sub8 == 4 + i, piece, spare)
    gate_rows = (
        jnp.concatenate(
            [jnp.where(four, hi, pltpu.roll(lo, 4, 0)), jnp.where(four, mid, spare)], axis=0
        ),
        jnp.concatenate(
            [jnp.where(four, pltpu.roll(hi, 4, 0), lo), jnp.where(four, pltpu.roll(mid, 4, 0), 0.0)],
            axis=0,
        ),
    )
    for c in range(2):
        spot = (c, maj[c], maj[1 - c])
        kv[spot + (slice(0, HD),)] = key_rows[c].astype(BF16)
        kv[spot + (slice(HD, ROWS),)] = vt[HD * c : HD * c + HD].astype(BF16)
        kv[spot + (slice(ROWS, BLOCK),)] = gate_rows[c].astype(BF16)
    for h in range(8):
        p, e = h // 2, h % 2
        qf = q_ref[:, 128 * p : 128 * p + 128].astype(F32) * 0.125
        turn = pltpu.roll(qf, HD, 1)
        at = slice(ROWS * e, ROWS * e + ROWS)
        picks = (lax.rem(lane, 4) == h % 4) & (lax.rem(lane, 16) < 12)
        picks = jnp.where(picks, 1.0, 0.0).astype(BF16)
        head, other = (qf, turn) if e == 0 else (turn, qf)
        qs[p, 0, at, 0:ROWS] = jnp.where(low, head, 0.0).astype(BF16)
        qs[p, 1, at, 0:ROWS] = jnp.where(low, 0.0, other).astype(BF16)
        for n in range(2):
            qs[p, n, at, ROWS : 2 * ROWS] = picks

    for copy in ins[4:7]:
        copy.wait()
    for d in range(1, RING):
        pl.when(y + d < RING)(lambda: pl.semaphore_wait(ready_row.at[y + d], 1))

    halos = []
    for i, (src, dst) in enumerate(((x_ref, hx), (w_ref, hw), (r_ref, hr))):
        halos.append(
            remote(src.at[pl.ds(ROWS - 16, 16)], dst, halo_send.at[i], halo_recv.at[i], at_sp(after))
        )

    def each_halo(do):
        for h in halos:
            do(h)

    pl.when(me < RING * RING - 1)(lambda: each_halo(lambda h: h.start()))

    def first(c, d):
        peer = mod8(y + d) if c == 0 else z + d
        own = kv.at[c, maj[c], maj[1 - c]]
        return remote(own, own, kv1_send.at[c, d], kv1_recv.at[c, maj[1 - c]], {axis_of[1 - c]: peer})

    def first_arrival(c, b):
        slot = kv.at[c, maj[c], b]
        return remote(slot, slot, kv1_send.at[c, 0], kv1_recv.at[c, b], {axis_of[1 - c]: b})

    def relayed(i):
        from_left = (i == 3) | ((i == 4) & (tp == 0))
        block = mod8(jnp.where(from_left, y - 2, y + 2))
        peer = mod8(y + 1) if i == 3 else mod8(y - 1) if i == 5 else mod8(jnp.where(from_left, y + 2, y - 2))
        slot = kv.at[0, z, block]
        return remote(slot, slot, kv1_send.at[0, i], kv1_recv.at[0, block], {"sp_1": peer})

    for d in (1, 7, 2, 6):
        first(0, d).start()

    for d in range(1, RING):
        @pl.when(z + d < RING)
        def _():
            pl.semaphore_wait(ready.at[z + d], 1)
            first(1, d).start()

    ones = jnp.ones((16, ROWS), BF16)
    pair_query = lax.rem(lax.broadcasted_iota(jnp.int32, (HD, 2 * ROWS), 1), ROWS)
    pair_key = lax.broadcasted_iota(jnp.int32, (HD, 2 * ROWS), 0)
    lane_block = lane // 16

    def turned_gates(gates):
        f = jnp.concatenate([g.astype(F32) for g in gates], axis=0)
        if f.shape[0] < ROWS:
            f = jnp.concatenate([f, jnp.zeros((ROWS - f.shape[0], ROWS), F32)], axis=0)
        return f.T

    def scores(keys, gates, p, n):
        return dot(jnp.concatenate([keys, gates], axis=1), qs[p, n], NT)

    for c in range(2):
        own = kv.at[c, maj[c], maj[1 - c]]
        turned = turned_gates([own[ROWS:BLOCK]]).astype(BF16)
        vals = jnp.concatenate([own[HD:ROWS], ones], axis=0)
        for p in (2 * c, 2 * c + 1):
            s0 = scores(own[0:HD], turned[0:HD], p, 0)
            s1_ = scores(own[0:HD], turned[HD:ROWS], p, 1)
            s0 = jnp.where(pair_key <= pair_query, s0, NEG)
            s1_ = jnp.where(pair_key + HD <= pair_query, s1_, NEG)
            m = jnp.maximum(jnp.max(s0, axis=0, keepdims=True), jnp.max(s1_, axis=0, keepdims=True))
            probs = jnp.concatenate([jnp.exp(s0 - m), jnp.exp(s1_ - m)], axis=0).astype(BF16)
            m_sc[p] = jnp.broadcast_to(m, (8, 2 * ROWS))
            acc_sc[p] = dot(vals, probs)

    for copy in ins[10:]:
        copy.wait()

    @pl.when(me > 0)
    def _():
        each_halo(lambda h: h.wait_recv())

    opening = me > 0

    def filtered(rows, halo, taps):
        old = jnp.where(opening, halo[...].astype(F32), 0.0)
        padded = jnp.concatenate([old, rows[...].astype(F32)], axis=0)
        t = taps[...].astype(F32)
        total = t[0:1] * padded[13 : 13 + ROWS]
        for o in range(1, 4):
            total = total + t[o : o + 1] * padded[13 + o : 13 + o + ROWS]
        return silu(total).astype(BF16)

    xs_sc[...] = filtered(x_ref, hx, xtap_ref)
    wr = filtered(w_ref, hw, wtap_ref)
    rd = filtered(r_ref, hr, rtap_ref)
    rd_sc[...] = rd
    scale = jnp.exp(end - cum) * step
    wide[0:8] = cum
    wide[8:16] = scale
    wide[16:24] = jnp.broadcast_to(end, (8, ROWS))
    turned = wide[...].T
    inner = dot(rd, wr, NT)
    causal = lane <= sub
    for p in range(4):
        xp = xs_sc[:, 128 * p : 128 * p + 128]
        parts = []
        for e in range(2):
            h = 2 * p + e
            gap = jnp.where(causal, turned[:, h : h + 1] - cum[h : h + 1, :], NEG)
            mix = inner * (jnp.exp(gap) * step[h : h + 1, :])
            parts.append(dot(mix.astype(BF16), xp))
        xf = xp.astype(F32)
        skip = jnp.where(low, bypass_ref[:, 2 * p : 2 * p + 1], bypass_ref[:, 2 * p + 1 : 2 * p + 2])
        ms_sc[:, 128 * p : 128 * p + 128] = jnp.where(low, parts[0], parts[1]) + skip * xf
        ends = jnp.where(low, turned[:, 8 + 2 * p : 9 + 2 * p], turned[:, 9 + 2 * p : 10 + 2 * p])
        ecum_sc[:, 128 * p : 128 * p + 128] = jnp.exp(
            jnp.where(low, turned[:, 2 * p : 2 * p + 1], turned[:, 2 * p + 1 : 2 * p + 2])
        )
        state = dot((xf * ends).astype(BF16), wr, TN)
        for e in range(2):
            h = 2 * p + e
            msg[h] = state[HD * e : HD * e + HD].astype(BF16)

    def decay_rows(total):
        a, b, c3 = split3(total)
        return jnp.concatenate([jnp.where(four, a, c3), b], axis=0).astype(BF16)

    def decay_of(rows):
        f = rows.astype(F32)
        return (f[0:1] + f[8:9]) + f[4:5]

    def around(src, dst, send, recv, axis, d):
        me_on = y if axis == "sp_1" else z
        peer = mod8(me_on + d)
        return remote(src(peer), dst.at[me_on], send.at[d], recv.at[RING - d], {axis: peer})

    def around_arrival(dst, send, recv, axis, d):
        me_on = y if axis == "sp_1" else z
        peer = mod8(me_on + d)
        slot = dst.at[peer]
        return remote(slot, slot, send.at[d], recv.at[d], {axis: peer})

    def up_total(d):
        return remote(tot, s2.at[z], s2_send.at[d], s2_recv.at[z], {"sp_0": z + d})

    for d in (2, 6):
        first_arrival(0, mod8(y + d)).wait_recv()
    for i in (3, 5, 4):
        relayed(i).start()

    s1_out = [around(lambda p: msg.at[p], s1, s1_send, s1_recv, "sp_1", d) for d in range(1, RING)]
    for o in s1_out:
        o.start()
    s1[y] = msg[y]

    def bundle(c, row, half):
        return kv.at[c, row, pl.ds(4 * half, 4)]

    def hop(c, d, k):
        away = -(k // 2) if d == 0 else k // 2
        half = (0 if d == 0 else 1) if k == 6 else k % 2
        slot = bundle(c, mod8(maj[c] + away), half)
        to = mod8(maj[c] + (1 if d == 0 else -1))
        return remote(slot, slot, kv_send.at[c, d, k], kv_recv.at[c, d, k], {axis_of[c]: to})

    def hop_arrival(c, d, k):
        away = -(k // 2) - 1 if d == 0 else k // 2 + 1
        half = (0 if d == 0 else 1) if k == 6 else k % 2
        slot = bundle(c, mod8(maj[c] + away), half)
        to = mod8(maj[c] + (1 if d == 0 else -1))
        return remote(slot, slot, kv_send.at[c, d, k], kv_recv.at[c, d, k], {axis_of[c]: to})

    def going(c, d, k):
        half = (0 if d == 0 else 1) if k == 6 else k % 2
        if c == 1:
            return z >= 4 * half
        if d == 0:
            return (z - k // 2 >= 0) & (z < last)
        return mod8(z + k // 2) <= 2 + half

    def coming(c, d, k):
        half = (0 if d == 0 else 1) if k == 6 else k % 2
        if c == 1:
            return z >= 4 * half
        if d == 0:
            return z - 1 - k // 2 >= 0
        return mod8(z + 1 + k // 2) <= 2 + half

    def send(c, d, k):
        pl.when(going(c, d, k))(lambda: hop(c, d, k).start())

    def attend(head, up, down, half_up, half_down):
        def one(c, carry):
            mine = jnp.where(c == 0, z, y)
            row_u, row_d = mod8(mine + up), mod8(mine + down)
            stride = jnp.where(c == 0, RING, 1)
            inner_stride = jnp.where(c == 0, 1, RING)
            lead_u = row_u * stride + 4 * half_up * inner_stride
            lead_d = row_d * stride + 4 * half_down * inner_stride

            @pl.when(jnp.minimum(lead_u, lead_d) < me)
            def _():
                spots = [(row_u, 4 * half_up + b) for b in range(4)]
                spots += [(row_d, 4 * half_down + b) for b in range(4)]
                leads = [lead_u + b * inner_stride for b in range(4)]
                leads += [lead_d + b * inner_stride for b in range(4)]
                turned = turned_gates([kv[c, r, b, ROWS:BLOCK] for r, b in spots])
                gates = []
                for n, lead in enumerate(leads):
                    off = jnp.where(lead < me, 0.0, NEG)
                    gates.append(jnp.where(lane_block == n, turned + off, 0.0).astype(BF16))
                for part in range(1):
                    at = range(8)
                    keys = jnp.concatenate([kv[(c,) + spots[n] + (slice(0, HD),)] for n in at], axis=0)
                    vals = [kv[(c,) + spots[n] + (slice(HD, ROWS),)] for n in at]
                    vals = jnp.concatenate(
                        [jnp.concatenate(vals, axis=1), jnp.concatenate([ones] * len(at), axis=1)], axis=0
                    )
                    gates_0 = jnp.concatenate([gates[n][0:HD] for n in at], axis=0)
                    gates_1 = jnp.concatenate([gates[n][HD:ROWS] for n in at], axis=0)
                    for i in range(2):
                        p = 2 * c + i
                        s0 = scores(keys, gates_0, p, 0)
                        s1_ = scores(keys, gates_1, p, 1)
                        m_old = m_sc[p, 0:1]
                        m = jnp.max(jnp.maximum(s0, s1_), axis=0, keepdims=True)
                        m = jnp.maximum(m, m_old)
                        m_sc[p, 0:1] = m
                        e0, e1 = jnp.exp(s0 - m).astype(BF16), jnp.exp(s1_ - m).astype(BF16)
                        probs = []
                        for b in range(len(at)):
                            probs += [e0[HD * b : HD * b + HD], e1[HD * b : HD * b + HD]]
                        probs = jnp.concatenate(probs, axis=0)
                        acc_sc[p] = acc_sc[p] * jnp.exp(m_old - m) + dot(vals, probs)

            return carry

        one(head, 0)

    def arrive(c, half):
        for b in range(4 * half, 4 * half + 4):
            there = (b != y) & (b != mod8(y + 2)) & (b != mod8(y - 2)) if c == 0 else (b < z)
            pl.when(there)(lambda: first_arrival(c, b).wait_recv())
        for d in range(2):
            send(c, d, half)

    arrive(1, 0)
    arrive(1, 1)
    attend(1, 0, 0, 0, 1)
    arrive(0, 0)
    arrive(0, 1)
    attend(0, 0, 0, 0, 1)

    def entering_states():
        for j in range(RING - 1):
            slot = s2.at[j]
            come = remote(slot, slot, s2_send.at[0], s2_recv.at[j], {"sp_0": j})
            pl.when(j < z)(lambda: come.wait_recv())
        entering = jnp.zeros((HD, ROWS), F32)
        for j in range(RING - 1):
            later = jnp.exp(decay_of(s2[j, HD:MSG])) * entering + s2[j, 0:HD].astype(F32)
            entering = jnp.where(j < z, later, entering)
        for j in range(RING):
            back[j] = (pre[j] + jnp.exp(cumpre[j, 0:1]) * entering).astype(BF16)
        for d in range(1, RING):
            around(lambda p: back.at[p], carried, s3_send, s3_recv, "sp_1", d).start()
        carried[y] = back[y]

    def stage(k):
        if k == 0:
            weights_arrival(0, 0).wait_recv()
            passed_on(0).start()
            weights_arrival(1, 1).wait_recv()
            passed_on(1).start()
        if k == 0:
            for d in range(1, RING):
                around_arrival(s1, s1_send, s1_recv, "sp_1", d).wait_recv()
            run = jnp.zeros((HD, ROWS), F32)
            total = jnp.zeros((1, ROWS), F32)
            for j in range(RING):
                pre[j] = run
                cumpre[j] = jnp.broadcast_to(total, (8, ROWS))
                g = kv[0, z, j, ROWS:BLOCK].astype(F32)
                ld = (g[12:13] + g[13:14]) + g[14:15]
                ld = jnp.sum(jnp.where(lane[0:1] == y, ld, 0.0), axis=1, keepdims=True)
                ld = jnp.broadcast_to(ld, (1, ROWS))
                run = jnp.exp(ld) * run + s1[j].astype(F32)
                total = total + ld
            tot[0:HD] = run.astype(BF16)
            tot[HD:MSG] = decay_rows(jnp.broadcast_to(total, (8, ROWS)))
            for d in range(1, RING):
                pl.when(z + d < RING)(lambda: up_total(d).start())
        if k == 2:
            pl.when(z < 4)(entering_states)
        if k == 4:
            pl.when(z >= 4)(entering_states)
        if k == 6:
            for d in range(1, RING):
                around_arrival(carried, s3_send, s3_recv, "sp_1", d).wait_recv()
            states = jnp.concatenate([carried[h] for h in range(8)], axis=0)
            u = dot(rd_sc[...], states, NT) * ecum_sc[...] + ms_sc[...]
            u = u * silu(gate_ref[...].astype(F32))
            stretch = lax.rsqrt(jnp.mean(u * u, axis=1, keepdims=True) + EPSILON)
            xs_sc[...] = (u * stretch * gain_ref[...]).astype(BF16)
            for o in owns:
                o.wait()
            weights_arrival(0, 1).wait_recv()
            for n, f in enumerate((fx, mod4(fx - 1), mod4(fx + 1))):
                early[n] = dot(xs_sc[...], wbuf[0, f])

    for k in range(7):
        half_up = 0 if k == 6 else k % 2
        half_down = 1 if k == 6 else k % 2
        for c in (0, 1):
            for d in range(2):
                pl.when(coming(c, d, k))(lambda: hop_arrival(c, d, k).wait_recv())
            if k < 5:
                send(c, 0, k + 2)
            if k < 4:
                send(c, 1, k + 2)
            if k == 5:
                send(c, 1, 6)
            attend(c, -(k // 2) - 1, k // 2 + 1, half_up, half_down)
        stage(k)

    attended = []
    for p in range(4):
        acc = acc_sc[p]
        out = acc[0:HD] / acc[HD : HD + 1]
        out = jnp.concatenate([out[:, 0:ROWS], out[:, ROWS : 2 * ROWS]], axis=0)
        attended.append(out.T.astype(BF16))
    attended = jnp.concatenate(attended, axis=1)
    state_out = xs_sc[...]
    half_rows = ROWS // 2

    def across(n, f):
        slot = take_out.at[:, pl.ds(pl.multiple_of(512 * f, 512), 512)]
        return remote(give.at[n], slot, tp_send.at[n], tp_recv.at[n], {"tp": 1 - tp})

    def written(n, f):
        slot = keep_out.at[:, pl.ds(pl.multiple_of(512 * f, 512), 512)]
        return pltpu.make_async_copy(keep.at[n], slot, out_sem.at[n])

    columns = (fx, mod4(fx - 1), mod4(fx + 1), mod4(fx + 2))
    for n, f in enumerate(columns):
        if n == 1:
            weights_arrival(1, 0).wait_recv()
        if n == 3:
            passed_arrival(0).wait_recv()
            passed_arrival(1).wait_recv()
        merged = (early[n] if n < 3 else dot(state_out, wbuf[0, f])) + dot(attended, wbuf[1, f])
        top, bottom = merged[0:half_rows], merged[half_rows:ROWS]
        give[n] = jnp.where(tp == 0, bottom, top).astype(BF16)
        keep[n] = jnp.where(tp == 0, top, bottom)
        across(n, f).start()
        written(n, f).start()
    pl.when(me < RING * RING - 1)(lambda: each_halo(lambda h: h.wait_send()))
    for d in range(1, RING):
        (first(0, d) if d in (1, 2, 6, 7) else relayed(d)).wait_send()
        around(lambda p: msg.at[p], s1, s1_send, s1_recv, "sp_1", d).wait_send()
        around(lambda p: back.at[p], carried, s3_send, s3_recv, "sp_1", d).wait_send()

        @pl.when(z + d < RING)
        def _():
            first(1, d).wait_send()
            up_total(d).wait_send()
    for k in range(7):
        for c in range(2):
            for d in range(2):
                pl.when(going(c, d, k))(lambda: hop(c, d, k).wait_send())
    for j in range(2):
        for d in range(2):
            weights(j, d).wait_send()
        passed_on(j).wait_send()

    for n, f in enumerate(columns):
        written(n, f).wait()
        across(n, f).wait_send()
        across(n, f).wait_recv()


def shards(
    state_head_inputs, state_write_vectors, state_read_vectors, state_output_gate,
    presoftplus_steps, extra_decay_log, lane_shrinkage_powers, bypass_coefficient_vector,
    feeder_smoothing_stencil, stored_smoothing_stencil, lookup_smoothing_stencil,
    bundled_rescaling_vector, queries, attention_keys, attention_values, forget_gate_cumsum,
    state_out_weight, attention_out_weight,
):
    hbm = pl.BlockSpec(memory_space=pltpu.HBM)
    dma = pltpu.SemaphoreType.DMA
    kept, taken = pl.pallas_call(
        kernel,
        out_shape=(
            jax.ShapeDtypeStruct((ROWS // 2, 512 * FS), F32),
            jax.ShapeDtypeStruct((ROWS // 2, 512 * FS), BF16),
        ),
        in_specs=[hbm] * 18,
        out_specs=(hbm, hbm),
        scratch_shapes=[
            pltpu.VMEM((ROWS, 512), BF16), pltpu.VMEM((ROWS, ROWS), BF16), pltpu.VMEM((ROWS, ROWS), BF16),
            pltpu.VMEM((ROWS, 512), BF16), pltpu.VMEM((8, ROWS), F32), pltpu.VMEM((8, ROWS), F32),
            pltpu.VMEM((1, 8), F32), pltpu.VMEM((1, 8), F32),
            pltpu.VMEM((4, 512), BF16), pltpu.VMEM((4, ROWS), BF16), pltpu.VMEM((4, ROWS), BF16),
            pltpu.VMEM((1, 512), F32), pltpu.VMEM((ROWS, 512), BF16), pltpu.VMEM((ROWS, ROWS), BF16),
            pltpu.VMEM((ROWS, ROWS), BF16), pltpu.VMEM((8, ROWS), F32),
            pltpu.VMEM((2, RING, RING, BLOCK, ROWS), BF16),
            pltpu.VMEM((4, 2, 2 * ROWS, 2 * ROWS), BF16),
            pltpu.VMEM((ROWS, ROWS), F32),
            pltpu.VMEM((16, 512), BF16),
            pltpu.VMEM((16, ROWS), BF16),
            pltpu.VMEM((16, ROWS), BF16),
            pltpu.VMEM((4, 8, 2 * ROWS), F32),
            pltpu.VMEM((4, HD + 16, 2 * ROWS), F32),
            pltpu.VMEM((RING, HD, ROWS), BF16),
            pltpu.VMEM((RING, HD, ROWS), BF16),
            pltpu.VMEM((MSG, ROWS), BF16),
            pltpu.VMEM((RING, MSG, ROWS), BF16),
            pltpu.VMEM((RING, HD, ROWS), F32),
            pltpu.VMEM((RING, 8, ROWS), F32),
            pltpu.VMEM((RING, HD, ROWS), BF16),
            pltpu.VMEM((RING, HD, ROWS), BF16),
            pltpu.VMEM((ROWS, 512), BF16),
            pltpu.VMEM((ROWS, 512), F32),
            pltpu.VMEM((ROWS, ROWS), BF16),
            pltpu.VMEM((ROWS, 512), F32),
            pltpu.VMEM((2, FS, 512, 512), BF16),
            pltpu.VMEM((FS, ROWS // 2, 512), BF16),
            pltpu.VMEM((FS, ROWS // 2, 512), F32),
            pltpu.VMEM((3, ROWS, 512), F32),
            dma((2, RING)), dma((2, RING)),
            dma((2, 2, 7)), dma((2, 2, 7)),
            dma((RING,)), dma((RING,)), dma((RING,)), dma((RING,)), dma((RING,)), dma((RING,)),
            dma((2, 3)), dma((2, 3)), dma((2,)),
            dma((3,)), dma((3,)), dma((FS,)), dma((FS,)), dma((16,)), dma((FS,)),
            pltpu.SemaphoreType.REGULAR((RING,)), pltpu.SemaphoreType.REGULAR((RING,)),
        ],
        compiler_params=pltpu.CompilerParams(
            collective_id=0, has_side_effects=True, vmem_limit_bytes=60 * 1024 * 1024
        ),
        name="mixer",
    )(
        state_head_inputs[0], state_write_vectors[0], state_read_vectors[0], state_output_gate[0],
        presoftplus_steps[0], extra_decay_log[0],
        lane_shrinkage_powers.reshape(1, -1), bypass_coefficient_vector.reshape(1, -1),
        feeder_smoothing_stencil, stored_smoothing_stencil, lookup_smoothing_stencil,
        bundled_rescaling_vector.reshape(1, -1), queries[0], attention_keys[0], attention_values[0],
        forget_gate_cumsum[0].T, state_out_weight, attention_out_weight,
    )
    return (kept + taken.astype(F32)).astype(BF16)[None]


def solution(mesh):
    split = Mesh(
        mesh.devices.reshape(8, 8, mesh.shape["fs"], mesh.shape["tp"]), ("sp_0", "sp_1", "fs", "tp")
    )
    placed = (
        P("fs", SP, "tp"),
        P("fs", SP, "tp"),
        P("fs", SP, "tp"),
        P("fs", SP, "tp"),
        P("fs", "tp", SP),
        P("fs", "tp", SP),
        P("tp"),
        P("tp"),
        P(None, "tp"),
        P(None, "tp"),
        P(None, "tp"),
        P("tp"),
        P("fs", SP, "tp"),
        P("fs", SP, "tp"),
        P("fs", SP, "tp"),
        P("fs", SP, "tp"),
        P("tp", "fs"),
        P("tp", "fs"),
    )
    return jax.shard_map(
        shards, mesh=split, in_specs=placed, out_specs=P("fs", SP_TP, None), check_vma=False
    )
```
